256 devices in a mesh: sp: 64 (over z, x, core), tp: 4 (over y).
Axes of the slice: x: 4, y: 4, z: 8, core: 2. Of those that a mesh axis runs over, the one named last changes fastest.
Arguments:
- full_queries: bfloat16 [8192, 1024], P('sp', 'tp'), may hold values from -7 to 7
- full_keys: bfloat16 [8192, 512], P('sp', 'tp'), may hold values from -6 to 6
- full_values: bfloat16 [8192, 512], P('sp', 'tp'), may hold values from -6 to 6
- full_gates: float32 [8192, 8], P(None, 'tp'), may hold values from -4096 to 0, as said below
- half_queries: bfloat16 [8192, 1024], P('sp', 'tp'), may hold values from -7 to 7
- half_keys: bfloat16 [8192, 512], P('sp', 'tp'), may hold values from -6 to 6
- half_values: bfloat16 [8192, 512], P('sp', 'tp'), may hold values from -6 to 6
- half_gates: float32 [8192, 16], P(None, 'tp'), may hold values from -4096 to 0, as said below
- residual: bfloat16 [8192, 4096], P('sp'), may hold values from -48 to 48
- full_output: bfloat16 [1024, 4096], P('tp'), may hold values from -0.25 to 0.25
- half_output: bfloat16 [1024, 4096], P('tp'), may hold values from -0.25 to 0.25
- norm_gain: float32 [4096], replicated, may hold values from 0.1 to 1.9
- routes: int32 [8192, 4], P('sp'), may hold values from 0 to 63, all different within a row; in each aligned block of 32 rows (0 to 31, 32 to 63, ...) at most 4 rows name the same one
- route_weights: float32 [8192, 4], P('sp'), may hold values from 0.25 to 1.25
- expert_gate: bfloat16 [64, 4096, 512], P('sp', None, 'tp'), may hold values from -0.09375 to 0.09375
- expert_up: bfloat16 [64, 4096, 512], P('sp', None, 'tp'), may hold values from -0.09375 to 0.09375
- expert_down: bfloat16 [64, 512, 4096], P('sp', 'tp'), may hold values from -0.25 to 0.25
- shared_gate: bfloat16 [4096, 512], P(None, 'tp'), may hold values from -0.09375 to 0.09375
- shared_up: bfloat16 [4096, 512], P(None, 'tp'), may hold values from -0.09375 to 0.09375
- shared_down: bfloat16 [512, 4096], P('tp'), may hold values from -0.25 to 0.25
Outputs:
- mixed: bfloat16 [8192, 4096], P(('sp', 'tp'))
The draws below stay inside these ranges and needn't reach their ends.
Inputs may be any that keep to these rules, and one draw needn't show every extreme that they name: `routes`: in each aligned block of 32 rows no expert is named by more than 4 rows; some expert is named by exactly 4 rows in some block. `full_gates`: each column is a running sum of non-positive terms from the first position on. `half_gates`: each column is a running sum of non-positive terms from the first position on.
All inputs are finite; a program needn't handle non-finite values.
Results may differ from the reference program's by a relative error of at most 0.012.
Values may be sent and summed in bfloat16 or wider, within the bound.
A program may use at most 128 MiB of HBM per device.

```python
import math
import jax
import jax.numpy as jnp
import numpy as np
from jax import lax

D = 4096
WH = 8
WD = 128
WK = 4
NH = 16
ND = 64
NK = 8
FE = 512
FS = 512
TOP = 4
TOK_DEV = 128
SEQUENCE_TOKENS = 8192
TQ = 32
EXPERTS = 64
CAP = 4
N_TP = 4


def clipped_normal(seed_key, shape):
    return jnp.clip(jax.random.normal(seed_key, shape, jnp.float32), -6.0, 6.0)


def cumulative_gates(seed_key, total_head_count, slow_count):
    divided_random_keys = jax.random.split(seed_key, 7)
    order_drawn = jax.random.permutation(divided_random_keys[0], total_head_count)
    gradual_heads = (order_drawn < slow_count).astype(jnp.float32)
    slow_rate = jax.random.uniform(divided_random_keys[1], (total_head_count,), jnp.float32, 0.3, 0.8) / SEQUENCE_TOKENS
    fast_rate = jax.random.uniform(divided_random_keys[2], (total_head_count,), jnp.float32, 0.04, 0.1)
    head_rates = gradual_heads * slow_rate + (1.0 - gradual_heads) * fast_rate
    block_factor = jnp.exp(jax.random.uniform(divided_random_keys[3], (SEQUENCE_TOKENS // TOK_DEV, 1), jnp.float32, math.log(0.5), math.log(2.0)))
    block_factor = jnp.repeat(block_factor, TOK_DEV, axis=0)
    roughness = jax.random.uniform(divided_random_keys[4], (SEQUENCE_TOKENS, total_head_count), jnp.float32, 0.3, 1.7)
    logarithm_steps = -head_rates[None, :] * block_factor * roughness
    spike_position = jax.random.randint(divided_random_keys[5], (2,), 0, SEQUENCE_TOKENS)
    spike_penalty = jax.random.uniform(divided_random_keys[6], (2, total_head_count), jnp.float32, 0.2, 0.4)
    sequence_positions = jnp.arange(SEQUENCE_TOKENS)
    for spike_index in range(2):
        spike_row = (sequence_positions == spike_position[spike_index]).astype(jnp.float32)[:, None]
        logarithm_steps = logarithm_steps + spike_row * jnp.log(1.0 - spike_penalty[spike_index])[None, :] * gradual_heads[None, :]
    return jnp.cumsum(logarithm_steps, axis=0)


def draw_full_queries(key, part):
    drawn = clipped_normal(jax.random.fold_in(key, 1), (SEQUENCE_TOKENS, WH * WD))
    return drawn.astype(jnp.bfloat16)


def draw_full_keys(key, part):
    drawn = clipped_normal(jax.random.fold_in(key, 2), (SEQUENCE_TOKENS, WK * WD))
    return drawn.astype(jnp.bfloat16)


def draw_half_queries(key, part):
    drawn = clipped_normal(jax.random.fold_in(key, 3), (SEQUENCE_TOKENS, NH * ND))
    return drawn.astype(jnp.bfloat16)


def draw_half_keys(key, part):
    drawn = clipped_normal(jax.random.fold_in(key, 4), (SEQUENCE_TOKENS, NK * ND))
    return drawn.astype(jnp.bfloat16)


def draw_full_gates(key, part):
    slow_count = WH // 2
    return cumulative_gates(jax.random.fold_in(key, 5), WH, slow_count).astype(jnp.float32)


def draw_half_gates(key, part):
    slow_count = NH // 2
    return cumulative_gates(jax.random.fold_in(key, 6), NH, slow_count).astype(jnp.float32)


def draw_residual(key, part):
    divided_random_keys = jax.random.split(jax.random.fold_in(key, 7), 3)
    drawn = clipped_normal(divided_random_keys[0], (SEQUENCE_TOKENS, D))
    row_scale = jnp.exp(jax.random.uniform(divided_random_keys[1], (SEQUENCE_TOKENS, 1), jnp.float32, math.log(0.5), math.log(2.0)))
    column_scale = jnp.exp(jax.random.uniform(divided_random_keys[2], (1, D), jnp.float32, math.log(0.4), math.log(4.0)))
    return (drawn * row_scale * column_scale).astype(jnp.bfloat16)


def steps_of(stream_key, shape, shards, smallest, top_value):
    level = 1.0
    for position, blocks in shards:
        heights = jax.random.uniform(jax.random.fold_in(jax.random.fold_in(stream_key, 6), position), (blocks,), jnp.float32, smallest / len(shards), top_value / len(shards))
        level = level * jnp.repeat(jnp.exp(heights), shape[position] // blocks).reshape((-1,) + (1,) * (len(shape) - 1 - position))
    return level


def deal_out(key, own, number, rows, count, top, limit, lean):
    ranking = jax.random.permutation(key, count)
    heavy_load, usual = portions_of(count, rows * top, limit, lean, True), portions_of(count, rows * top, limit, lean, False)
    places = jnp.arange(count)

    def named(sizes, turn):
        used = int((sizes > 0).sum())
        fixed = max(1, used // 4)
        shifted = fixed + (places - fixed + turn * (used - fixed)) % max(1, count - fixed)
        return jnp.zeros((count,), jnp.int32).at[ranking[jnp.where(places < fixed, places, shifted)]].set(jnp.asarray(sizes, jnp.int32))

    sizes = jnp.where(number % 4 == 0, named(heavy_load, number // 4), named(usual, number - number // 4 - 1))
    mixed = jax.random.permutation(jax.random.fold_in(own, 3), count)
    source_of, sink = mixed[0:count // 2 * 2:2], mixed[1:count // 2 * 2:2]
    margin = jnp.minimum(sizes[source_of] - 1, limit - sizes[sink]) // 2
    margin = jnp.where((source_of == ranking[0]) | (sink == ranking[0]) | (sizes[sink] == 0), 0, jnp.maximum(margin, 0))
    shifted = jax.random.randint(jax.random.fold_in(own, 4), (count // 2,), 0, 1 << 20) % (margin + 1)
    sizes = sizes.at[source_of].add(-shifted).at[sink].add(shifted)
    items = jnp.searchsorted(jnp.cumsum(sizes), jnp.arange(rows * top), side="right").astype(jnp.int32)
    listing = items.reshape(top, rows).T
    listing = listing[jax.random.permutation(jax.random.fold_in(own, 1), rows)]
    turn = jax.random.randint(jax.random.fold_in(own, 2), (rows, 1), 0, top)
    return jnp.take_along_axis(listing, (jnp.arange(top)[None, :] + turn) % top, axis=1)


def portions_of(number_of, total, limit, skew, full):
    portions = [(1 << 20) // math.isqrt(grade ** skew) + 1 for grade in range(1, number_of + 1)]
    largest = limit if full else min(limit, max(-(-total // number_of), total * portions[0] // sum(portions)))
    least = 1 if total - largest >= number_of - 1 else 0
    given, surplus = [largest] + [least] * (number_of - 1), total - largest - least * (number_of - 1)
    while surplus > 0:
        movable = [i for i in range(1, number_of) if given[i] < largest] or [i for i in range(1, number_of) if given[i] < limit]
        pool, left = sum([portions[i] for i in movable]), surplus
        for i in movable:
            extra = min(limit - given[i], max(1, left * portions[i] // pool), surplus)
            given[i] = given[i] + extra
            surplus = surplus - extra
    return np.array(given)


def normal_values(stream_key, shape, scale, reach, cuts=(), held_as=jnp.bfloat16):
    values = scale * jax.random.normal(stream_key, shape, jnp.float32)
    if cuts:
        values = values * steps_of(stream_key, shape, cuts, -0.22, 0.18)
    return jnp.clip(values, -reach, reach).astype(held_as)


def setup_inputs(seed: int = 0) -> dict:
    streams_of = jax.random.split(jax.random.key(seed), 21)
    full_queries = draw_full_queries(jax.random.fold_in(streams_of[20], 71), 0)
    full_keys = draw_full_keys(jax.random.fold_in(streams_of[20], 71), 0)
    full_values = normal_values(streams_of[2], (SEQUENCE_TOKENS, WK * WD), 1.0, 6.0, ((0, 64), (1, 4)))
    full_gates = draw_full_gates(jax.random.fold_in(streams_of[20], 71), 0)
    half_queries = draw_half_queries(jax.random.fold_in(streams_of[20], 71), 0)
    half_keys = draw_half_keys(jax.random.fold_in(streams_of[20], 71), 0)
    half_values = normal_values(streams_of[6], (SEQUENCE_TOKENS, NK * ND), 1.0, 6.0, ((0, 64), (1, 4)))
    half_gates = draw_half_gates(jax.random.fold_in(streams_of[20], 71), 0)
    residual = draw_residual(jax.random.fold_in(streams_of[20], 71), 0)
    full_output = normal_values(streams_of[9], (WH * WD, D), ((WH * WD + NH * ND) // 4) ** -0.5, 0.25, ((0, 4),))
    half_output = normal_values(streams_of[10], (NH * ND, D), ((WH * WD + NH * ND) // 4) ** -0.5, 0.25, ((0, 4),))
    norm_gain = jnp.clip(1.0 + 0.18 * jax.random.normal(streams_of[11], (D,), jnp.float32), 0.1, 1.9)
    routes_keys = jax.random.split(jax.random.fold_in(streams_of[12], 1), SEQUENCE_TOKENS // TQ)
    routes_turns = jax.random.permutation(jax.random.fold_in(streams_of[12], 3), SEQUENCE_TOKENS // TQ)
    routes = jax.vmap(lambda own, number: deal_out(jax.random.fold_in(streams_of[12], 2), own, number, TQ, EXPERTS, TOP, CAP, 2))(routes_keys, routes_turns).reshape((SEQUENCE_TOKENS, TOP))
    route_weights = jnp.clip(0.25 + 1.0 * jax.random.uniform(streams_of[13], (SEQUENCE_TOKENS, TOP), jnp.float32) ** steps_of(streams_of[13], (SEQUENCE_TOKENS, TOP), ((0, 64),), -0.2, 0.2), 0.25, 1.25)
    expert_gate = normal_values(streams_of[14], (EXPERTS, D, FE), D ** -0.5, 0.09375, ((0, 64), (2, 4)))
    expert_up = normal_values(streams_of[15], (EXPERTS, D, FE), D ** -0.5, 0.09375, ((0, 64), (2, 4)))
    expert_down = normal_values(streams_of[16], (EXPERTS, FE, D), FE ** -0.5, 0.25, ((0, 64), (1, 4)))
    shared_gate = normal_values(streams_of[17], (D, FS), D ** -0.5, 0.09375, ((1, 4),))
    shared_up = normal_values(streams_of[18], (D, FS), D ** -0.5, 0.09375, ((1, 4),))
    shared_down = normal_values(streams_of[19], (FS, D), FS ** -0.5, 0.25, ((0, 4),))
    return dict(full_queries=full_queries, full_keys=full_keys, full_values=full_values, full_gates=full_gates, half_queries=half_queries, half_keys=half_keys, half_values=half_values, half_gates=half_gates, residual=residual, full_output=full_output, half_output=half_output, norm_gain=norm_gain, routes=routes, route_weights=route_weights, expert_gate=expert_gate, expert_up=expert_up, expert_down=expert_down, shared_gate=shared_gate, shared_up=shared_up, shared_down=shared_down)


def group_attention(queries, keys_in, values_in, gates, total_head_count, key_heads, head_dim):
    tokens = queries.shape[0]
    group_size = total_head_count // key_heads
    block_rows = math.gcd(tokens, 256)
    key_float = keys_in.astype(jnp.float32).reshape(tokens, key_heads, head_dim)
    value_float = values_in.astype(jnp.float32).reshape(tokens, key_heads, head_dim)
    key_gates = jnp.transpose(gates.reshape(tokens, key_heads, group_size), (1, 2, 0))[:, :, None, :]
    sequence_positions = jnp.arange(tokens, dtype=jnp.int32)

    def one_block(block_index):
        first_row = (block_index * block_rows).astype(jnp.int32)
        query_rows = lax.dynamic_slice_in_dim(queries, first_row, block_rows, 0)
        query_rows = query_rows.astype(jnp.float32).reshape(block_rows, key_heads, group_size, head_dim)
        query_gates = lax.dynamic_slice_in_dim(gates, first_row, block_rows, 0)
        query_gates = jnp.transpose(query_gates.reshape(block_rows, key_heads, group_size), (1, 2, 0))[..., None]
        scores = jnp.einsum('tkgd,skd->kgts', query_rows, key_float) * head_dim ** (-0.5)
        scores = scores + query_gates - key_gates
        query_pos = first_row + jnp.arange(block_rows, dtype=jnp.int32)
        allowed = sequence_positions[None, :] <= query_pos[:, None]
        scores = jnp.where(allowed, scores, -jnp.inf)
        row_max = lax.optimization_barrier(jnp.max(scores, axis=-1, keepdims=True))
        weights = jnp.where(allowed, jnp.exp(scores - row_max), 0.0)
        row_total = lax.optimization_barrier(jnp.sum(weights, axis=-1))
        rounded = lax.optimization_barrier(weights.astype(jnp.bfloat16)).astype(jnp.float32)
        summed = jnp.einsum('kgts,skd->kgtd', rounded, value_float)
        result = summed / row_total[..., None]
        result = jnp.transpose(result, (2, 0, 1, 3)).reshape(block_rows, total_head_count * head_dim)
        return result.astype(jnp.bfloat16)
    pieces = lax.map(one_block, jnp.arange(tokens // block_rows, dtype=jnp.int32))
    return pieces.reshape(tokens, total_head_count * head_dim)

def block_swiglu(rows_in, gate_weight, up_weight, down_weight):
    gate_part = jnp.dot(rows_in, gate_weight, preferred_element_type=jnp.float32)
    up_part = jnp.dot(rows_in, up_weight, preferred_element_type=jnp.float32)
    hidden = (jax.nn.silu(gate_part) * up_part).astype(jnp.bfloat16)
    block_width = hidden.shape[1] // N_TP
    summed = jnp.zeros((rows_in.shape[0], down_weight.shape[1]), jnp.float32)
    for block_index in range(N_TP):
        low_edge = block_index * block_width
        product = jnp.dot(hidden[:, low_edge:low_edge + block_width], down_weight[low_edge:low_edge + block_width], preferred_element_type=jnp.float32)
        summed = summed + lax.optimization_barrier(product.astype(jnp.bfloat16)).astype(jnp.float32)
    return summed

def reference(full_queries, full_keys, full_values, full_gates, half_queries, half_keys, half_values, half_gates, residual, full_output, half_output, norm_gain, routes, route_weights, expert_gate, expert_up, expert_down, shared_gate, shared_up, shared_down):
    full_attention = group_attention(full_queries, full_keys, full_values, full_gates, WH, WK, WD)
    half_attention = group_attention(half_queries, half_keys, half_values, half_gates, NH, NK, ND)
    middle = residual.astype(jnp.float32) + jnp.dot(full_attention, full_output, preferred_element_type=jnp.float32) + jnp.dot(half_attention, half_output, preferred_element_type=jnp.float32)
    normed = (middle * lax.rsqrt(lax.optimization_barrier(jnp.mean(middle * middle, axis=-1, keepdims=True)) + 1e-06) * norm_gain).astype(jnp.bfloat16)
    shared_out = block_swiglu(normed, shared_gate, shared_up, shared_down)
    flat_routes = routes.reshape(-1).astype(jnp.int32)
    flat_weights = route_weights.reshape(-1)
    slot_total = SEQUENCE_TOKENS // TQ * CAP

    def one_expert(routed_sum, expert_index):
        sort_key = jnp.where(flat_routes == expert_index, 0, 1).astype(jnp.int32)
        route_order = jnp.argsort(sort_key, stable=True)[:slot_total].astype(jnp.int32)
        is_valid = (flat_routes[route_order] == expert_index).astype(jnp.float32)
        token_index = (route_order // TOP).astype(jnp.int32)
        expert_rows = normed[token_index]
        result = block_swiglu(expert_rows, expert_gate[expert_index], expert_up[expert_index], expert_down[expert_index])
        result = lax.optimization_barrier(result.astype(jnp.bfloat16)).astype(jnp.float32)
        route_scale = flat_weights[route_order] * is_valid
        return (routed_sum.at[token_index].add(route_scale[:, None] * result), None)
    routed, _ = lax.scan(one_expert, jnp.zeros((SEQUENCE_TOKENS, D), jnp.float32), jnp.arange(EXPERTS, dtype=jnp.int32))
    return (middle + shared_out + routed).astype(jnp.bfloat16)
```

```python
import functools
import heapq

import jax
import jax.numpy as jnp
from jax import lax
from jax.experimental import pallas as pl
from jax.experimental.pallas import tpu as pltpu
from jax.sharding import PartitionSpec as P

D = 4096
LOG2E = 1.4426950408889634
BF = jnp.bfloat16
F32 = jnp.float32
MESH = pl.DeviceIdType.MESH
NEG = -1e30


def kv_schedule():
    def onward(part, dz, dx, link):
        out = []
        if part == 0:
            if link in ("own", "z+", "z-"):
                if link == "own":
                    out += ["z+", "z-"]
                elif link == "z+" and dz < 4:
                    out.append("z+")
                elif link == "z-" and dz > -3:
                    out.append("z-")
                out += ["x+", "x-"]
            elif link == "x+" and dx == 1 and dz % 2 == 0:
                out.append("x+")
            elif link == "x-" and dx == -1 and dz % 2 == 1:
                out.append("x-")
        else:
            if link in ("own", "x+", "x-"):
                if link == "own":
                    out += ["x+", "x-"]
                elif link == "x+" and dx == 1:
                    out.append("x+")
                out += ["z+", "z-"]
            elif link == "z+" and (dz < 3 or (dz == 3 and dx in (0, 1))):
                out.append("z+")
            elif link == "z-" and dz < 0 and (dz > -3 or dx not in (0, 1)):
                out.append("z-")
        return out

    free = {"z+": 0.0, "z-": 0.0, "x+": 0.0, "x-": 0.0}
    heap, events, count = [], [], 0

    def send(now, part, dz, dx, link):
        nonlocal count
        start = max(now, free[link])
        free[link] = start + 1.4
        step = 1 if link[1] == "+" else -1
        ndz, ndx = (dz + step, dx) if link[0] == "z" else (dz, dx + step)
        if link[0] == "z" and ndz == -4:
            ndz = 4
        if link[0] == "x" and ndx == -2:
            ndx = 2
        heapq.heappush(heap, (free[link] + 1.5, count, part, ndz, ndx, link))
        count += 1

    for part in (1, 0):
        for link in onward(part, 0, 0, "own"):
            send(0.0, part, 0, 0, link)
    seen = set()
    while heap:
        now, _, part, dz, dx, link = heapq.heappop(heap)
        assert (part, dz, dx) not in seen
        seen.add((part, dz, dx))
        links = onward(part, dz, dx, link)
        events.append((part, dz, dx, tuple(links)))
        for out in links:
            send(now, part, dz, dx, out)
    assert len(events) == 62
    own = [(part, 0, 0, tuple(onward(part, 0, 0, "own"))) for part in (1, 0)]
    return own, events


def position():
    s = lax.axis_index("sp")
    y = lax.axis_index("tp")
    z, x, c = s // 8, (s // 2) % 4, s % 2
    return s, y, z, x, c


def sp_of(z, x, c):
    return lax.rem(z + 8, 8) * 8 + lax.rem(x + 4, 4) * 2 + c


def greet(peers):
    barrier = pltpu.get_barrier_semaphore()
    for peer in peers:
        pl.semaphore_signal(barrier, inc=1, device_id=peer, device_id_type=MESH)
    pl.semaphore_wait(barrier, len(peers))


class YGather:
    def __init__(self, src, dst, send_sem, recv_sem):
        s, y, *_ = position()
        self.src, self.dst, self.send, self.recv = src, dst, send_sem, recv_sem
        self.y = y
        self.up = (s, lax.rem(y + 1, 4))
        self.down = (s, lax.rem(y + 3, 4))

    def copy(self, half, src_y, way, hop):
        slot = way * 3 + (half if hop == 0 else 2)
        return pltpu.make_async_remote_copy(
            src_ref=self.src[half] if hop == 0 else self.dst(src_y, half),
            dst_ref=self.dst(src_y, half),
            send_sem=self.send.at[slot],
            recv_sem=self.recv.at[slot],
            device_id=self.up if way == 0 else self.down,
            device_id_type=MESH,
        )

    def start(self):
        self.copy(0, self.y, 0, 0).start()
        self.copy(1, self.y, 1, 0).start()
        self.copy(1, self.y, 0, 0).start()
        self.copy(0, self.y, 1, 0).start()

    def relay(self):
        below, above = lax.rem(self.y + 3, 4), lax.rem(self.y + 1, 4)
        self.copy(0, below, 0, 0).wait_recv()
        self.copy(0, below, 0, 1).start()
        self.copy(1, above, 1, 0).wait_recv()
        self.copy(1, above, 1, 1).start()

    def finish(self):
        below, above, far = lax.rem(self.y + 3, 4), lax.rem(self.y + 1, 4), lax.rem(self.y + 2, 4)
        self.copy(1, below, 0, 0).wait_recv()
        self.copy(0, above, 1, 0).wait_recv()
        self.copy(0, far, 0, 1).wait_recv()
        self.copy(1, far, 1, 1).wait_recv()
        self.sent()

    def sent(self):
        below, above = lax.rem(self.y + 3, 4), lax.rem(self.y + 1, 4)
        for half in (0, 1):
            for way in (0, 1):
                self.copy(half, self.y, way, 0).wait_send()
        self.copy(0, below, 0, 1).wait_send()
        self.copy(1, above, 1, 1).wait_send()


def attend_kernel(
    fq, fk, fv, gf, hq, hk, hv, gh, res, wf, wh, gain, eg, eu,
    mid_out, norm_out, gate_out, up_out,
    kva, kvb, qs, acc, mx, tot, att, part, inbox, resv,
    own_sem, kv_send, kv_recv, w_send, w_recv, rs_send, rs_recv, res_sem,
):
    s, y, z, x, c = position()
    sib = (s + 1 - 2 * c, y)
    to = {
        "z+": (sp_of(z + 1, x, c), y),
        "z-": (sp_of(z - 1, x, c), y),
        "x+": (sp_of(z, x + 1, c), y),
        "x-": (sp_of(z, x - 1, c), y),
    }
    others = [(s, lax.rem(y + k, 4)) for k in (2, 1, 3)]
    greet(list(to.values()) + [sib] + others)

    kv = (kva, kvb)
    pieces = [
        (fk, kva, 0), (fv, kva, 128), (hk, kvb, 0), (hv, kvb, 128),
    ]
    own = [
        pltpu.make_async_copy(src, dst.at[s, :, pl.ds(at, 128)], own_sem.at[i])
        for i, (src, dst, at) in enumerate(pieces)
    ]
    for copy in own:
        copy.start()
    res_copy = pltpu.make_async_copy(res.at[pl.ds(y * 32, 32)], resv, res_sem)
    res_copy.start()

    def hop(prt, idx, device):
        return pltpu.make_async_remote_copy(
            src_ref=kv[prt].at[idx],
            dst_ref=kv[prt].at[idx],
            send_sem=kv_send.at[prt],
            recv_sem=kv_recv.at[prt, idx],
            device_id=device,
            device_id_type=MESH,
        )

    own_events, events = kv_schedule()
    for prt, _, _, links in own_events:
        own[2 * prt].wait()
        own[2 * prt + 1].wait()
        for link in links:
            hop(prt, s, to[link]).start()
        hop(prt, s, sib).start()

    half_rows = 2048
    gates = YGather(
        [eg.at[pl.ds(h * half_rows, half_rows)] for h in (0, 1)],
        lambda j, h: gate_out.at[j, pl.ds(h * half_rows, half_rows)],
        w_send.at[0], w_recv.at[0],
    )
    ups = YGather(
        [eu.at[pl.ds(h * 1024, 1024)] for h in (0, 1)],
        lambda j, h: up_out.at[j, pl.ds(h * 1024, 1024)],
        w_send.at[1], w_recv.at[1],
    )
    gates.start()
    ups.start()

    lane = lax.broadcasted_iota(jnp.int32, (128, 128), 1)
    qs[0, 0:128] = fq[:, 0:128]
    qs[0, 128:256] = fq[:, 128:256]
    h01 = hq[:, 0:128].astype(F32)
    h23 = hq[:, 128:256].astype(F32)
    qs[1, 0:128] = jnp.where(lane < 64, h01, 0.0).astype(BF)
    qs[1, 128:256] = jnp.where(lane < 64, pltpu.roll(h01, 64, 1), 0.0).astype(BF)
    qs[2, 0:128] = jnp.where(lane >= 64, pltpu.roll(h23, 64, 1), 0.0).astype(BF)
    qs[2, 128:256] = jnp.where(lane >= 64, h23, 0.0).astype(BF)
    acc[...] = jnp.zeros_like(acc)
    tot[...] = jnp.zeros_like(tot)
    mx[...] = jnp.full_like(mx, NEG)

    for i, (prt, dz, dx, links) in enumerate(events):
        idx = sp_of(z - dz, x - dx, c)
        hop(prt, idx, sib).wait_recv()
        for link in links:
            hop(prt, idx, to[link]).start()
        hop(prt, idx, sib).start()
        if i == 30:
            gates.relay()
    ups.relay()

    @pl.loop(0, 32)
    def _(i):
        idx = 2 * i + 1 - c
        for prt in (0, 1):
            hop(prt, idx, sib).wait_recv()

    row0 = s * 128
    gfirst = gf[:, pl.ds(pl.multiple_of(row0, 128), 128)][:, 0:1]
    hfirst = gh[:, pl.ds(pl.multiple_of(row0, 128), 128)][:, 0:1]

    def chunk(at, masked):
        key0 = pl.multiple_of(at * 1024, 1024)
        fg = (gf[:, pl.ds(key0, 1024)] - gfirst) * LOG2E
        hg = (gh[:, pl.ds(key0, 1024)] - hfirst) * LOG2E
        if masked:
            qpos = (s % 8) * 128 + lax.broadcasted_iota(jnp.int32, (128, 1024), 0)
            kpos = lax.broadcasted_iota(jnp.int32, (128, 1024), 1)
            allowed = kpos <= qpos
        for g in range(3):
            store = kva if g == 0 else kvb
            k = store[pl.ds(at * 8, 8), :, 0:128].reshape(1024, 128)
            v = store[pl.ds(at * 8, 8), :, 128:256].reshape(1024, 128)
            scale = (128 ** -0.5 if g == 0 else 0.125) * LOG2E
            scores = lax.dot_general(
                qs[g], k, (((1,), (1,)), ((), ())), preferred_element_type=F32
            )
            for r in (0, 1):
                row = fg[r : r + 1] if g == 0 else hg[2 * (g - 1) + r : 2 * (g - 1) + r + 1]
                t = scores[r * 128 : (r + 1) * 128] * scale - row
                if masked:
                    t = jnp.where(allowed, t, NEG)
                old = mx[g, pl.ds(r * 128, 128)]
                new = jnp.maximum(old, jnp.max(t, axis=1, keepdims=True))
                p = jnp.exp2(t - new[:, 0:1])
                shrink = jnp.exp2(old - new)
                mx[g, pl.ds(r * 128, 128)] = new
                tot[g, pl.ds(r * 128, 128)] = (
                    tot[g, pl.ds(r * 128, 128)] * shrink + jnp.sum(p, axis=1, keepdims=True)
                )
                acc[g, pl.ds(r * 128, 128)] = acc[g, pl.ds(r * 128, 128)] * shrink + jnp.dot(
                    p.astype(BF), v, preferred_element_type=F32
                )

    @pl.loop(0, z)
    def _(at):
        chunk(at, False)

    chunk(z, True)

    outs = [
        [acc[g, r * 128 : (r + 1) * 128] / tot[g, r * 128 : (r + 1) * 128] for r in (0, 1)]
        for g in range(3)
    ]
    att[:, 0:128] = outs[0][0].astype(BF)
    att[:, 128:256] = outs[0][1].astype(BF)
    att[:, 256:384] = jnp.where(lane < 64, outs[1][0], pltpu.roll(outs[1][1], 64, 1)).astype(BF)
    att[:, 384:512] = jnp.where(lane < 64, pltpu.roll(outs[2][0], 64, 1), outs[2][1]).astype(BF)

    gates.finish()
    ups.finish()

    def share(k, n, device):
        return pltpu.make_async_remote_copy(
            src_ref=part.at[lax.rem(y + k, 4), :, pl.ds(n * 1024, 1024)],
            dst_ref=inbox.at[k - 1, :, pl.ds(n * 1024, 1024)],
            send_sem=rs_send.at[k - 1, n],
            recv_sem=rs_recv.at[k - 1, n],
            device_id=device,
            device_id_type=MESH,
        )

    for n in range(4):
        cols = slice(n * 1024, (n + 1) * 1024)
        product = jnp.dot(att[:, 0:256], wf[:, cols], preferred_element_type=F32) + jnp.dot(
            att[:, 256:512], wh[:, cols], preferred_element_type=F32
        )
        part[:, :, cols] = product.astype(BF).reshape(4, 32, 1024)
        for k, device in zip((2, 1, 3), others):
            share(k, n, device).start()
    res_copy.wait()
    square = jnp.zeros((32, 1), F32)
    for n in range(4):
        cols = slice(n * 1024, (n + 1) * 1024)
        total = resv[:, cols].astype(F32) + part[y, :, cols].astype(F32)
        for k, device in zip((2, 1, 3), others):
            share(k, n, device).wait_recv()
            total = total + inbox[k - 1, :, cols].astype(F32)
        mid_out[:, cols] = total
        square = square + jnp.sum(total * total, axis=1, keepdims=True)
    factor = lax.rsqrt(square * (1.0 / D) + 1e-06)
    norm_out[...] = (mid_out[...] * factor * gain[...]).astype(BF)

    for n in range(4):
        for k, device in zip((2, 1, 3), others):
            share(k, n, device).wait_send()
    for prt in (0, 1):
        everything = kv[prt].at[pl.ds(0, 63)]
        pltpu.make_async_copy(everything, everything, kv_send.at[prt]).wait()


def attend(fq, fk, fv, gf, hq, hk, hv, gh, res, wf, wh, gain, eg, eu):
    vmem = pl.BlockSpec(memory_space=pltpu.VMEM)
    anym = pl.BlockSpec(memory_space=pl.ANY)
    return pl.pallas_call(
        attend_kernel,
        name="attend",
        out_shape=(
            jax.ShapeDtypeStruct((32, D), F32),
            jax.ShapeDtypeStruct((32, D), BF),
            jax.ShapeDtypeStruct((4, 4096, 128), BF),
            jax.ShapeDtypeStruct((4, 2048, 128), BF),
        ),
        in_specs=[vmem, anym, anym, vmem, vmem, anym, anym, vmem, anym, vmem, vmem, vmem, anym, anym],
        out_specs=[vmem, vmem, anym, anym],
        scratch_shapes=[
            pltpu.VMEM((64, 128, 256), BF),
            pltpu.VMEM((64, 128, 256), BF),
            pltpu.VMEM((3, 256, 128), BF),
            pltpu.VMEM((3, 256, 128), F32),
            pltpu.VMEM((3, 256, 128), F32),
            pltpu.VMEM((3, 256, 128), F32),
            pltpu.VMEM((128, 512), BF),
            pltpu.VMEM((4, 32, D), BF),
            pltpu.VMEM((3, 32, D), BF),
            pltpu.VMEM((32, D), BF),
            pltpu.SemaphoreType.DMA((4,)),
            pltpu.SemaphoreType.DMA((2,)),
            pltpu.SemaphoreType.DMA((2, 64)),
            pltpu.SemaphoreType.DMA((2, 6)),
            pltpu.SemaphoreType.DMA((2, 6)),
            pltpu.SemaphoreType.DMA((3, 4)),
            pltpu.SemaphoreType.DMA((3, 4)),
            pltpu.SemaphoreType.DMA,
        ],
        compiler_params=pltpu.CompilerParams(
            collective_id=0, has_side_effects=True, vmem_limit_bytes=56 * 1024 * 1024
        ),
    )(fq, fk, fv, gf, hq, hk, hv, gh, res, wf, wh, gain, eg, eu)


def build_picks(route_rows, experts_count, capacity):
    flat_routes = route_rows.reshape(-1)
    onehot = (flat_routes[:, None] == jnp.arange(experts_count, dtype=jnp.int32)[None, :]).astype(
        jnp.int32
    )
    earlier = jnp.cumsum(onehot, axis=0) - onehot
    slot_rank = jnp.sum(earlier * onehot, axis=1)
    slot_ids = flat_routes * capacity + slot_rank
    picked = slot_ids[:, None] == jnp.arange(experts_count * capacity, dtype=jnp.int32)[None, :]
    return picked.astype(jnp.bfloat16).reshape(
        route_rows.shape[0], route_rows.shape[1], experts_count * capacity
    )


def body(
    full_queries, full_keys, full_values, full_gates, half_queries, half_keys, half_values,
    half_gates, residual, full_output, half_output, norm_gain, routes, route_weights,
    expert_gate, expert_up, expert_down, shared_gate, shared_up, shared_down,
):
    quarter = lax.axis_index("tp")
    middle, normed_own, gates_g, ups_g = attend(
        full_queries, full_keys, full_values, full_gates.T, half_queries, half_keys, half_values,
        half_gates.T, residual, full_output, half_output, norm_gain.reshape(1, D),
        expert_gate[0], expert_up[0],
    )
    own_g = lax.dynamic_update_slice(gates_g, expert_gate, (quarter, 0, 0))
    own_u = lax.dynamic_update_slice(ups_g, expert_up[:, :2048], (quarter, 0, 0))
    whole_gate = jnp.moveaxis(own_g, 0, 1).reshape(4096, 512)
    up_top = jnp.moveaxis(own_u, 0, 1).reshape(2048, 512)
    up_bot = lax.all_gather(expert_up[0, 2048:], "tp", axis=1, tiled=True)
    whole_up = jnp.concatenate([up_top, up_bot], 0)
    whole_down = lax.all_gather(expert_down[0], "tp", axis=0, tiled=True)
    normed = lax.all_gather(normed_own, "tp", axis=0, tiled=True)
    shared_hidden = (
        jax.nn.silu(jnp.dot(normed, shared_gate, preferred_element_type=F32))
        * jnp.dot(normed, shared_up, preferred_element_type=F32)
    ).astype(BF)
    shared_term = jnp.dot(shared_hidden, shared_down, preferred_element_type=F32).reshape(4, 32, D)
    own_routes = lax.dynamic_slice_in_dim(routes, quarter * 32, 32, 0)
    own_picks = build_picks(own_routes, 64, 4)
    occupancy = jnp.sum(own_picks, axis=1)
    buffer_rows = jnp.einsum("ts,td->sd", occupancy, normed_own, preferred_element_type=F32).astype(BF)
    received = lax.all_to_all(buffer_rows.reshape(64, 4, D), "sp", split_axis=0, concat_axis=0, tiled=True)
    flat_rows = received.reshape(-1, D)
    gate_part = jnp.dot(flat_rows, whole_gate, preferred_element_type=F32)
    up_part = jnp.dot(flat_rows, whole_up, preferred_element_type=F32)
    hidden = (jax.nn.silu(gate_part) * up_part).astype(BF)
    finished = jnp.dot(hidden, whole_down, preferred_element_type=F32).astype(BF).reshape(64, 4, D)
    summed = lax.psum_scatter(shared_term.astype(BF), "tp", scatter_dimension=0, tiled=True).astype(F32)[0]
    returned = lax.all_to_all(finished, "sp", split_axis=0, concat_axis=0, tiled=True)
    gathered = jnp.einsum("tks,sd->tkd", own_picks, returned.reshape(256, D), preferred_element_type=F32)
    own_weights = lax.dynamic_slice_in_dim(route_weights, quarter * 32, 32, 0)
    routed = jnp.sum(own_weights[..., None] * gathered, axis=1)
    return (middle + summed + routed).astype(BF)


def solution(mesh):
    return jax.shard_map(
        body,
        mesh=mesh,
        in_specs=(
            P("sp", "tp"), P("sp", "tp"), P("sp", "tp"), P(None, "tp"),
            P("sp", "tp"), P("sp", "tp"), P("sp", "tp"), P(None, "tp"),
            P("sp", None), P("tp", None), P("tp", None), P(), P("sp", None), P("sp", None),
            P("sp", None, "tp"), P("sp", None, "tp"), P("sp", "tp", None),
            P(None, "tp"), P(None, "tp"), P("tp", None),
        ),
        out_specs=P(("sp", "tp"), None),
        check_vma=False,
    )
```

```python
import functools
import heapq

import jax
import jax.numpy as jnp
from jax import lax
from jax.experimental import pallas as pl
from jax.experimental.pallas import tpu as pltpu
from jax.sharding import PartitionSpec as P

D = 4096
LOG2E = 1.4426950408889634
BF = jnp.bfloat16
F32 = jnp.float32
MESH = pl.DeviceIdType.MESH
NEG = -1e30


def kv_schedule():
    def onward(part, dz, dx, link):
        out = []
        if part == 0:
            if link in ("own", "z+", "z-"):
                if link == "own":
                    out += ["z+", "z-"]
                elif link == "z+" and dz < 4:
                    out.append("z+")
                elif link == "z-" and dz > -3:
                    out.append("z-")
                out += ["x+", "x-"]
            elif link == "x+" and dx == 1 and dz % 2 == 0:
                out.append("x+")
            elif link == "x-" and dx == -1 and dz % 2 == 1:
                out.append("x-")
        else:
            if link in ("own", "x+", "x-"):
                if link == "own":
                    out += ["x+", "x-"]
                elif link == "x+" and dx == 1:
                    out.append("x+")
                out += ["z+", "z-"]
            elif link == "z+" and (dz < 3 or (dz == 3 and dx in (0, 1))):
                out.append("z+")
            elif link == "z-" and dz < 0 and (dz > -3 or dx not in (0, 1)):
                out.append("z-")
        return out

    free = {"z+": 0.0, "z-": 0.0, "x+": 0.0, "x-": 0.0}
    heap, events, count = [], [], 0

    def send(now, part, dz, dx, link):
        nonlocal count
        start = max(now, free[link])
        free[link] = start + 1.4
        step = 1 if link[1] == "+" else -1
        ndz, ndx = (dz + step, dx) if link[0] == "z" else (dz, dx + step)
        if link[0] == "z" and ndz == -4:
            ndz = 4
        if link[0] == "x" and ndx == -2:
            ndx = 2
        heapq.heappush(heap, (free[link] + 1.5, count, part, ndz, ndx, link))
        count += 1

    for part in (1, 0):
        for link in onward(part, 0, 0, "own"):
            send(0.0, part, 0, 0, link)
    seen = set()
    while heap:
        now, _, part, dz, dx, link = heapq.heappop(heap)
        assert (part, dz, dx) not in seen
        seen.add((part, dz, dx))
        links = onward(part, dz, dx, link)
        events.append((part, dz, dx, tuple(links)))
        for out in links:
            send(now, part, dz, dx, out)
    assert len(events) == 62
    own = [(part, 0, 0, tuple(onward(part, 0, 0, "own"))) for part in (1, 0)]
    return own, events


def position():
    s = lax.axis_index("sp")
    y = lax.axis_index("tp")
    z, x, c = s // 8, (s // 2) % 4, s % 2
    return s, y, z, x, c


def sp_of(z, x, c):
    return lax.rem(z + 8, 8) * 8 + lax.rem(x + 4, 4) * 2 + c


def greet(peers):
    barrier = pltpu.get_barrier_semaphore()
    for peer in peers:
        pl.semaphore_signal(barrier, inc=1, device_id=peer, device_id_type=MESH)
    pl.semaphore_wait(barrier, len(peers))


class YGather:
    def __init__(self, src, dst, send_sem, recv_sem):
        s, y, *_ = position()
        self.src, self.dst, self.send, self.recv = src, dst, send_sem, recv_sem
        self.y = y
        self.up = (s, lax.rem(y + 1, 4))
        self.down = (s, lax.rem(y + 3, 4))

    def copy(self, half, src_y, way, hop):
        slot = way * 3 + (half if hop == 0 else 2)
        return pltpu.make_async_remote_copy(
            src_ref=self.src[half] if hop == 0 else self.dst(src_y, half),
            dst_ref=self.dst(src_y, half),
            send_sem=self.send.at[slot],
            recv_sem=self.recv.at[slot],
            device_id=self.up if way == 0 else self.down,
            device_id_type=MESH,
        )

    def start(self):
        self.copy(0, self.y, 0, 0).start()
        self.copy(1, self.y, 1, 0).start()
        self.copy(1, self.y, 0, 0).start()
        self.copy(0, self.y, 1, 0).start()

    def relay(self):
        below, above = lax.rem(self.y + 3, 4), lax.rem(self.y + 1, 4)
        self.copy(0, below, 0, 0).wait_recv()
        self.copy(0, below, 0, 1).start()
        self.copy(1, above, 1, 0).wait_recv()
        self.copy(1, above, 1, 1).start()

    def finish(self):
        below, above, far = lax.rem(self.y + 3, 4), lax.rem(self.y + 1, 4), lax.rem(self.y + 2, 4)
        self.copy(1, below, 0, 0).wait_recv()
        self.copy(0, above, 1, 0).wait_recv()
        self.copy(0, far, 0, 1).wait_recv()
        self.copy(1, far, 1, 1).wait_recv()
        self.sent()

    def sent(self):
        below, above = lax.rem(self.y + 3, 4), lax.rem(self.y + 1, 4)
        for half in (0, 1):
            for way in (0, 1):
                self.copy(half, self.y, way, 0).wait_send()
        self.copy(0, below, 0, 1).wait_send()
        self.copy(1, above, 1, 1).wait_send()


def attend_kernel(
    fq, fk, fv, gf, hq, hk, hv, gh, res, wf, wh, gain, eg, eu,
    mid_out, norm_out, gate_out, up_out,
    kva, kvb, qs, acc, mx, tot, att, part, inbox, resv,
    own_sem, kv_send, kv_recv, w_send, w_recv, rs_send, rs_recv, res_sem,
):
    s, y, z, x, c = position()
    sib = (s + 1 - 2 * c, y)
    to = {
        "z+": (sp_of(z + 1, x, c), y),
        "z-": (sp_of(z - 1, x, c), y),
        "x+": (sp_of(z, x + 1, c), y),
        "x-": (sp_of(z, x - 1, c), y),
    }
    others = [(s, lax.rem(y + k, 4)) for k in (2, 1, 3)]
    greet(list(to.values()) + [sib] + others)

    kv = (kva, kvb)
    pieces = [
        (fk, kva, 0), (fv, kva, 128), (hk, kvb, 0), (hv, kvb, 128),
    ]
    own = [
        pltpu.make_async_copy(src, dst.at[s, :, pl.ds(at, 128)], own_sem.at[i])
        for i, (src, dst, at) in enumerate(pieces)
    ]
    for copy in own:
        copy.start()
    res_copy = pltpu.make_async_copy(res.at[pl.ds(y * 32, 32)], resv, res_sem)
    res_copy.start()

    def hop(prt, idx, device):
        return pltpu.make_async_remote_copy(
            src_ref=kv[prt].at[idx],
            dst_ref=kv[prt].at[idx],
            send_sem=kv_send.at[prt],
            recv_sem=kv_recv.at[prt, idx],
            device_id=device,
            device_id_type=MESH,
        )

    own_events, events = kv_schedule()
    for prt, _, _, links in own_events:
        own[2 * prt].wait()
        own[2 * prt + 1].wait()
        for link in links:
            hop(prt, s, to[link]).start()
        hop(prt, s, sib).start()

    half_rows = 2048
    gates = YGather(
        [eg.at[pl.ds(h * half_rows, half_rows)] for h in (0, 1)],
        lambda j, h: gate_out.at[j, pl.ds(h * half_rows, half_rows)],
        w_send.at[0], w_recv.at[0],
    )
    ups = YGather(
        [eu.at[pl.ds(h * 1024, 1024)] for h in (0, 1)],
        lambda j, h: up_out.at[j, pl.ds(h * 1024, 1024)],
        w_send.at[1], w_recv.at[1],
    )
    gates.start()
    ups.start()

    lane = lax.broadcasted_iota(jnp.int32, (128, 128), 1)
    qs[0, 0:128] = fq[:, 0:128]
    qs[0, 128:256] = fq[:, 128:256]
    h01 = hq[:, 0:128].astype(F32)
    h23 = hq[:, 128:256].astype(F32)
    qs[1, 0:128] = jnp.where(lane < 64, h01, 0.0).astype(BF)
    qs[1, 128:256] = jnp.where(lane < 64, pltpu.roll(h01, 64, 1), 0.0).astype(BF)
    qs[2, 0:128] = jnp.where(lane >= 64, pltpu.roll(h23, 64, 1), 0.0).astype(BF)
    qs[2, 128:256] = jnp.where(lane >= 64, h23, 0.0).astype(BF)
    acc[...] = jnp.zeros_like(acc)
    tot[...] = jnp.zeros_like(tot)
    mx[...] = jnp.full_like(mx, NEG)

    for i, (prt, dz, dx, links) in enumerate(events):
        idx = sp_of(z - dz, x - dx, c)
        hop(prt, idx, sib).wait_recv()
        for link in links:
            hop(prt, idx, to[link]).start()
        hop(prt, idx, sib).start()
        if i == 30:
            gates.relay()
    ups.relay()

    @pl.loop(0, 32)
    def _(i):
        idx = 2 * i + 1 - c
        for prt in (0, 1):
            hop(prt, idx, sib).wait_recv()

    row0 = s * 128
    gfirst = gf[:, pl.ds(pl.multiple_of(row0, 128), 128)][:, 0:1]
    hfirst = gh[:, pl.ds(pl.multiple_of(row0, 128), 128)][:, 0:1]

    def chunk(at, masked):
        key0 = pl.multiple_of(at * 1024, 1024)
        fg = (gf[:, pl.ds(key0, 1024)] - gfirst) * LOG2E
        hg = (gh[:, pl.ds(key0, 1024)] - hfirst) * LOG2E
        if masked:
            qpos = (s % 8) * 128 + lax.broadcasted_iota(jnp.int32, (128, 1024), 0)
            kpos = lax.broadcasted_iota(jnp.int32, (128, 1024), 1)
            allowed = kpos <= qpos
        for g in range(3):
            store = kva if g == 0 else kvb
            k = store[pl.ds(at * 8, 8), :, 0:128].reshape(1024, 128)
            v = store[pl.ds(at * 8, 8), :, 128:256].reshape(1024, 128)
            scale = (128 ** -0.5 if g == 0 else 0.125) * LOG2E
            scores = lax.dot_general(
                qs[g], k, (((1,), (1,)), ((), ())), preferred_element_type=F32
            )
            for r in (0, 1):
                row = fg[r : r + 1] if g == 0 else hg[2 * (g - 1) + r : 2 * (g - 1) + r + 1]
                t = scores[r * 128 : (r + 1) * 128] * scale - row
                if masked:
                    t = jnp.where(allowed, t, NEG)
                old = mx[g, pl.ds(r * 128, 128)]
                new = jnp.maximum(old, jnp.max(t, axis=1, keepdims=True))
                p = jnp.exp2(t - new[:, 0:1])
                shrink = jnp.exp2(old - new)
                mx[g, pl.ds(r * 128, 128)] = new
                tot[g, pl.ds(r * 128, 128)] = (
                    tot[g, pl.ds(r * 128, 128)] * shrink + jnp.sum(p, axis=1, keepdims=True)
                )
                acc[g, pl.ds(r * 128, 128)] = acc[g, pl.ds(r * 128, 128)] * shrink + jnp.dot(
                    p.astype(BF), v, preferred_element_type=F32
                )

    @pl.loop(0, z)
    def _(at):
        chunk(at, False)

    chunk(z, True)

    outs = [
        [acc[g, r * 128 : (r + 1) * 128] / tot[g, r * 128 : (r + 1) * 128] for r in (0, 1)]
        for g in range(3)
    ]
    att[:, 0:128] = outs[0][0].astype(BF)
    att[:, 128:256] = outs[0][1].astype(BF)
    att[:, 256:384] = jnp.where(lane < 64, outs[1][0], pltpu.roll(outs[1][1], 64, 1)).astype(BF)
    att[:, 384:512] = jnp.where(lane < 64, pltpu.roll(outs[2][0], 64, 1), outs[2][1]).astype(BF)

    gates.finish()
    ups.finish()

    def share(k, n, device):
        return pltpu.make_async_remote_copy(
            src_ref=part.at[lax.rem(y + k, 4), :, pl.ds(n * 1024, 1024)],
            dst_ref=inbox.at[k - 1, :, pl.ds(n * 1024, 1024)],
            send_sem=rs_send.at[k - 1, n],
            recv_sem=rs_recv.at[k - 1, n],
            device_id=device,
            device_id_type=MESH,
        )

    for n in range(4):
        cols = slice(n * 1024, (n + 1) * 1024)
        product = jnp.dot(att[:, 0:256], wf[:, cols], preferred_element_type=F32) + jnp.dot(
            att[:, 256:512], wh[:, cols], preferred_element_type=F32
        )
        part[:, :, cols] = product.astype(BF).reshape(4, 32, 1024)
        for k, device in zip((2, 1, 3), others):
            share(k, n, device).start()
    res_copy.wait()
    square = jnp.zeros((32, 1), F32)
    for n in range(4):
        cols = slice(n * 1024, (n + 1) * 1024)
        total = resv[:, cols].astype(F32) + part[y, :, cols].astype(F32)
        for k, device in zip((2, 1, 3), others):
            share(k, n, device).wait_recv()
            total = total + inbox[k - 1, :, cols].astype(F32)
        mid_out[:, cols] = total
        square = square + jnp.sum(total * total, axis=1, keepdims=True)
    factor = lax.rsqrt(square * (1.0 / D) + 1e-06)
    norm_out[...] = (mid_out[...] * factor * gain[...]).astype(BF)

    for n in range(4):
        for k, device in zip((2, 1, 3), others):
            share(k, n, device).wait_send()
    for prt in (0, 1):
        everything = kv[prt].at[pl.ds(0, 63)]
        pltpu.make_async_copy(everything, everything, kv_send.at[prt]).wait()


def attend(fq, fk, fv, gf, hq, hk, hv, gh, res, wf, wh, gain, eg, eu):
    vmem = pl.BlockSpec(memory_space=pltpu.VMEM)
    anym = pl.BlockSpec(memory_space=pl.ANY)
    return pl.pallas_call(
        attend_kernel,
        name="attend",
        out_shape=(
            jax.ShapeDtypeStruct((32, D), F32),
            jax.ShapeDtypeStruct((32, D), BF),
            jax.ShapeDtypeStruct((4, 4096, 128), BF),
            jax.ShapeDtypeStruct((4, 2048, 128), BF),
        ),
        in_specs=[vmem, anym, anym, vmem, vmem, anym, anym, vmem, anym, vmem, vmem, vmem, anym, anym],
        out_specs=[vmem, vmem, anym, anym],
        scratch_shapes=[
            pltpu.VMEM((64, 128, 256), BF),
            pltpu.VMEM((64, 128, 256), BF),
            pltpu.VMEM((3, 256, 128), BF),
            pltpu.VMEM((3, 256, 128), F32),
            pltpu.VMEM((3, 256, 128), F32),
            pltpu.VMEM((3, 256, 128), F32),
            pltpu.VMEM((128, 512), BF),
            pltpu.VMEM((4, 32, D), BF),
            pltpu.VMEM((3, 32, D), BF),
            pltpu.VMEM((32, D), BF),
            pltpu.SemaphoreType.DMA((4,)),
            pltpu.SemaphoreType.DMA((2,)),
            pltpu.SemaphoreType.DMA((2, 64)),
            pltpu.SemaphoreType.DMA((2, 6)),
            pltpu.SemaphoreType.DMA((2, 6)),
            pltpu.SemaphoreType.DMA((3, 4)),
            pltpu.SemaphoreType.DMA((3, 4)),
            pltpu.SemaphoreType.DMA,
        ],
        compiler_params=pltpu.CompilerParams(
            collective_id=0, has_side_effects=True, vmem_limit_bytes=56 * 1024 * 1024
        ),
    )(fq, fk, fv, gf, hq, hk, hv, gh, res, wf, wh, gain, eg, eu)


REL = (0, -1, 1, -2, 2, -3, 3, 4)
AT = {r: i for i, r in enumerate(REL)}
AT[-4] = AT[4]


class Exchange:
    def __init__(self, src, dst, relay, send, recv, rsend, rrecv):
        self.src, self.dst, self.rl = src, dst, relay
        self.send, self.recv, self.rsend, self.rrecv = send, recv, rsend, rrecv
        s, y, z, x, c = position()
        self.core = (c, 1 - c)
        self.dev = lambda d, core: (sp_of(z, x + d, core), y)

    def direct(self, g, d, crel):
        m = d * 2 + crel
        slot = ((4 - d) % 4) * 2 + crel
        if d == 2:
            return pltpu.make_async_remote_copy(
                src_ref=self.src.at[pl.ds(g * 128 + 16 * m, 16)],
                dst_ref=self.rl.at[g, crel],
                send_sem=self.send.at[g, m],
                recv_sem=self.rrecv.at[g, crel],
                device_id=self.dev(1 if crel == 0 else 3, self.core[0]),
                device_id_type=MESH,
            )
        return pltpu.make_async_remote_copy(
            src_ref=self.src.at[pl.ds(g * 128 + 16 * m, 16)],
            dst_ref=self.dst.at[pl.ds(g * 128 + 16 * slot, 16)],
            send_sem=self.send.at[g, m],
            recv_sem=self.recv.at[g, slot],
            device_id=self.dev(d, self.core[crel]),
            device_id_type=MESH,
        )

    def passed(self, g, crel):
        slot = 4 + crel
        return pltpu.make_async_remote_copy(
            src_ref=self.rl.at[g, crel],
            dst_ref=self.dst.at[pl.ds(g * 128 + 16 * slot, 16)],
            send_sem=self.rsend.at[g, crel],
            recv_sem=self.recv.at[g, slot],
            device_id=self.dev(1 if crel == 0 else 3, self.core[crel]),
            device_id_type=MESH,
        )

    def local(self, g):
        return pltpu.make_async_copy(
            self.src.at[pl.ds(g * 128, 16)],
            self.dst.at[pl.ds(g * 128, 16)],
            self.recv.at[g, 0],
        )

    def start(self, g):
        for d, crel in ((2, 0), (2, 1), (1, 0), (3, 0), (1, 1), (3, 1), (0, 1)):
            self.direct(g, d, crel).start()
        self.local(g).start()

    def relay(self, g):
        for crel in (0, 1):
            self.direct(g, 2, crel).wait_recv()
            self.passed(g, crel).start()

    def arrived(self, g):
        self.local(g).wait()
        for d, crel in ((0, 1), (1, 0), (3, 0), (1, 1), (3, 1)):
            self.direct(g, d, crel).wait_recv()
        for crel in (0, 1):
            self.passed(g, crel).wait_recv()

    def sent(self, g):
        for d, crel in ((2, 0), (2, 1), (1, 0), (3, 0), (1, 1), (3, 1), (0, 1)):
            self.direct(g, d, crel).wait_send()
        for crel in (0, 1):
            self.passed(g, crel).wait_send()


def experts_kernel(
    normed, middle, tile, gate_g, up_g, eg, eu, ed, sg, su, sd,
    out,
    tiles, tok, sel, wts, sb, xr, yb, yr, rl0, rl1, pz, zr, gu, dn, hid, sgv, suv, sdv, nall, spart, sin,
    tile_send, tile_recv, ag_send, ag_recv, zs_send, zs_recv,
    x_send, x_recv, xr_send, xr_recv, w_send, w_recv, s_send, s_recv, ld,
):
    s, y, z, x, c = position()
    zup, zdown = (sp_of(z + 1, x, c), y), (sp_of(z - 1, x, c), y)
    zs = [(sp_of(z + k, x, c), y) for k in range(1, 8)]
    xs = [(sp_of(z, x + d, core), y) for d in (1, 3) for core in (c, 1 - c)]
    sib = (s + 1 - 2 * c, y)
    others = [(s, lax.rem(y + k, 4)) for k in (1, 2, 3)]
    greet(zs + xs + [sib] + others)

    loads = [
        pltpu.make_async_copy(tile, tiles.at[z], ld.at[0]),
        pltpu.make_async_copy(normed, tok.at[pl.ds(0, 32)], ld.at[1]),
        pltpu.make_async_copy(normed, nall.at[y], ld.at[2]),
        pltpu.make_async_copy(eg, gu.at[y, :, pl.ds(0, 128)], ld.at[3]),
        pltpu.make_async_copy(eu, gu.at[y, :, pl.ds(128, 128)], ld.at[4]),
        pltpu.make_async_copy(ed, dn.at[pl.ds(y * 128, 128)], ld.at[5]),
        pltpu.make_async_copy(sg, sgv, ld.at[6]),
        pltpu.make_async_copy(su, suv, ld.at[7]),
        pltpu.make_async_copy(sd, sdv, ld.at[8]),
    ]
    for k in (1, 2, 3):
        j = lax.rem(y + k, 4)
        loads.append(pltpu.make_async_copy(gate_g.at[j], gu.at[j, :, pl.ds(0, 128)], ld.at[7 + 2 * k]))
        loads.append(
            pltpu.make_async_copy(up_g.at[j], gu.at[j, pl.ds(0, 2048), pl.ds(128, 128)], ld.at[8 + 2 * k])
        )
    for copy in loads:
        copy.start()

    loads[0].wait()

    def tile_copy(k):
        return pltpu.make_async_remote_copy(
            src_ref=tiles.at[z],
            dst_ref=tiles.at[z],
            send_sem=tile_send.at[k - 1],
            recv_sem=tile_recv.at[k - 1],
            device_id=zs[k - 1],
            device_id_type=MESH,
        )

    for k in range(1, 8):
        tile_copy(k).start()

    def ag(way, k, h):
        sign = -1 if way == 0 else 1
        return pltpu.make_async_remote_copy(
            src_ref=tok.at[pl.ds(32 * AT[sign * (k - 1)] + 16 * h, 16)],
            dst_ref=tok.at[pl.ds(32 * AT[sign * k] + 16 * h, 16)],
            send_sem=ag_send.at[way, k - 1, h],
            recv_sem=ag_recv.at[way, k - 1, h],
            device_id=zup if way == 0 else zdown,
            device_id_type=MESH,
        )

    def hops(way, k):
        return (0, 1) if k < 4 else ((0,) if way == 0 else (1,))

    loads[1].wait()
    for h in (0, 1):
        for way in (0, 1):
            ag(way, 1, h).start()

    ups = YGather(
        [eu.at[pl.ds(2048 + h * 1024, 1024)] for h in (0, 1)],
        lambda j, h: gu.at[j, pl.ds(2048 + h * 1024, 1024), pl.ds(128, 128)],
        w_send.at[0], w_recv.at[0],
    )
    downs = YGather(
        [ed.at[pl.ds(h * 64, 64)] for h in (0, 1)],
        lambda j, h: dn.at[pl.ds(j * 128 + h * 64, 64)],
        w_send.at[1], w_recv.at[1],
    )
    ups.start()
    downs.start()

    for k in range(1, 8):
        tile_copy(k).wait_recv()

    lane = lax.broadcasted_iota(jnp.int32, (4, 128), 1) // 32
    row16 = lax.broadcasted_iota(jnp.int32, (16, 128), 0)
    lane16 = lax.broadcasted_iota(jnp.int32, (16, 128), 1) // 32
    r0 = lax.broadcasted_iota(jnp.int32, (128, 128), 0)
    r1 = lax.broadcasted_iota(jnp.int32, (128, 128), 1)
    earlier = jnp.where((r0 // 32 == r1 // 32) & (r0 < r1), 1.0, 0.0).astype(BF)

    def picks(g):
        names = jnp.zeros((4, 128), F32)
        scale = jnp.zeros((4, 128), F32)
        for i in range(4):
            src = lax.rem(z + REL[g * 4 + i] + 8, 8)
            names = jnp.where(lane == i, tiles[src, 0:4], names)
            scale = jnp.where(lane == i, tiles[src, 4:8], scale)
        occ, wrow = [], []
        for d in range(4):
            for crel in (0, 1):
                core = c + crel - 2 * c * crel
                expert = (z * 8 + lax.rem(x + d, 4) * 2 + core).astype(F32)
                hit = jnp.where(names == expert, 1.0, 0.0)
                occ.append(jnp.sum(hit, axis=0, keepdims=True))
                wrow.append(jnp.sum(hit * scale, axis=0, keepdims=True))
        occupied = jnp.concatenate(occ, axis=0)
        rank = jnp.dot(occupied.astype(BF), earlier, preferred_element_type=F32)
        weighted = []
        for m in range(8):
            chosen = (
                (lane16 == row16 // 4)
                & (rank[m : m + 1] == (row16 % 4).astype(F32))
                & (occ[m] > 0.5)
            )
            sel[g, pl.ds(16 * m, 16)] = jnp.where(chosen, 1.0, 0.0).astype(BF)
            weighted.append(jnp.where(chosen, wrow[m], 0.0))
        full = jnp.concatenate(weighted, axis=0).T
        high = full.astype(BF)
        wts[g, 0] = high
        wts[g, 1] = (full - high.astype(F32)).astype(BF)

    fwd = Exchange(sb, xr, rl0, x_send.at[0], x_recv.at[0], xr_send.at[0], xr_recv.at[0])
    back = Exchange(yb, yr, rl1, x_send.at[1], x_recv.at[1], xr_send.at[1], xr_recv.at[1])

    def select(g):
        for n in range(4):
            cols = slice(n * 1024, (n + 1) * 1024)
            sb[g * 128 : (g + 1) * 128, cols] = jnp.dot(
                sel[g], tok[g * 128 : (g + 1) * 128, cols], preferred_element_type=F32
            ).astype(BF)
        fwd.start(g)

    picks(0)
    picks(1)
    for k in range(1, 5):
        for h in (0, 1):
            for way in (0, 1):
                if h in hops(way, k):
                    ag(way, k, h).wait_recv()
                    if k < 4 and h in hops(way, k + 1):
                        ag(way, k + 1, h).start()
        if k == 2:
            select(0)
            ups.relay()
        if k == 3:
            fwd.relay(0)
    select(1)
    downs.relay()

    def rows(k):
        return pltpu.make_async_remote_copy(
            src_ref=nall.at[y],
            dst_ref=nall.at[y],
            send_sem=s_send.at[0, k - 1],
            recv_sem=s_recv.at[0, k - 1],
            device_id=others[k - 1],
            device_id_type=MESH,
        )

    loads[2].wait()
    for k in (2, 1, 3):
        rows(k).start()

    fwd.relay(1)
    for copy in loads[3:]:
        copy.wait()
    ups.finish()
    fwd.arrived(0)
    fwd.arrived(1)

    @pl.loop(0, 4)
    def _(j):
        both = jnp.dot(xr[...], gu[j], preferred_element_type=F32)
        g, u = both[:, 0:128], both[:, 128:256]
        hid[:, pl.ds(pl.multiple_of(j * 128, 128), 128)] = (g / (1.0 + jnp.exp(-g)) * u).astype(BF)

    downs.finish()

    @pl.loop(0, 4)
    def _(n):
        cols = pl.ds(pl.multiple_of(n * 1024, 1024), 1024)
        yb[:, cols] = jnp.dot(hid[...], dn[:, cols], preferred_element_type=F32).astype(BF)

    back.start(1)
    back.start(0)

    for k in (2, 1, 3):
        rows(k).wait_recv()
    everyone = nall[...].reshape(128, D)
    g = jnp.dot(everyone, sgv[...], preferred_element_type=F32)
    u = jnp.dot(everyone, suv[...], preferred_element_type=F32)
    shared_hidden = (g / (1.0 + jnp.exp(-g)) * u).astype(BF)
    for n in range(4):
        cols = slice(n * 1024, (n + 1) * 1024)
        spart[:, :, cols] = (
            jnp.dot(shared_hidden, sdv[:, cols], preferred_element_type=F32).astype(BF).reshape(4, 32, 1024)
        )

    def share(k):
        return pltpu.make_async_remote_copy(
            src_ref=spart.at[lax.rem(y + k, 4)],
            dst_ref=sin.at[k - 1],
            send_sem=s_send.at[1, k - 1],
            recv_sem=s_recv.at[1, k - 1],
            device_id=others[k - 1],
            device_id_type=MESH,
        )

    for k in (2, 1, 3):
        share(k).start()

    back.relay(1)
    back.relay(0)

    def combine(g):
        back.arrived(g)
        for n in range(4):
            cols = slice(n * 1024, (n + 1) * 1024)
            pz[g * 128 : (g + 1) * 128, cols] = (
                jnp.dot(wts[g, 0], yr[g * 128 : (g + 1) * 128, cols], preferred_element_type=F32)
                + jnp.dot(wts[g, 1], yr[g * 128 : (g + 1) * 128, cols], preferred_element_type=F32)
            ).astype(BF)

    def zsum(way, m, h):
        sign = 1 if way == 0 else -1
        return pltpu.make_async_remote_copy(
            src_ref=pz.at[pl.ds(32 * AT[sign * m] + 16 * h, 16)],
            dst_ref=zr.at[way, m - 1, pl.ds(16 * h, 16)],
            send_sem=zs_send.at[way, m - 1, h],
            recv_sem=zs_recv.at[way, m - 1, h],
            device_id=zup if way == 0 else zdown,
            device_id_type=MESH,
        )

    def add_and_send(m):
        for h in (0, 1):
            for way in (0, 1):
                if h not in hops(way, m):
                    continue
                sign = 1 if way == 0 else -1
                if m < 4 and h in hops(way, m + 1):
                    zsum(way, m + 1, h).wait_recv()
                    at = slice(32 * AT[sign * m] + 16 * h, 32 * AT[sign * m] + 16 * h + 16)
                    pz[at] = (
                        pz[at].astype(F32) + zr[way, m, 16 * h : 16 * h + 16].astype(F32)
                    ).astype(BF)
                zsum(way, m, h).start()

    combine(1)
    add_and_send(4)
    add_and_send(3)
    combine(0)
    add_and_send(2)
    add_and_send(1)

    for k in (2, 1, 3):
        share(k).wait_recv()
    for h in (0, 1):
        for way in (0, 1):
            zsum(way, 1, h).wait_recv()
    for n in range(4):
        cols = slice(n * 1024, (n + 1) * 1024)
        total = middle[:, cols] + spart[y, :, cols].astype(F32)
        for k in range(3):
            total = total + sin[k, :, cols].astype(F32)
        total = total + pz[0:32, cols].astype(F32)
        total = total + zr[0, 0, :, cols].astype(F32) + zr[1, 0, :, cols].astype(F32)
        out[:, cols] = total.astype(BF)

    for k in range(1, 8):
        tile_copy(k).wait_send()
    for k in range(1, 5):
        for way in (0, 1):
            for h in hops(way, k):
                ag(way, k, h).wait_send()
                zsum(way, k, h).wait_send()
    for g in (0, 1):
        fwd.sent(g)
        back.sent(g)
    for k in (1, 2, 3):
        rows(k).wait_send()
        share(k).wait_send()


def experts(normed, middle, tile, gate_g, up_g, eg, eu, ed, sg, su, sd):
    vmem = pl.BlockSpec(memory_space=pltpu.VMEM)
    anym = pl.BlockSpec(memory_space=pl.ANY)
    dma = pltpu.SemaphoreType.DMA
    return pl.pallas_call(
        experts_kernel,
        name="experts",
        out_shape=jax.ShapeDtypeStruct((32, D), BF),
        in_specs=[anym, vmem] + [anym] * 9,
        out_specs=vmem,
        scratch_shapes=[
            pltpu.VMEM((8, 8, 128), F32),
            pltpu.VMEM((256, D), BF),
            pltpu.VMEM((2, 128, 128), BF),
            pltpu.VMEM((2, 2, 128, 128), BF),
            pltpu.VMEM((256, D), BF),
            pltpu.VMEM((256, D), BF),
            pltpu.VMEM((256, D), BF),
            pltpu.VMEM((256, D), BF),
            pltpu.VMEM((2, 2, 16, D), BF),
            pltpu.VMEM((2, 2, 16, D), BF),
            pltpu.VMEM((256, D), BF),
            pltpu.VMEM((2, 4, 32, D), BF),
            pltpu.VMEM((4, 4096, 256), BF),
            pltpu.VMEM((512, D), BF),
            pltpu.VMEM((256, 512), BF),
            pltpu.VMEM((4096, 128), BF),
            pltpu.VMEM((4096, 128), BF),
            pltpu.VMEM((128, D), BF),
            pltpu.VMEM((4, 32, D), BF),
            pltpu.VMEM((4, 32, D), BF),
            pltpu.VMEM((3, 32, D), BF),
            dma((7,)), dma((7,)),
            dma((2, 4, 2)), dma((2, 4, 2)),
            dma((2, 4, 2)), dma((2, 4, 2)),
            dma((2, 2, 8)), dma((2, 2, 8)),
            dma((2, 2, 2)), dma((2, 2, 2)),
            dma((2, 6)), dma((2, 6)),
            dma((2, 3)), dma((2, 3)),
            dma((15,)),
        ],
        compiler_params=pltpu.CompilerParams(
            collective_id=1, has_side_effects=True, vmem_limit_bytes=60 * 1024 * 1024
        ),
    )(normed, middle, tile, gate_g, up_g, eg, eu, ed, sg, su, sd)


def body(
    full_queries, full_keys, full_values, full_gates, half_queries, half_keys, half_values,
    half_gates, residual, full_output, half_output, norm_gain, routes, route_weights,
    expert_gate, expert_up, expert_down, shared_gate, shared_up, shared_down,
):
    quarter = lax.axis_index("tp")
    own = lambda a: lax.dynamic_slice_in_dim(a.T.astype(F32), quarter * 32, 32, 1)
    tile = jnp.tile(jnp.concatenate([own(routes), own(route_weights)], axis=0), (1, 4))
    middle, normed, gates, ups = attend(
        full_queries, full_keys, full_values, full_gates.T, half_queries, half_keys, half_values,
        half_gates.T, residual, full_output, half_output, norm_gain.reshape(1, D),
        expert_gate[0], expert_up[0],
    )
    return experts(
        normed, middle, tile, gates, ups, expert_gate[0], expert_up[0], expert_down[0],
        shared_gate, shared_up, shared_down,
    )


def solution(mesh):
    return jax.shard_map(
        body,
        mesh=mesh,
        in_specs=(
            P("sp", "tp"), P("sp", "tp"), P("sp", "tp"), P(None, "tp"),
            P("sp", "tp"), P("sp", "tp"), P("sp", "tp"), P(None, "tp"),
            P("sp", None), P("tp", None), P("tp", None), P(), P("sp", None), P("sp", None),
            P("sp", None, "tp"), P("sp", None, "tp"), P("sp", "tp", None),
            P(None, "tp"), P(None, "tp"), P("tp", None),
        ),
        out_specs=P(("sp", "tp"), None),
        check_vma=False,
    )
```

```python
import functools
import heapq

import jax
import jax.numpy as jnp
from jax import lax
from jax.experimental import pallas as pl
from jax.experimental.pallas import tpu as pltpu
from jax.sharding import PartitionSpec as P

D = 4096
LOG2E = 1.4426950408889634
BF = jnp.bfloat16
F32 = jnp.float32
MESH = pl.DeviceIdType.MESH
NEG = -1e30


def kv_schedule():
    def onward(part, dz, dx, link):
        out = []
        if part == 0:
            if link in ("own", "z+", "z-"):
                if link == "own":
                    out += ["z+", "z-"]
                elif link == "z+" and dz < 4:
                    out.append("z+")
                elif link == "z-" and dz > -3:
                    out.append("z-")
                out += ["x+", "x-"]
            elif link == "x+" and dx == 1 and dz % 2 == 0:
                out.append("x+")
            elif link == "x-" and dx == -1 and dz % 2 == 1:
                out.append("x-")
        else:
            if link in ("own", "x+", "x-"):
                if link == "own":
                    out += ["x+", "x-"]
                elif link == "x+" and dx == 1:
                    out.append("x+")
                out += ["z+", "z-"]
            elif link == "z+" and (dz < 3 or (dz == 3 and dx in (0, 1))):
                out.append("z+")
            elif link == "z-" and dz < 0 and (dz > -3 or dx not in (0, 1)):
                out.append("z-")
        return out

    free = {"z+": 0.0, "z-": 0.0, "x+": 0.0, "x-": 0.0}
    heap, events, count = [], [], 0

    def send(now, part, dz, dx, link):
        nonlocal count
        start = max(now, free[link])
        free[link] = start + 1.4
        step = 1 if link[1] == "+" else -1
        ndz, ndx = (dz + step, dx) if link[0] == "z" else (dz, dx + step)
        if link[0] == "z" and ndz == -4:
            ndz = 4
        if link[0] == "x" and ndx == -2:
            ndx = 2
        heapq.heappush(heap, (free[link] + 1.5, count, part, ndz, ndx, link))
        count += 1

    for part in (1, 0):
        for link in onward(part, 0, 0, "own"):
            send(0.0, part, 0, 0, link)
    seen = set()
    while heap:
        now, _, part, dz, dx, link = heapq.heappop(heap)
        assert (part, dz, dx) not in seen
        seen.add((part, dz, dx))
        links = onward(part, dz, dx, link)
        events.append((part, dz, dx, tuple(links)))
        for out in links:
            send(now, part, dz, dx, out)
    assert len(events) == 62
    own = [(part, 0, 0, tuple(onward(part, 0, 0, "own"))) for part in (1, 0)]
    return own, events


def position():
    s = lax.axis_index("sp")
    y = lax.axis_index("tp")
    z, x, c = s // 8, (s // 2) % 4, s % 2
    return s, y, z, x, c


def sp_of(z, x, c):
    return lax.rem(z + 8, 8) * 8 + lax.rem(x + 4, 4) * 2 + c


def greet(peers):
    barrier = pltpu.get_barrier_semaphore()
    for peer in peers:
        pl.semaphore_signal(barrier, inc=1, device_id=peer, device_id_type=MESH)
    pl.semaphore_wait(barrier, len(peers))


class YGather:
    def __init__(self, src, dst, send_sem, recv_sem):
        s, y, *_ = position()
        self.src, self.dst, self.send, self.recv = src, dst, send_sem, recv_sem
        self.y = y
        self.up = (s, lax.rem(y + 1, 4))
        self.down = (s, lax.rem(y + 3, 4))

    def copy(self, half, src_y, way, hop):
        slot = way * 3 + (half if hop == 0 else 2)
        return pltpu.make_async_remote_copy(
            src_ref=self.src[half] if hop == 0 else self.dst(src_y, half),
            dst_ref=self.dst(src_y, half),
            send_sem=self.send.at[slot],
            recv_sem=self.recv.at[slot],
            device_id=self.up if way == 0 else self.down,
            device_id_type=MESH,
        )

    def start(self):
        self.copy(0, self.y, 0, 0).start()
        self.copy(1, self.y, 1, 0).start()
        self.copy(1, self.y, 0, 0).start()
        self.copy(0, self.y, 1, 0).start()

    def relay(self):
        below, above = lax.rem(self.y + 3, 4), lax.rem(self.y + 1, 4)
        self.copy(0, below, 0, 0).wait_recv()
        self.copy(0, below, 0, 1).start()
        self.copy(1, above, 1, 0).wait_recv()
        self.copy(1, above, 1, 1).start()

    def finish(self):
        below, above, far = lax.rem(self.y + 3, 4), lax.rem(self.y + 1, 4), lax.rem(self.y + 2, 4)
        self.copy(1, below, 0, 0).wait_recv()
        self.copy(0, above, 1, 0).wait_recv()
        self.copy(0, far, 0, 1).wait_recv()
        self.copy(1, far, 1, 1).wait_recv()
        self.sent()

    def sent(self):
        below, above = lax.rem(self.y + 3, 4), lax.rem(self.y + 1, 4)
        for half in (0, 1):
            for way in (0, 1):
                self.copy(half, self.y, way, 0).wait_send()
        self.copy(0, below, 0, 1).wait_send()
        self.copy(1, above, 1, 1).wait_send()


class YReduce:
    def __init__(self, part, far, near, send_sem, recv_sem, width):
        s, y, *_ = position()
        self.part, self.far, self.near = part, far, near
        self.send, self.recv, self.width = send_sem, recv_sem, width
        self.next = (lax.rem(y + 1, 4), lax.rem(y + 3, 4))
        self.across = lax.rem(y + 2, 4)
        self.dev = [(s, self.next[0]), (s, self.next[1])]

    def copy(self, n, way, kind):
        cols = pl.ds(n * self.width, self.width)
        low, high = pl.ds(0, 16), pl.ds(16, 16)
        merged, plain = (high, low) if way == 0 else (low, high)
        if kind == 0:
            src, dst = self.part.at[self.across, merged, cols], self.far.at[way, :, cols]
        else:
            rows = plain if kind == 1 else merged
            src, dst = self.part.at[self.next[way], rows, cols], self.near.at[way, rows, cols]
        return pltpu.make_async_remote_copy(
            src_ref=src,
            dst_ref=dst,
            send_sem=self.send.at[n, way, kind],
            recv_sem=self.recv.at[n, way, kind],
            device_id=self.dev[way],
            device_id_type=MESH,
        )

    def start(self, n):
        for kind in (0, 1):
            for way in (0, 1):
                self.copy(n, way, kind).start()

    def relay(self, n):
        cols = pl.ds(n * self.width, self.width)
        for way in (0, 1):
            rows = pl.ds(16, 16) if way == 0 else pl.ds(0, 16)
            self.copy(n, way, 0).wait_recv()
            self.part[self.next[way], rows, cols] = (
                self.part[self.next[way], rows, cols].astype(F32) + self.far[way, :, cols].astype(F32)
            ).astype(BF)
            self.copy(n, way, 2).start()

    def arrived(self, n):
        for kind in (1, 2):
            for way in (0, 1):
                self.copy(n, way, kind).wait_recv()

    def sent(self, n):
        for kind in (0, 1, 2):
            for way in (0, 1):
                self.copy(n, way, kind).wait_send()


def attend_kernel(
    fq, fk, fv, gf, hq, hk, hv, gh, res, wf, wh, gain, eg, eu,
    mid_out, norm_out, gate_out, up_out,
    kva, kvb, qs, acc, mx, tot, att, part, far, near, resv,
    own_sem, kv_send, kv_recv, w_send, w_recv, rs_send, rs_recv, res_sem,
):
    s, y, z, x, c = position()
    sib = (s + 1 - 2 * c, y)
    to = {
        "z+": (sp_of(z + 1, x, c), y),
        "z-": (sp_of(z - 1, x, c), y),
        "x+": (sp_of(z, x + 1, c), y),
        "x-": (sp_of(z, x - 1, c), y),
    }
    others = [(s, lax.rem(y + k, 4)) for k in (2, 1, 3)]
    greet(list(to.values()) + [sib] + others)

    kv = (kva, kvb)
    pieces = [
        (fk, kva, 0), (fv, kva, 128), (hk, kvb, 0), (hv, kvb, 128),
    ]
    own = [
        pltpu.make_async_copy(src, dst.at[s, :, pl.ds(at, 128)], own_sem.at[i])
        for i, (src, dst, at) in enumerate(pieces)
    ]
    for copy in own:
        copy.start()
    res_copy = pltpu.make_async_copy(res.at[pl.ds(y * 32, 32)], resv, res_sem)
    res_copy.start()

    def hop(prt, idx, device):
        return pltpu.make_async_remote_copy(
            src_ref=kv[prt].at[idx],
            dst_ref=kv[prt].at[idx],
            send_sem=kv_send.at[prt],
            recv_sem=kv_recv.at[prt, idx],
            device_id=device,
            device_id_type=MESH,
        )

    own_events, events = kv_schedule()
    for prt, _, _, links in own_events:
        own[2 * prt].wait()
        own[2 * prt + 1].wait()
        for link in links:
            hop(prt, s, to[link]).start()
        hop(prt, s, sib).start()

    half_rows = 2048
    gates = YGather(
        [eg.at[pl.ds(h * half_rows, half_rows)] for h in (0, 1)],
        lambda j, h: gate_out.at[j, pl.ds(h * half_rows, half_rows)],
        w_send.at[0], w_recv.at[0],
    )
    ups = YGather(
        [eu.at[pl.ds(h * 1024, 1024)] for h in (0, 1)],
        lambda j, h: up_out.at[j, pl.ds(h * 1024, 1024)],
        w_send.at[1], w_recv.at[1],
    )
    gates.start()
    ups.start()

    lane = lax.broadcasted_iota(jnp.int32, (128, 128), 1)
    qs[0, 0:128] = fq[:, 0:128]
    qs[0, 128:256] = fq[:, 128:256]
    h01 = hq[:, 0:128].astype(F32)
    h23 = hq[:, 128:256].astype(F32)
    qs[1, 0:128] = jnp.where(lane < 64, h01, 0.0).astype(BF)
    qs[1, 128:256] = jnp.where(lane < 64, pltpu.roll(h01, 64, 1), 0.0).astype(BF)
    qs[2, 0:128] = jnp.where(lane >= 64, pltpu.roll(h23, 64, 1), 0.0).astype(BF)
    qs[2, 128:256] = jnp.where(lane >= 64, h23, 0.0).astype(BF)
    acc[...] = jnp.zeros_like(acc)
    tot[...] = jnp.zeros_like(tot)
    mx[...] = jnp.full_like(mx, NEG)

    for i, (prt, dz, dx, links) in enumerate(events):
        idx = sp_of(z - dz, x - dx, c)
        hop(prt, idx, sib).wait_recv()
        for link in links:
            hop(prt, idx, to[link]).start()
        hop(prt, idx, sib).start()
        if i == 30:
            gates.relay()
    ups.relay()

    @pl.loop(0, 32)
    def _(i):
        idx = 2 * i + 1 - c
        for prt in (0, 1):
            hop(prt, idx, sib).wait_recv()

    row0 = s * 128
    gfirst = gf[:, pl.ds(pl.multiple_of(row0, 128), 128)][:, 0:1]
    hfirst = gh[:, pl.ds(pl.multiple_of(row0, 128), 128)][:, 0:1]

    def chunk(at, masked):
        key0 = pl.multiple_of(at * 1024, 1024)
        fg = (gf[:, pl.ds(key0, 1024)] - gfirst) * LOG2E
        hg = (gh[:, pl.ds(key0, 1024)] - hfirst) * LOG2E
        if masked:
            qpos = (s % 8) * 128 + lax.broadcasted_iota(jnp.int32, (128, 1024), 0)
            kpos = lax.broadcasted_iota(jnp.int32, (128, 1024), 1)
            allowed = kpos <= qpos
        for g in range(3):
            store = kva if g == 0 else kvb
            k = store[pl.ds(at * 8, 8), :, 0:128].reshape(1024, 128)
            v = store[pl.ds(at * 8, 8), :, 128:256].reshape(1024, 128)
            scale = (128 ** -0.5 if g == 0 else 0.125) * LOG2E
            scores = lax.dot_general(
                qs[g], k, (((1,), (1,)), ((), ())), preferred_element_type=F32
            )
            for r in (0, 1):
                row = fg[r : r + 1] if g == 0 else hg[2 * (g - 1) + r : 2 * (g - 1) + r + 1]
                t = scores[r * 128 : (r + 1) * 128] * scale - row
                if masked:
                    t = jnp.where(allowed, t, NEG)
                old = mx[g, pl.ds(r * 128, 128)]
                new = jnp.maximum(old, jnp.max(t, axis=1, keepdims=True))
                p = jnp.exp2(t - new[:, 0:1])
                shrink = jnp.exp2(old - new)
                mx[g, pl.ds(r * 128, 128)] = new
                tot[g, pl.ds(r * 128, 128)] = (
                    tot[g, pl.ds(r * 128, 128)] * shrink + jnp.sum(p, axis=1, keepdims=True)
                )
                acc[g, pl.ds(r * 128, 128)] = acc[g, pl.ds(r * 128, 128)] * shrink + jnp.dot(
                    p.astype(BF), v, preferred_element_type=F32
                )

    @pl.loop(0, z)
    def _(at):
        chunk(at, False)

    chunk(z, True)

    outs = [
        [acc[g, r * 128 : (r + 1) * 128] / tot[g, r * 128 : (r + 1) * 128] for r in (0, 1)]
        for g in range(3)
    ]
    att[:, 0:128] = outs[0][0].astype(BF)
    att[:, 128:256] = outs[0][1].astype(BF)
    att[:, 256:384] = jnp.where(lane < 64, outs[1][0], pltpu.roll(outs[1][1], 64, 1)).astype(BF)
    att[:, 384:512] = jnp.where(lane < 64, pltpu.roll(outs[2][0], 64, 1), outs[2][1]).astype(BF)

    gates.finish()
    ups.finish()

    sums = YReduce(part, far, near, rs_send, rs_recv, 1024)
    for n in range(4):
        cols = slice(n * 1024, (n + 1) * 1024)
        product = jnp.dot(att[:, 0:256], wf[:, cols], preferred_element_type=F32) + jnp.dot(
            att[:, 256:512], wh[:, cols], preferred_element_type=F32
        )
        part[:, :, cols] = product.astype(BF).reshape(4, 32, 1024)
        sums.start(n)
    for n in range(4):
        sums.relay(n)
    res_copy.wait()
    square = jnp.zeros((32, 1), F32)
    for n in range(4):
        cols = slice(n * 1024, (n + 1) * 1024)
        total = resv[:, cols].astype(F32) + part[y, :, cols].astype(F32)
        sums.arrived(n)
        total = total + near[0, :, cols].astype(F32) + near[1, :, cols].astype(F32)
        mid_out[:, cols] = total
        square = square + jnp.sum(total * total, axis=1, keepdims=True)
    factor = lax.rsqrt(square * (1.0 / D) + 1e-06)
    norm_out[...] = (mid_out[...] * factor * gain[...]).astype(BF)

    for n in range(4):
        sums.sent(n)
    for prt in (0, 1):
        everything = kv[prt].at[pl.ds(0, 63)]
        pltpu.make_async_copy(everything, everything, kv_send.at[prt]).wait()


def attend(fq, fk, fv, gf, hq, hk, hv, gh, res, wf, wh, gain, eg, eu):
    vmem = pl.BlockSpec(memory_space=pltpu.VMEM)
    anym = pl.BlockSpec(memory_space=pl.ANY)
    return pl.pallas_call(
        attend_kernel,
        name="attend",
        out_shape=(
            jax.ShapeDtypeStruct((32, D), F32),
            jax.ShapeDtypeStruct((32, D), BF),
            jax.ShapeDtypeStruct((4, 4096, 128), BF),
            jax.ShapeDtypeStruct((4, 2048, 128), BF),
        ),
        in_specs=[vmem, anym, anym, vmem, vmem, anym, anym, vmem, anym, vmem, vmem, vmem, anym, anym],
        out_specs=[vmem, vmem, anym, anym],
        scratch_shapes=[
            pltpu.VMEM((64, 128, 256), BF),
            pltpu.VMEM((64, 128, 256), BF),
            pltpu.VMEM((3, 256, 128), BF),
            pltpu.VMEM((3, 256, 128), F32),
            pltpu.VMEM((3, 256, 128), F32),
            pltpu.VMEM((3, 256, 128), F32),
            pltpu.VMEM((128, 512), BF),
            pltpu.VMEM((4, 32, D), BF),
            pltpu.VMEM((2, 16, D), BF),
            pltpu.VMEM((2, 32, D), BF),
            pltpu.VMEM((32, D), BF),
            pltpu.SemaphoreType.DMA((4,)),
            pltpu.SemaphoreType.DMA((2,)),
            pltpu.SemaphoreType.DMA((2, 64)),
            pltpu.SemaphoreType.DMA((2, 6)),
            pltpu.SemaphoreType.DMA((2, 6)),
            pltpu.SemaphoreType.DMA((4, 2, 3)),
            pltpu.SemaphoreType.DMA((4, 2, 3)),
            pltpu.SemaphoreType.DMA,
        ],
        compiler_params=pltpu.CompilerParams(
            collective_id=0, has_side_effects=True, vmem_limit_bytes=56 * 1024 * 1024
        ),
    )(fq, fk, fv, gf, hq, hk, hv, gh, res, wf, wh, gain, eg, eu)


REL = (0, -1, 1, -2, 2, -3, 3, 4)
AT = {r: i for i, r in enumerate(REL)}
AT[-4] = AT[4]


class Exchange:
    def __init__(self, src, dst, relay, send, recv, rsend, rrecv, width):
        self.width = width
        self.src, self.dst, self.rl = src, dst, relay
        self.send, self.recv, self.rsend, self.rrecv = send, recv, rsend, rrecv
        s, y, z, x, c = position()
        self.core = (c, 1 - c)
        self.dev = lambda d, core: (sp_of(z, x + d, core), y)

    def direct(self, g, d, crel, n=0):
        cols = pl.ds(n * self.width, self.width)
        m = d * 2 + crel
        slot = ((4 - d) % 4) * 2 + crel
        if d == 2:
            return pltpu.make_async_remote_copy(
                src_ref=self.src.at[pl.ds(g * 128 + 16 * m, 16), cols],
                dst_ref=self.rl.at[g, crel, :, cols],
                send_sem=self.send.at[n, g, m],
                recv_sem=self.rrecv.at[n, g, crel],
                device_id=self.dev(1 if crel == 0 else 3, self.core[0]),
                device_id_type=MESH,
            )
        return pltpu.make_async_remote_copy(
            src_ref=self.src.at[pl.ds(g * 128 + 16 * m, 16), cols],
            dst_ref=self.dst.at[pl.ds(g * 128 + 16 * slot, 16), cols],
            send_sem=self.send.at[n, g, m],
            recv_sem=self.recv.at[n, g, slot],
            device_id=self.dev(d, self.core[crel]),
            device_id_type=MESH,
        )

    def passed(self, g, crel, n=0):
        cols = pl.ds(n * self.width, self.width)
        slot = 4 + crel
        return pltpu.make_async_remote_copy(
            src_ref=self.rl.at[g, crel, :, cols],
            dst_ref=self.dst.at[pl.ds(g * 128 + 16 * slot, 16), cols],
            send_sem=self.rsend.at[n, g, crel],
            recv_sem=self.recv.at[n, g, slot],
            device_id=self.dev(1 if crel == 0 else 3, self.core[crel]),
            device_id_type=MESH,
        )

    def local(self, g, n=0):
        cols = pl.ds(n * self.width, self.width)
        return pltpu.make_async_copy(
            self.src.at[pl.ds(g * 128, 16), cols],
            self.dst.at[pl.ds(g * 128, 16), cols],
            self.recv.at[n, g, 0],
        )

    def start(self, g, n=0):
        for d, crel in ((2, 0), (2, 1), (1, 0), (3, 0), (1, 1), (3, 1), (0, 1)):
            self.direct(g, d, crel, n).start()
        self.local(g, n).start()

    def relay(self, g, n=0):
        for crel in (0, 1):
            self.direct(g, 2, crel, n).wait_recv()
            self.passed(g, crel, n).start()

    def arrived(self, g, n=0):
        self.local(g, n).wait()
        for d, crel in ((0, 1), (1, 0), (3, 0), (1, 1), (3, 1)):
            self.direct(g, d, crel, n).wait_recv()
        for crel in (0, 1):
            self.passed(g, crel, n).wait_recv()

    def sent(self, g, n=0):
        for d, crel in ((2, 0), (2, 1), (1, 0), (3, 0), (1, 1), (3, 1), (0, 1)):
            self.direct(g, d, crel, n).wait_send()
        for crel in (0, 1):
            self.passed(g, crel, n).wait_send()


def experts_kernel(
    normed, middle, tile, gate_g, up_g, eg, eu, ed, sg, su, sd,
    out,
    tiles, tok, sel, wts, sb, xr, yb, yr, rl0, rl1, pz, zr, gu, dn, hid, sgv, suv, sdv, nall, spart, sfar, snear,
    tile_send, tile_recv, ag_send, ag_recv, zs_send, zs_recv,
    x_send, x_recv, xr_send, xr_recv, w_send, w_recv, g_send, g_recv, s_send, s_recv, ld,
):
    s, y, z, x, c = position()
    zup, zdown = (sp_of(z + 1, x, c), y), (sp_of(z - 1, x, c), y)
    zs = [(sp_of(z + k, x, c), y) for k in range(1, 8)]
    xs = [(sp_of(z, x + d, core), y) for d in (1, 3) for core in (c, 1 - c)]
    sib = (s + 1 - 2 * c, y)
    others = [(s, lax.rem(y + k, 4)) for k in (1, 2, 3)]
    greet(zs + xs + [sib] + others)

    loads = [
        pltpu.make_async_copy(tile, tiles.at[z], ld.at[0]),
        pltpu.make_async_copy(normed, tok.at[pl.ds(0, 32)], ld.at[1]),
        pltpu.make_async_copy(normed, nall.at[y], ld.at[2]),
        pltpu.make_async_copy(eg, gu.at[y, :, pl.ds(0, 128)], ld.at[3]),
        pltpu.make_async_copy(eu, gu.at[y, :, pl.ds(128, 128)], ld.at[4]),
        pltpu.make_async_copy(ed, dn.at[pl.ds(y * 128, 128)], ld.at[5]),
        pltpu.make_async_copy(sg, sgv, ld.at[6]),
        pltpu.make_async_copy(su, suv, ld.at[7]),
        pltpu.make_async_copy(sd, sdv, ld.at[8]),
    ]
    for k in (1, 2, 3):
        j = lax.rem(y + k, 4)
        loads.append(pltpu.make_async_copy(gate_g.at[j], gu.at[j, :, pl.ds(0, 128)], ld.at[7 + 2 * k]))
        loads.append(
            pltpu.make_async_copy(up_g.at[j], gu.at[j, pl.ds(0, 2048), pl.ds(128, 128)], ld.at[8 + 2 * k])
        )
    for copy in loads:
        copy.start()

    loads[0].wait()

    def tile_copy(k):
        return pltpu.make_async_remote_copy(
            src_ref=tiles.at[z],
            dst_ref=tiles.at[z],
            send_sem=tile_send.at[k - 1],
            recv_sem=tile_recv.at[k - 1],
            device_id=zs[k - 1],
            device_id_type=MESH,
        )

    for k in range(1, 8):
        tile_copy(k).start()

    def ag(way, k, h):
        sign = -1 if way == 0 else 1
        return pltpu.make_async_remote_copy(
            src_ref=tok.at[pl.ds(32 * AT[sign * (k - 1)] + 16 * h, 16)],
            dst_ref=tok.at[pl.ds(32 * AT[sign * k] + 16 * h, 16)],
            send_sem=ag_send.at[way, k - 1, h],
            recv_sem=ag_recv.at[way, k - 1, h],
            device_id=zup if way == 0 else zdown,
            device_id_type=MESH,
        )

    def hops(way, k):
        return (0, 1) if k < 4 else ((0,) if way == 0 else (1,))

    loads[1].wait()
    for h in (0, 1):
        for way in (0, 1):
            ag(way, 1, h).start()

    ups = YGather(
        [eu.at[pl.ds(2048 + h * 1024, 1024)] for h in (0, 1)],
        lambda j, h: gu.at[j, pl.ds(2048 + h * 1024, 1024), pl.ds(128, 128)],
        w_send.at[0], w_recv.at[0],
    )
    def down_chunk(n):
        cols = pl.ds(n * 1024, 1024)
        return YGather(
            [ed.at[pl.ds(h * 64, 64), cols] for h in (0, 1)],
            lambda j, h: dn.at[pl.ds(j * 128 + h * 64, 64), cols],
            w_send.at[1 + n], w_recv.at[1 + n],
        )

    downs = [down_chunk(n) for n in range(4)]
    rows = YGather(
        [normed.at[pl.ds(h * 16, 16)] for h in (0, 1)],
        lambda j, h: nall.at[j, pl.ds(h * 16, 16)],
        g_send, g_recv,
    )
    ups.start()
    downs[0].start()
    downs[1].start()

    for k in range(1, 8):
        tile_copy(k).wait_recv()

    lane = lax.broadcasted_iota(jnp.int32, (4, 128), 1) // 32
    row16 = lax.broadcasted_iota(jnp.int32, (16, 128), 0)
    lane16 = lax.broadcasted_iota(jnp.int32, (16, 128), 1) // 32
    r0 = lax.broadcasted_iota(jnp.int32, (128, 128), 0)
    r1 = lax.broadcasted_iota(jnp.int32, (128, 128), 1)
    earlier = jnp.where((r0 // 32 == r1 // 32) & (r0 < r1), 1.0, 0.0).astype(BF)

    def picks(g):
        names = jnp.zeros((4, 128), F32)
        scale = jnp.zeros((4, 128), F32)
        for i in range(4):
            src = lax.rem(z + REL[g * 4 + i] + 8, 8)
            names = jnp.where(lane == i, tiles[src, 0:4], names)
            scale = jnp.where(lane == i, tiles[src, 4:8], scale)
        occ, wrow = [], []
        for d in range(4):
            for crel in (0, 1):
                core = c + crel - 2 * c * crel
                expert = (z * 8 + lax.rem(x + d, 4) * 2 + core).astype(F32)
                hit = jnp.where(names == expert, 1.0, 0.0)
                occ.append(jnp.sum(hit, axis=0, keepdims=True))
                wrow.append(jnp.sum(hit * scale, axis=0, keepdims=True))
        occupied = jnp.concatenate(occ, axis=0)
        rank = jnp.dot(occupied.astype(BF), earlier, preferred_element_type=F32)
        weighted = []
        for m in range(8):
            chosen = (
                (lane16 == row16 // 4)
                & (rank[m : m + 1] == (row16 % 4).astype(F32))
                & (occ[m] > 0.5)
            )
            sel[g, pl.ds(16 * m, 16)] = jnp.where(chosen, 1.0, 0.0).astype(BF)
            weighted.append(jnp.where(chosen, wrow[m], 0.0))
        full = jnp.concatenate(weighted, axis=0).T
        high = full.astype(BF)
        wts[g, 0] = high
        wts[g, 1] = (full - high.astype(F32)).astype(BF)

    fwd = Exchange(sb, xr, rl0, x_send.at[pl.ds(0, 1)], x_recv.at[pl.ds(0, 1)], xr_send.at[pl.ds(0, 1)], xr_recv.at[pl.ds(0, 1)], D)
    back = Exchange(yb, yr, rl1, x_send.at[pl.ds(1, 4)], x_recv.at[pl.ds(1, 4)], xr_send.at[pl.ds(1, 4)], xr_recv.at[pl.ds(1, 4)], 1024)

    def select(g):
        for n in range(4):
            cols = slice(n * 1024, (n + 1) * 1024)
            sb[g * 128 : (g + 1) * 128, cols] = jnp.dot(
                sel[g], tok[g * 128 : (g + 1) * 128, cols], preferred_element_type=F32
            ).astype(BF)
        fwd.start(g)

    picks(0)
    picks(1)
    for k in range(1, 5):
        for h in (0, 1):
            for way in (0, 1):
                if h in hops(way, k):
                    ag(way, k, h).wait_recv()
                    if k < 4 and h in hops(way, k + 1):
                        ag(way, k + 1, h).start()
        if k == 2:
            select(0)
            ups.relay()
            downs[2].start()
            downs[3].start()
        if k == 3:
            fwd.relay(0)
            downs[0].relay()
    select(1)
    downs[1].relay()

    fwd.relay(1)
    downs[2].relay()
    rows.start()
    for copy in loads[2:]:
        copy.wait()
    ups.finish()
    fwd.arrived(0)
    fwd.arrived(1)

    @pl.loop(0, 4)
    def _(j):
        both = jnp.dot(xr[...], gu[j], preferred_element_type=F32)
        g, u = both[:, 0:128], both[:, 128:256]
        hid[:, pl.ds(pl.multiple_of(j * 128, 128), 128)] = (g / (1.0 + jnp.exp(-g)) * u).astype(BF)

    sums = YReduce(spart, sfar, snear, s_send, s_recv, D)

    def finish_rows(n):
        downs[n].finish()
        cols = slice(n * 1024, (n + 1) * 1024)
        yb[:, cols] = jnp.dot(hid[...], dn[:, cols], preferred_element_type=F32).astype(BF)
        for g in (1, 0):
            back.start(g, n)

    def shared():
        rows.finish()
        everyone = nall[...].reshape(128, D)
        g = jnp.dot(everyone, sgv[...], preferred_element_type=F32)
        u = jnp.dot(everyone, suv[...], preferred_element_type=F32)
        shared_hidden = (g / (1.0 + jnp.exp(-g)) * u).astype(BF)
        for n in range(4):
            cols = slice(n * 1024, (n + 1) * 1024)
            spart[:, :, cols] = (
                jnp.dot(shared_hidden, sdv[:, cols], preferred_element_type=F32)
                .astype(BF)
                .reshape(4, 32, 1024)
            )
        sums.start(0)

    def combine(n):
        cols = slice(n * 1024, (n + 1) * 1024)
        for g in (1, 0):
            back.arrived(g, n)
            pz[g * 128 : (g + 1) * 128, cols] = (
                jnp.dot(wts[g, 0], yr[g * 128 : (g + 1) * 128, cols], preferred_element_type=F32)
                + jnp.dot(wts[g, 1], yr[g * 128 : (g + 1) * 128, cols], preferred_element_type=F32)
            ).astype(BF)

    def zsum(n, way, m, h):
        sign = 1 if way == 0 else -1
        cols = pl.ds(n * 1024, 1024)
        return pltpu.make_async_remote_copy(
            src_ref=pz.at[pl.ds(32 * AT[sign * m] + 16 * h, 16), cols],
            dst_ref=zr.at[way, m - 1, pl.ds(16 * h, 16), cols],
            send_sem=zs_send.at[n, way, m - 1, h],
            recv_sem=zs_recv.at[n, way, m - 1, h],
            device_id=zup if way == 0 else zdown,
            device_id_type=MESH,
        )

    def add_and_send(n, m):
        cols = slice(n * 1024, (n + 1) * 1024)
        for h in (0, 1):
            for way in (0, 1):
                if h not in hops(way, m):
                    continue
                sign = 1 if way == 0 else -1
                if m < 4 and h in hops(way, m + 1):
                    zsum(n, way, m + 1, h).wait_recv()
                    at = slice(32 * AT[sign * m] + 16 * h, 32 * AT[sign * m] + 16 * h + 16)
                    pz[at, cols] = (
                        pz[at, cols].astype(F32) + zr[way, m, 16 * h : 16 * h + 16, cols].astype(F32)
                    ).astype(BF)
                zsum(n, way, m, h).start()

    def last(n):
        cols = slice(n * 1024, (n + 1) * 1024)
        for h in (0, 1):
            for way in (0, 1):
                zsum(n, way, 1, h).wait_recv()
        total = middle[:, cols] + spart[y, :, cols].astype(F32)
        total = total + snear[0, :, cols].astype(F32) + snear[1, :, cols].astype(F32)
        total = total + pz[0:32, cols].astype(F32)
        total = total + zr[0, 0, :, cols].astype(F32) + zr[1, 0, :, cols].astype(F32)
        out[:, cols] = total.astype(BF)

    for t in range(10):
        for m in (1, 2, 3):
            if 0 <= t - 6 + m <= 3:
                add_and_send(t - 6 + m, m)
        if 2 <= t < 6:
            combine(t - 2)
            add_and_send(t - 2, 4)
        if 1 <= t < 5:
            for g in (1, 0):
                back.relay(g, t - 1)
        if t < 4:
            finish_rows(t)
        if t == 0:
            downs[3].relay()
        if t == 2:
            rows.relay()
        if t == 4:
            shared()
        if t == 6:
            sums.relay(0)
        if t == 8:
            sums.arrived(0)
            last(0)
            last(1)
            last(2)
    last(3)

    for k in range(1, 8):
        tile_copy(k).wait_send()
    for k in range(1, 5):
        for way in (0, 1):
            for h in hops(way, k):
                ag(way, k, h).wait_send()
                for n in range(4):
                    zsum(n, way, k, h).wait_send()
    for g in (0, 1):
        fwd.sent(g)
        for n in range(4):
            back.sent(g, n)
    sums.sent(0)


def experts(normed, middle, tile, gate_g, up_g, eg, eu, ed, sg, su, sd):
    vmem = pl.BlockSpec(memory_space=pltpu.VMEM)
    anym = pl.BlockSpec(memory_space=pl.ANY)
    dma = pltpu.SemaphoreType.DMA
    return pl.pallas_call(
        experts_kernel,
        name="experts",
        out_shape=jax.ShapeDtypeStruct((32, D), BF),
        in_specs=[anym, vmem] + [anym] * 9,
        out_specs=vmem,
        scratch_shapes=[
            pltpu.VMEM((8, 8, 128), F32),
            pltpu.VMEM((256, D), BF),
            pltpu.VMEM((2, 128, 128), BF),
            pltpu.VMEM((2, 2, 128, 128), BF),
            pltpu.VMEM((256, D), BF),
            pltpu.VMEM((256, D), BF),
            pltpu.VMEM((256, D), BF),
            pltpu.VMEM((256, D), BF),
            pltpu.VMEM((2, 2, 16, D), BF),
            pltpu.VMEM((2, 2, 16, D), BF),
            pltpu.VMEM((256, D), BF),
            pltpu.VMEM((2, 4, 32, D), BF),
            pltpu.VMEM((4, 4096, 256), BF),
            pltpu.VMEM((512, D), BF),
            pltpu.VMEM((256, 512), BF),
            pltpu.VMEM((4096, 128), BF),
            pltpu.VMEM((4096, 128), BF),
            pltpu.VMEM((128, D), BF),
            pltpu.VMEM((4, 32, D), BF),
            pltpu.VMEM((4, 32, D), BF),
            pltpu.VMEM((2, 16, D), BF),
            pltpu.VMEM((2, 32, D), BF),
            dma((7,)), dma((7,)),
            dma((2, 4, 2)), dma((2, 4, 2)),
            dma((4, 2, 4, 2)), dma((4, 2, 4, 2)),
            dma((5, 2, 8)), dma((5, 2, 8)),
            dma((5, 2, 2)), dma((5, 2, 2)),
            dma((5, 6)), dma((5, 6)),
            dma((6,)), dma((6,)),
            dma((1, 2, 3)), dma((1, 2, 3)),
            dma((15,)),
        ],
        compiler_params=pltpu.CompilerParams(
            collective_id=1, has_side_effects=True, vmem_limit_bytes=60 * 1024 * 1024
        ),
    )(normed, middle, tile, gate_g, up_g, eg, eu, ed, sg, su, sd)


def body(
    full_queries, full_keys, full_values, full_gates, half_queries, half_keys, half_values,
    half_gates, residual, full_output, half_output, norm_gain, routes, route_weights,
    expert_gate, expert_up, expert_down, shared_gate, shared_up, shared_down,
):
    quarter = lax.axis_index("tp")
    own = lambda a: lax.dynamic_slice_in_dim(a.T.astype(F32), quarter * 32, 32, 1)
    tile = jnp.tile(jnp.concatenate([own(routes), own(route_weights)], axis=0), (1, 4))
    middle, normed, gates, ups = attend(
        full_queries, full_keys, full_values, full_gates.T, half_queries, half_keys, half_values,
        half_gates.T, residual, full_output, half_output, norm_gain.reshape(1, D),
        expert_gate[0], expert_up[0],
    )
    return experts(
        normed, middle, tile, gates, ups, expert_gate[0], expert_up[0], expert_down[0],
        shared_gate, shared_up, shared_down,
    )


def solution(mesh):
    return jax.shard_map(
        body,
        mesh=mesh,
        in_specs=(
            P("sp", "tp"), P("sp", "tp"), P("sp", "tp"), P(None, "tp"),
            P("sp", "tp"), P("sp", "tp"), P("sp", "tp"), P(None, "tp"),
            P("sp", None), P("tp", None), P("tp", None), P(), P("sp", None), P("sp", None),
            P("sp", None, "tp"), P("sp", None, "tp"), P("sp", "tp", None),
            P(None, "tp"), P(None, "tp"), P("tp", None),
        ),
        out_specs=P(("sp", "tp"), None),
        check_vma=False,
    )
```

```python
import functools
import heapq

import jax
import jax.numpy as jnp
from jax import lax
from jax.experimental import pallas as pl
from jax.experimental.pallas import tpu as pltpu
from jax.sharding import PartitionSpec as P

D = 4096
LOG2E = 1.4426950408889634
BF = jnp.bfloat16
F32 = jnp.float32
MESH = pl.DeviceIdType.MESH
NEG = -1e30
UP_ROWS = 1024


def kv_schedule():
    def onward(part, dz, dx, link):
        out = []
        if part == 0:
            if link in ("own", "z+", "z-"):
                if link == "own":
                    out += ["z+", "z-"]
                elif link == "z+" and dz < 4:
                    out.append("z+")
                elif link == "z-" and dz > -3:
                    out.append("z-")
                out += ["x+", "x-"]
            elif link == "x+" and dx == 1 and dz % 2 == 0:
                out.append("x+")
            elif link == "x-" and dx == -1 and dz % 2 == 1:
                out.append("x-")
        else:
            if link in ("own", "x+", "x-"):
                if link == "own":
                    out += ["x+", "x-"]
                elif link == "x+" and dx == 1:
                    out.append("x+")
                out += ["z+", "z-"]
            elif link == "z+" and (dz < 3 or (dz == 3 and dx in (0, 1))):
                out.append("z+")
            elif link == "z-" and dz < 0 and (dz > -3 or dx not in (0, 1)):
                out.append("z-")
        return out

    free = {"z+": 0.0, "z-": 0.0, "x+": 0.0, "x-": 0.0}
    heap, events, count = [], [], 0

    def send(now, part, dz, dx, link):
        nonlocal count
        start = max(now, free[link])
        free[link] = start + 1.4
        step = 1 if link[1] == "+" else -1
        ndz, ndx = (dz + step, dx) if link[0] == "z" else (dz, dx + step)
        if link[0] == "z" and ndz == -4:
            ndz = 4
        if link[0] == "x" and ndx == -2:
            ndx = 2
        heapq.heappush(heap, (free[link] + 1.5, count, part, ndz, ndx, link))
        count += 1

    for part in (1, 0):
        for link in onward(part, 0, 0, "own"):
            send(0.0, part, 0, 0, link)
    seen = set()
    while heap:
        now, _, part, dz, dx, link = heapq.heappop(heap)
        assert (part, dz, dx) not in seen
        seen.add((part, dz, dx))
        links = onward(part, dz, dx, link)
        events.append((part, dz, dx, tuple(links)))
        for out in links:
            send(now, part, dz, dx, out)
    assert len(events) == 62
    own = [(part, 0, 0, tuple(onward(part, 0, 0, "own"))) for part in (1, 0)]
    return own, events


def position():
    s = lax.axis_index("sp")
    y = lax.axis_index("tp")
    z, x, c = s // 8, (s // 2) % 4, s % 2
    return s, y, z, x, c


def sp_of(z, x, c):
    return lax.rem(z + 8, 8) * 8 + lax.rem(x + 4, 4) * 2 + c


def greet(peers):
    barrier = pltpu.get_barrier_semaphore()
    for peer in peers:
        pl.semaphore_signal(barrier, inc=1, device_id=peer, device_id_type=MESH)
    pl.semaphore_wait(barrier, len(peers))


class YGather:
    def __init__(self, src, dst, send_sem, recv_sem):
        s, y, *_ = position()
        self.src, self.dst, self.send, self.recv = src, dst, send_sem, recv_sem
        self.y = y
        self.up = (s, lax.rem(y + 1, 4))
        self.down = (s, lax.rem(y + 3, 4))

    def copy(self, half, src_y, way, hop):
        slot = way * 3 + (half if hop == 0 else 2)
        return pltpu.make_async_remote_copy(
            src_ref=self.src[half] if hop == 0 else self.dst(src_y, half),
            dst_ref=self.dst(src_y, half),
            send_sem=self.send.at[slot],
            recv_sem=self.recv.at[slot],
            device_id=self.up if way == 0 else self.down,
            device_id_type=MESH,
        )

    def start(self):
        self.copy(0, self.y, 0, 0).start()
        self.copy(1, self.y, 1, 0).start()
        self.copy(1, self.y, 0, 0).start()
        self.copy(0, self.y, 1, 0).start()

    def relay(self):
        below, above = lax.rem(self.y + 3, 4), lax.rem(self.y + 1, 4)
        self.copy(0, below, 0, 0).wait_recv()
        self.copy(0, below, 0, 1).start()
        self.copy(1, above, 1, 0).wait_recv()
        self.copy(1, above, 1, 1).start()

    def finish(self):
        below, above, far = lax.rem(self.y + 3, 4), lax.rem(self.y + 1, 4), lax.rem(self.y + 2, 4)
        self.copy(1, below, 0, 0).wait_recv()
        self.copy(0, above, 1, 0).wait_recv()
        self.copy(0, far, 0, 1).wait_recv()
        self.copy(1, far, 1, 1).wait_recv()
        self.sent()

    def sent(self):
        below, above = lax.rem(self.y + 3, 4), lax.rem(self.y + 1, 4)
        for half in (0, 1):
            for way in (0, 1):
                self.copy(half, self.y, way, 0).wait_send()
        self.copy(0, below, 0, 1).wait_send()
        self.copy(1, above, 1, 1).wait_send()


class YReduce:
    def __init__(self, part, far, near, send_sem, recv_sem, width):
        s, y, *_ = position()
        self.part, self.far, self.near = part, far, near
        self.send, self.recv, self.width = send_sem, recv_sem, width
        self.next = (lax.rem(y + 1, 4), lax.rem(y + 3, 4))
        self.across = lax.rem(y + 2, 4)
        self.dev = [(s, self.next[0]), (s, self.next[1])]

    def copy(self, n, way, kind):
        cols = pl.ds(n * self.width, self.width)
        low, high = pl.ds(0, 16), pl.ds(16, 16)
        merged, plain = (high, low) if way == 0 else (low, high)
        if kind == 0:
            src, dst = self.part.at[self.across, merged, cols], self.far.at[way, :, cols]
        else:
            rows = plain if kind == 1 else merged
            src, dst = self.part.at[self.next[way], rows, cols], self.near.at[way, rows, cols]
        return pltpu.make_async_remote_copy(
            src_ref=src,
            dst_ref=dst,
            send_sem=self.send.at[n, way, kind],
            recv_sem=self.recv.at[n, way, kind],
            device_id=self.dev[way],
            device_id_type=MESH,
        )

    def start(self, n):
        for kind in (0, 1):
            for way in (0, 1):
                self.copy(n, way, kind).start()

    def relay(self, n):
        cols = pl.ds(n * self.width, self.width)
        for way in (0, 1):
            rows = pl.ds(16, 16) if way == 0 else pl.ds(0, 16)
            self.copy(n, way, 0).wait_recv()
            self.part[self.next[way], rows, cols] = (
                self.part[self.next[way], rows, cols].astype(F32) + self.far[way, :, cols].astype(F32)
            ).astype(BF)
            self.copy(n, way, 2).start()

    def arrived(self, n):
        for kind in (1, 2):
            for way in (0, 1):
                self.copy(n, way, kind).wait_recv()

    def sent(self, n):
        for kind in (0, 1, 2):
            for way in (0, 1):
                self.copy(n, way, kind).wait_send()


REL = (0, -1, 1, -2, 2, -3, 3, 4)
AT = {r: i for i, r in enumerate(REL)}
AT[-4] = AT[4]


class Exchange:
    def __init__(self, src, dst, relay, send, recv, rsend, rrecv, width):
        self.width = width
        self.src, self.dst, self.rl = src, dst, relay
        self.send, self.recv, self.rsend, self.rrecv = send, recv, rsend, rrecv
        s, y, z, x, c = position()
        self.core = (c, 1 - c)
        self.dev = lambda d, core: (sp_of(z, x + d, core), y)

    def direct(self, g, d, crel, n=0):
        cols = pl.ds(n * self.width, self.width)
        m = d * 2 + crel
        slot = ((4 - d) % 4) * 2 + crel
        if d == 2:
            return pltpu.make_async_remote_copy(
                src_ref=self.src.at[pl.ds(g * 128 + 16 * m, 16), cols],
                dst_ref=self.rl.at[g, crel, :, cols],
                send_sem=self.send.at[n, g, m],
                recv_sem=self.rrecv.at[n, g, crel],
                device_id=self.dev(1 if crel == 0 else 3, self.core[0]),
                device_id_type=MESH,
            )
        return pltpu.make_async_remote_copy(
            src_ref=self.src.at[pl.ds(g * 128 + 16 * m, 16), cols],
            dst_ref=self.dst.at[pl.ds(g * 128 + 16 * slot, 16), cols],
            send_sem=self.send.at[n, g, m],
            recv_sem=self.recv.at[n, g, slot],
            device_id=self.dev(d, self.core[crel]),
            device_id_type=MESH,
        )

    def passed(self, g, crel, n=0):
        cols = pl.ds(n * self.width, self.width)
        slot = 4 + crel
        return pltpu.make_async_remote_copy(
            src_ref=self.rl.at[g, crel, :, cols],
            dst_ref=self.dst.at[pl.ds(g * 128 + 16 * slot, 16), cols],
            send_sem=self.rsend.at[n, g, crel],
            recv_sem=self.recv.at[n, g, slot],
            device_id=self.dev(1 if crel == 0 else 3, self.core[crel]),
            device_id_type=MESH,
        )

    def local(self, g, n=0):
        cols = pl.ds(n * self.width, self.width)
        return pltpu.make_async_copy(
            self.src.at[pl.ds(g * 128, 16), cols],
            self.dst.at[pl.ds(g * 128, 16), cols],
            self.recv.at[n, g, 0],
        )

    def start(self, g, n=0):
        for d, crel in ((2, 0), (2, 1), (1, 0), (3, 0), (1, 1), (3, 1), (0, 1)):
            self.direct(g, d, crel, n).start()
        self.local(g, n).start()

    def relay(self, g, n=0):
        for crel in (0, 1):
            self.direct(g, 2, crel, n).wait_recv()
            self.passed(g, crel, n).start()

    def arrived(self, g, n=0):
        self.local(g, n).wait()
        for d, crel in ((0, 1), (1, 0), (3, 0), (1, 1), (3, 1)):
            self.direct(g, d, crel, n).wait_recv()
        for crel in (0, 1):
            self.passed(g, crel, n).wait_recv()

    def sent(self, g, n=0):
        for d, crel in ((2, 0), (2, 1), (1, 0), (3, 0), (1, 1), (3, 1), (0, 1)):
            self.direct(g, d, crel, n).wait_send()
        for crel in (0, 1):
            self.passed(g, crel, n).wait_send()


def layer_kernel(
    fq, fk, fv, gf, hq, hk, hv, gh, res, wf, wh, gain, tile, eg, eu, ed, sg, su, sd,
    out,
    kva, kvb, qs, acc, mx, tot, att, part, far, near, resv, mid, wfv, whv,
    tiles, tok, sel, wts, sb, xr, yb, yr, rl0, rl1, pz, zr, gu, dn, hid, sgv, suv, sdv, nall, spart,
    sfar, snear,
    own_sem, kv_send, kv_recv, rs_send, rs_recv, res_sem,
    tile_send, tile_recv, ag_send, ag_recv, zs_send, zs_recv,
    x_send, x_recv, xr_send, xr_recv, w_send, w_recv, g_send, g_recv, s_send, s_recv, ld,
):
    s, y, z, x, c = position()
    sib = (s + 1 - 2 * c, y)
    to = {
        "z+": (sp_of(z + 1, x, c), y),
        "z-": (sp_of(z - 1, x, c), y),
        "x+": (sp_of(z, x + 1, c), y),
        "x-": (sp_of(z, x - 1, c), y),
    }
    zup, zdown = to["z+"], to["z-"]
    zs = [(sp_of(z + k, x, c), y) for k in range(1, 8)]
    xs = [(sp_of(z, x + d, core), y) for d in (1, 3) for core in (c, 1 - c)]
    greet(zs + xs + [sib] + [(s, lax.rem(y + k, 4)) for k in (1, 2, 3)])

    kv = (kva, kvb)
    pieces = [
        (fk, kva, 0), (fv, kva, 128), (hk, kvb, 0), (hv, kvb, 128),
    ]
    own = [
        pltpu.make_async_copy(src, dst.at[s, :, pl.ds(at, 128)], own_sem.at[i])
        for i, (src, dst, at) in enumerate(pieces)
    ]
    for copy in own:
        copy.start()
    res_copy = pltpu.make_async_copy(res.at[pl.ds(y * 32, 32)], resv, res_sem)
    res_copy.start()

    loads = [
        pltpu.make_async_copy(tile, tiles.at[z], ld.at[0]),
        pltpu.make_async_copy(eg, gu.at[y, :, pl.ds(0, 128)], ld.at[1]),
        pltpu.make_async_copy(eu, gu.at[y, :, pl.ds(128, 128)], ld.at[2]),
        pltpu.make_async_copy(ed, dn.at[pl.ds(y * 128, 128)], ld.at[3]),
        pltpu.make_async_copy(sg, sgv, ld.at[4]),
        pltpu.make_async_copy(su, suv, ld.at[5]),
        pltpu.make_async_copy(sd, sdv, ld.at[6]),
        pltpu.make_async_copy(wf, wfv, ld.at[7]),
        pltpu.make_async_copy(wh, whv, ld.at[8]),
    ]
    loads[0].start()

    def hop(prt, idx, device):
        return pltpu.make_async_remote_copy(
            src_ref=kv[prt].at[idx],
            dst_ref=kv[prt].at[idx],
            send_sem=kv_send.at[prt],
            recv_sem=kv_recv.at[prt, idx],
            device_id=device,
            device_id_type=MESH,
        )

    own_events, events = kv_schedule()
    for prt, _, _, links in own_events:
        own[2 * prt].wait()
        own[2 * prt + 1].wait()
        for link in links:
            hop(prt, s, to[link]).start()
        hop(prt, s, sib).start()

    def tile_copy(k):
        return pltpu.make_async_remote_copy(
            src_ref=tiles.at[z],
            dst_ref=tiles.at[z],
            send_sem=tile_send.at[k - 1],
            recv_sem=tile_recv.at[k - 1],
            device_id=zs[k - 1],
            device_id_type=MESH,
        )


    loads[0].wait()
    for k in range(1, 8):
        tile_copy(k).start()

    gates = YGather(
        [eg.at[pl.ds(h * 2048, 2048)] for h in (0, 1)],
        lambda j, h: gu.at[j, pl.ds(h * 2048, 2048), pl.ds(0, 128)],
        w_send.at[0], w_recv.at[0],
    )

    def up_rows(at, count, slot):
        return YGather(
            [eu.at[pl.ds(at + h * count // 2, count // 2)] for h in (0, 1)],
            lambda j, h: gu.at[j, pl.ds(at + h * count // 2, count // 2), pl.ds(128, 128)],
            w_send.at[slot], w_recv.at[slot],
        )

    ups0 = up_rows(0, UP_ROWS, 1)
    ups = up_rows(UP_ROWS, 4096 - UP_ROWS, 2)
    gates.start()
    ups0.start()
    for copy in loads[1:]:
        copy.start()

    lane = lax.broadcasted_iota(jnp.int32, (128, 128), 1)
    qs[0, 0:128] = fq[:, 0:128]
    qs[0, 128:256] = fq[:, 128:256]
    h01 = hq[:, 0:128].astype(F32)
    h23 = hq[:, 128:256].astype(F32)
    qs[1, 0:128] = jnp.where(lane < 64, h01, 0.0).astype(BF)
    qs[1, 128:256] = jnp.where(lane < 64, pltpu.roll(h01, 64, 1), 0.0).astype(BF)
    qs[2, 0:128] = jnp.where(lane >= 64, pltpu.roll(h23, 64, 1), 0.0).astype(BF)
    qs[2, 128:256] = jnp.where(lane >= 64, h23, 0.0).astype(BF)
    acc[...] = jnp.zeros_like(acc)
    tot[...] = jnp.zeros_like(tot)
    mx[...] = jnp.full_like(mx, NEG)

    row0 = s * 128
    gfirst = gf[:, pl.ds(pl.multiple_of(row0, 128), 128)][:, 0:1]
    hfirst = gh[:, pl.ds(pl.multiple_of(row0, 128), 128)][:, 0:1]

    def attend_to(plane, g, masked):
        key0 = pl.multiple_of(plane * 1024, 1024)
        if g == 0:
            gate = (gf[:, pl.ds(key0, 1024)] - gfirst) * LOG2E
        else:
            gate = (gh[:, pl.ds(key0, 1024)] - hfirst) * LOG2E
        store = kva if g == 0 else kvb
        k = store[pl.ds(plane * 8, 8), :, 0:128].reshape(1024, 128)
        v = store[pl.ds(plane * 8, 8), :, 128:256].reshape(1024, 128)
        scale = (128 ** -0.5 if g == 0 else 0.125) * LOG2E
        scores = lax.dot_general(
            qs[g], k, (((1,), (1,)), ((), ())), preferred_element_type=F32
        )
        for r in (0, 1):
            head = r if g == 0 else 2 * (g - 1) + r
            t = scores[r * 128 : (r + 1) * 128] * scale - gate[head : head + 1]
            if masked:
                qpos = (s % 8) * 128 + lax.broadcasted_iota(jnp.int32, (128, 1024), 0)
                kpos = lax.broadcasted_iota(jnp.int32, (128, 1024), 1)
                t = jnp.where(kpos <= qpos, t, NEG)
            old = mx[g, pl.ds(r * 128, 128)]
            new = jnp.maximum(old, jnp.max(t, axis=1, keepdims=True))
            p = jnp.exp2(t - new[:, 0:1])
            shrink = jnp.exp2(old - new)
            mx[g, pl.ds(r * 128, 128)] = new
            tot[g, pl.ds(r * 128, 128)] = (
                tot[g, pl.ds(r * 128, 128)] * shrink + jnp.sum(p, axis=1, keepdims=True)
            )
            acc[g, pl.ds(r * 128, 128)] = acc[g, pl.ds(r * 128, 128)] * shrink + jnp.dot(
                p.astype(BF), v, preferred_element_type=F32
            )

    waiting = []
    for dz in range(-3, 5):
        for g in range(3):
            last = max(
                i for i, (prt, edz, *_) in enumerate(events) if edz == dz and prt == min(g, 1)
            )
            waiting.append((last + 3, g, dz))
    waiting.sort()

    def next_item():
        _, g, dz = waiting.pop(0)
        plane = lax.rem(z - dz + 8, 8)
        if g < 2:
            for col in range(4):
                hop(g, sp_of(plane, col, 1 - c), sib).wait_recv()
        if dz == 0:
            attend_to(z, g, True)
        else:

            @pl.when(plane < z)
            def _():
                attend_to(plane, g, False)

    for i, (prt, dz, dx, links) in enumerate(events):
        idx = sp_of(z - dz, x - dx, c)
        hop(prt, idx, sib).wait_recv()
        for link in links:
            hop(prt, idx, to[link]).start()
        hop(prt, idx, sib).start()
        if waiting and waiting[0][0] <= i:
            next_item()
        if i == 30:
            gates.relay()
        if i == 46:
            ups0.relay()
    while waiting:
        next_item()

    outs = [
        [acc[g, r * 128 : (r + 1) * 128] / tot[g, r * 128 : (r + 1) * 128] for r in (0, 1)]
        for g in range(3)
    ]
    att[:, 0:128] = outs[0][0].astype(BF)
    att[:, 128:256] = outs[0][1].astype(BF)
    att[:, 256:384] = jnp.where(lane < 64, outs[1][0], pltpu.roll(outs[1][1], 64, 1)).astype(BF)
    att[:, 384:512] = jnp.where(lane < 64, pltpu.roll(outs[2][0], 64, 1), outs[2][1]).astype(BF)

    for copy in loads[7:]:
        copy.wait()
    asums = YReduce(part, far, near, rs_send, rs_recv, 1024)
    for n in range(4):
        cols = slice(n * 1024, (n + 1) * 1024)
        product = jnp.dot(att[:, 0:256], wfv[:, cols], preferred_element_type=F32) + jnp.dot(
            att[:, 256:512], whv[:, cols], preferred_element_type=F32
        )
        part[:, :, cols] = product.astype(BF).reshape(4, 32, 1024)
        asums.start(n)
    for k in range(1, 8):
        tile_copy(k).wait_recv()

    lane4 = lax.broadcasted_iota(jnp.int32, (4, 128), 1) // 32
    row16 = lax.broadcasted_iota(jnp.int32, (16, 128), 0)
    lane16 = lax.broadcasted_iota(jnp.int32, (16, 128), 1) // 32
    r0 = lax.broadcasted_iota(jnp.int32, (128, 128), 0)
    r1 = lax.broadcasted_iota(jnp.int32, (128, 128), 1)
    earlier = jnp.where((r0 // 32 == r1 // 32) & (r0 < r1), 1.0, 0.0).astype(BF)

    def picks(g):
        names = jnp.zeros((4, 128), F32)
        scale = jnp.zeros((4, 128), F32)
        for i in range(4):
            src = lax.rem(z + REL[g * 4 + i] + 8, 8)
            names = jnp.where(lane4 == i, tiles[src, 0:4], names)
            scale = jnp.where(lane4 == i, tiles[src, 4:8], scale)
        occ, wrow = [], []
        for d in range(4):
            for crel in (0, 1):
                core = c + crel - 2 * c * crel
                expert = (z * 8 + lax.rem(x + d, 4) * 2 + core).astype(F32)
                hit = jnp.where(names == expert, 1.0, 0.0)
                occ.append(jnp.sum(hit, axis=0, keepdims=True))
                wrow.append(jnp.sum(hit * scale, axis=0, keepdims=True))
        occupied = jnp.concatenate(occ, axis=0)
        rank = jnp.dot(occupied.astype(BF), earlier, preferred_element_type=F32)
        weighted = []
        for m in range(8):
            chosen = (
                (lane16 == row16 // 4)
                & (rank[m : m + 1] == (row16 % 4).astype(F32))
                & (occ[m] > 0.5)
            )
            sel[g, pl.ds(16 * m, 16)] = jnp.where(chosen, 1.0, 0.0).astype(BF)
            weighted.append(jnp.where(chosen, wrow[m], 0.0))
        full = jnp.concatenate(weighted, axis=0).T
        high = full.astype(BF)
        wts[g, 0] = high
        wts[g, 1] = (full - high.astype(F32)).astype(BF)

    picks(0)
    picks(1)
    for n in range(4):
        asums.relay(n)
    ups.start()
    res_copy.wait()
    square = jnp.zeros((32, 1), F32)
    for n in range(4):
        cols = slice(n * 1024, (n + 1) * 1024)
        total = resv[:, cols].astype(F32) + part[y, :, cols].astype(F32)
        asums.arrived(n)
        total = total + near[0, :, cols].astype(F32) + near[1, :, cols].astype(F32)
        mid[:, cols] = total
        square = square + jnp.sum(total * total, axis=1, keepdims=True)
    factor = lax.rsqrt(square * (1.0 / D) + 1e-06)
    for n in range(4):
        cols = slice(n * 1024, (n + 1) * 1024)
        normed = (mid[:, cols] * factor * gain[:, cols]).astype(BF)
        tok[0:32, cols] = normed
        nall[y, :, cols] = normed

    def ag(way, k, h):
        sign = -1 if way == 0 else 1
        return pltpu.make_async_remote_copy(
            src_ref=tok.at[pl.ds(32 * AT[sign * (k - 1)] + 16 * h, 16)],
            dst_ref=tok.at[pl.ds(32 * AT[sign * k] + 16 * h, 16)],
            send_sem=ag_send.at[way, k - 1, h],
            recv_sem=ag_recv.at[way, k - 1, h],
            device_id=zup if way == 0 else zdown,
            device_id_type=MESH,
        )

    def hops(way, k):
        return (0, 1) if k < 4 else ((0,) if way == 0 else (1,))

    for h in (0, 1):
        for way in (0, 1):
            ag(way, 1, h).start()

    def down_chunk(n):
        cols = pl.ds(n * 1024, 1024)
        return YGather(
            [ed.at[pl.ds(h * 64, 64), cols] for h in (0, 1)],
            lambda j, h: dn.at[pl.ds(j * 128 + h * 64, 64), cols],
            w_send.at[3 + n], w_recv.at[3 + n],
        )

    downs = [down_chunk(n) for n in range(4)]
    rows = YGather(
        [nall.at[y, pl.ds(h * 16, 16)] for h in (0, 1)],
        lambda j, h: nall.at[j, pl.ds(h * 16, 16)],
        g_send, g_recv,
    )
    downs[0].start()

    fwd = Exchange(sb, xr, rl0, x_send.at[pl.ds(0, 1)], x_recv.at[pl.ds(0, 1)], xr_send.at[pl.ds(0, 1)], xr_recv.at[pl.ds(0, 1)], D)
    back = Exchange(yb, yr, rl1, x_send.at[pl.ds(1, 4)], x_recv.at[pl.ds(1, 4)], xr_send.at[pl.ds(1, 4)], xr_recv.at[pl.ds(1, 4)], 1024)

    def select(g):
        for n in range(4):
            cols = slice(n * 1024, (n + 1) * 1024)
            sb[g * 128 : (g + 1) * 128, cols] = jnp.dot(
                sel[g], tok[g * 128 : (g + 1) * 128, cols], preferred_element_type=F32
            ).astype(BF)
        fwd.start(g)

    for k in range(1, 5):
        for h in (0, 1):
            for way in (0, 1):
                if h in hops(way, k):
                    ag(way, k, h).wait_recv()
                    if k < 4 and h in hops(way, k + 1):
                        ag(way, k + 1, h).start()
        if k == 2:
            select(0)
            ups.relay()
            downs[1].start()
        if k == 3:
            fwd.relay(0)
            downs[0].relay()
            downs[2].start()
    select(1)
    downs[1].relay()
    downs[3].start()

    fwd.relay(1)
    downs[2].relay()
    rows.start()
    for copy in loads[1:7]:
        copy.wait()
    gates.finish()
    ups0.finish()
    ups.finish()
    fwd.arrived(0)
    fwd.arrived(1)

    @pl.loop(0, 4)
    def _(j):
        both = jnp.dot(xr[...], gu[j], preferred_element_type=F32)
        g, u = both[:, 0:128], both[:, 128:256]
        hid[:, pl.ds(pl.multiple_of(j * 128, 128), 128)] = (g / (1.0 + jnp.exp(-g)) * u).astype(BF)

    sums = YReduce(spart, sfar, snear, s_send, s_recv, D)

    def finish_rows(n):
        downs[n].finish()
        cols = slice(n * 1024, (n + 1) * 1024)
        yb[:, cols] = jnp.dot(hid[...], dn[:, cols], preferred_element_type=F32).astype(BF)
        for g in (1, 0):
            back.start(g, n)

    def shared():
        rows.finish()
        everyone = nall[...].reshape(128, D)
        g = jnp.dot(everyone, sgv[...], preferred_element_type=F32)
        u = jnp.dot(everyone, suv[...], preferred_element_type=F32)
        shared_hidden = (g / (1.0 + jnp.exp(-g)) * u).astype(BF)
        for n in range(4):
            cols = slice(n * 1024, (n + 1) * 1024)
            spart[:, :, cols] = (
                jnp.dot(shared_hidden, sdv[:, cols], preferred_element_type=F32)
                .astype(BF)
                .reshape(4, 32, 1024)
            )
        sums.start(0)

    def combine(n):
        cols = slice(n * 1024, (n + 1) * 1024)
        for g in (1, 0):
            back.arrived(g, n)
            pz[g * 128 : (g + 1) * 128, cols] = (
                jnp.dot(wts[g, 0], yr[g * 128 : (g + 1) * 128, cols], preferred_element_type=F32)
                + jnp.dot(wts[g, 1], yr[g * 128 : (g + 1) * 128, cols], preferred_element_type=F32)
            ).astype(BF)

    def zsum(n, way, m, h):
        sign = 1 if way == 0 else -1
        cols = pl.ds(n * 1024, 1024)
        return pltpu.make_async_remote_copy(
            src_ref=pz.at[pl.ds(32 * AT[sign * m] + 16 * h, 16), cols],
            dst_ref=zr.at[way, m - 1, pl.ds(16 * h, 16), cols],
            send_sem=zs_send.at[n, way, m - 1, h],
            recv_sem=zs_recv.at[n, way, m - 1, h],
            device_id=zup if way == 0 else zdown,
            device_id_type=MESH,
        )

    def add_and_send(n, m):
        cols = slice(n * 1024, (n + 1) * 1024)
        for h in (0, 1):
            for way in (0, 1):
                if h not in hops(way, m):
                    continue
                sign = 1 if way == 0 else -1
                if m < 4 and h in hops(way, m + 1):
                    zsum(n, way, m + 1, h).wait_recv()
                    at = slice(32 * AT[sign * m] + 16 * h, 32 * AT[sign * m] + 16 * h + 16)
                    pz[at, cols] = (
                        pz[at, cols].astype(F32) + zr[way, m, 16 * h : 16 * h + 16, cols].astype(F32)
                    ).astype(BF)
                zsum(n, way, m, h).start()

    def last(n):
        cols = slice(n * 1024, (n + 1) * 1024)
        for h in (0, 1):
            for way in (0, 1):
                zsum(n, way, 1, h).wait_recv()
        total = mid[:, cols] + spart[y, :, cols].astype(F32)
        total = total + snear[0, :, cols].astype(F32) + snear[1, :, cols].astype(F32)
        total = total + pz[0:32, cols].astype(F32)
        total = total + zr[0, 0, :, cols].astype(F32) + zr[1, 0, :, cols].astype(F32)
        out[:, cols] = total.astype(BF)

    for t in range(10):
        for m in (1, 2, 3):
            if 0 <= t - 6 + m <= 3:
                add_and_send(t - 6 + m, m)
        if 2 <= t < 6:
            combine(t - 2)
            add_and_send(t - 2, 4)
        if 1 <= t < 5:
            for g in (1, 0):
                back.relay(g, t - 1)
        if t < 4:
            finish_rows(t)
        if t == 0:
            downs[3].relay()
        if t == 2:
            rows.relay()
        if t == 4:
            shared()
        if t == 6:
            sums.relay(0)
        if t == 8:
            sums.arrived(0)
            last(0)
            last(1)
            last(2)
    last(3)

    for k in range(1, 8):
        tile_copy(k).wait_send()
    for k in range(1, 5):
        for way in (0, 1):
            for h in hops(way, k):
                ag(way, k, h).wait_send()
                for n in range(4):
                    zsum(n, way, k, h).wait_send()
    for g in (0, 1):
        fwd.sent(g)
        for n in range(4):
            back.sent(g, n)
    sums.sent(0)

    for n in range(4):
        asums.sent(n)
    for prt in (0, 1):
        everything = kv[prt].at[pl.ds(0, 63)]
        pltpu.make_async_copy(everything, everything, kv_send.at[prt]).wait()


def layer(*args):
    vmem = pl.BlockSpec(memory_space=pltpu.VMEM)
    anym = pl.BlockSpec(memory_space=pl.ANY)
    dma = pltpu.SemaphoreType.DMA
    bf = lambda *shape: pltpu.VMEM(shape, BF)
    return pl.pallas_call(
        layer_kernel,
        name="layer",
        out_shape=jax.ShapeDtypeStruct((32, D), BF),
        in_specs=[vmem, anym, anym, vmem, vmem, anym, anym, vmem, anym, anym, anym, vmem] + [anym] * 7,
        out_specs=vmem,
        scratch_shapes=[
            bf(64, 128, 256), bf(64, 128, 256), bf(3, 256, 128),
            pltpu.VMEM((3, 256, 128), F32), pltpu.VMEM((3, 256, 128), F32),
            pltpu.VMEM((3, 256, 128), F32),
            bf(128, 512), bf(4, 32, D), bf(2, 16, D), bf(2, 32, D), bf(32, D),
            pltpu.VMEM((32, D), F32), bf(256, D), bf(256, D),
            pltpu.VMEM((8, 8, 128), F32), bf(256, D), bf(2, 128, 128), bf(2, 2, 128, 128),
            bf(256, D), bf(256, D), bf(256, D), bf(256, D), bf(2, 2, 16, D), bf(2, 2, 16, D),
            bf(256, D), bf(2, 4, 32, D), bf(4, 4096, 256), bf(512, D), bf(256, 512),
            bf(4096, 128), bf(4096, 128), bf(128, D), bf(4, 32, D), bf(4, 32, D),
            bf(2, 16, D), bf(2, 32, D),
            dma((4,)), dma((2,)), dma((2, 64)), dma((4, 2, 3)), dma((4, 2, 3)), dma,
            dma((7,)), dma((7,)), dma((2, 4, 2)), dma((2, 4, 2)),
            dma((4, 2, 4, 2)), dma((4, 2, 4, 2)), dma((5, 2, 8)), dma((5, 2, 8)),
            dma((5, 2, 2)), dma((5, 2, 2)), dma((7, 6)), dma((7, 6)), dma((6,)), dma((6,)),
            dma((1, 2, 3)), dma((1, 2, 3)), dma((9,)),
        ],
        compiler_params=pltpu.CompilerParams(
            collective_id=0, has_side_effects=True, vmem_limit_bytes=62 * 1024 * 1024
        ),
    )(*args)


def body(
    full_queries, full_keys, full_values, full_gates, half_queries, half_keys, half_values,
    half_gates, residual, full_output, half_output, norm_gain, routes, route_weights,
    expert_gate, expert_up, expert_down, shared_gate, shared_up, shared_down,
):
    quarter = lax.axis_index("tp")
    own = lambda a: lax.dynamic_slice_in_dim(a.T.astype(F32), quarter * 32, 32, 1)
    tile = jnp.tile(jnp.concatenate([own(routes), own(route_weights)], axis=0), (1, 4))
    return layer(
        full_queries, full_keys, full_values, full_gates.T, half_queries, half_keys, half_values,
        half_gates.T, residual, full_output, half_output, norm_gain.reshape(1, D), tile,
        expert_gate[0], expert_up[0], expert_down[0], shared_gate, shared_up, shared_down,
    )


def solution(mesh):
    return jax.shard_map(
        body,
        mesh=mesh,
        in_specs=(
            P("sp", "tp"), P("sp", "tp"), P("sp", "tp"), P(None, "tp"),
            P("sp", "tp"), P("sp", "tp"), P("sp", "tp"), P(None, "tp"),
            P("sp", None), P("tp", None), P("tp", None), P(), P("sp", None), P("sp", None),
            P("sp", None, "tp"), P("sp", None, "tp"), P("sp", "tp", None),
            P(None, "tp"), P(None, "tp"), P("tp", None),
        ),
        out_specs=P(("sp", "tp"), None),
        check_vma=False,
    )
```

```python
import functools
import heapq

import jax
import jax.numpy as jnp
from jax import lax
from jax.experimental import pallas as pl
from jax.experimental.pallas import tpu as pltpu
from jax.sharding import PartitionSpec as P

D = 4096
LOG2E = 1.4426950408889634
BF = jnp.bfloat16
F32 = jnp.float32
MESH = pl.DeviceIdType.MESH
NEG = -1e30
UP_ROWS = 1024


def kv_schedule():
    def onward(part, dz, dx, link):
        out = []
        if part == 0:
            if link in ("own", "z+", "z-"):
                if link == "own":
                    out += ["z+", "z-"]
                elif link == "z+" and dz < 4:
                    out.append("z+")
                elif link == "z-" and dz > -3:
                    out.append("z-")
                out += ["x+", "x-"]
            elif link == "x+" and dx == 1 and dz % 2 == 0:
                out.append("x+")
            elif link == "x-" and dx == -1 and dz % 2 == 1:
                out.append("x-")
        else:
            if link in ("own", "x+", "x-"):
                if link == "own":
                    out += ["x+", "x-"]
                elif link == "x+" and dx == 1:
                    out.append("x+")
                out += ["z+", "z-"]
            elif link == "z+" and (dz < 3 or (dz == 3 and dx in (0, 1))):
                out.append("z+")
            elif link == "z-" and dz < 0 and (dz > -3 or dx not in (0, 1)):
                out.append("z-")
        return out

    free = {"z+": 0.0, "z-": 0.0, "x+": 0.0, "x-": 0.0}
    heap, events, count = [], [], 0

    def send(now, part, dz, dx, link):
        nonlocal count
        start = max(now, free[link])
        free[link] = start + 1.4
        step = 1 if link[1] == "+" else -1
        ndz, ndx = (dz + step, dx) if link[0] == "z" else (dz, dx + step)
        if link[0] == "z" and ndz == -4:
            ndz = 4
        if link[0] == "x" and ndx == -2:
            ndx = 2
        heapq.heappush(heap, (free[link] + 2.5, count, part, ndz, ndx, link))
        count += 1

    for part in (0, 1):
        for link in onward(part, 0, 0, "own"):
            send(0.0, part, 0, 0, link)
    seen = set()
    while heap:
        now, _, part, dz, dx, link = heapq.heappop(heap)
        assert (part, dz, dx) not in seen
        seen.add((part, dz, dx))
        links = onward(part, dz, dx, link)
        events.append((part, dz, dx, tuple(links)))
        for out in links:
            send(now, part, dz, dx, out)
    assert len(events) == 62
    own = [(part, 0, 0, tuple(onward(part, 0, 0, "own"))) for part in (0, 1)]
    return own, events


def position():
    s = lax.axis_index("sp")
    y = lax.axis_index("tp")
    z, x, c = s // 8, (s // 2) % 4, s % 2
    return s, y, z, x, c


def sp_of(z, x, c):
    return lax.rem(z + 8, 8) * 8 + lax.rem(x + 4, 4) * 2 + c


def greet(peers):
    barrier = pltpu.get_barrier_semaphore()
    for peer in peers:
        pl.semaphore_signal(barrier, inc=1, device_id=peer, device_id_type=MESH)
    pl.semaphore_wait(barrier, len(peers))


class YGather:
    def __init__(self, src, dst, send_sem, recv_sem):
        s, y, *_ = position()
        self.src, self.dst, self.send, self.recv = src, dst, send_sem, recv_sem
        self.y = y
        self.up = (s, lax.rem(y + 1, 4))
        self.down = (s, lax.rem(y + 3, 4))

    def copy(self, half, src_y, way, hop):
        slot = way * 3 + (half if hop == 0 else 2)
        return pltpu.make_async_remote_copy(
            src_ref=self.src[half] if hop == 0 else self.dst(src_y, half),
            dst_ref=self.dst(src_y, half),
            send_sem=self.send.at[slot],
            recv_sem=self.recv.at[slot],
            device_id=self.up if way == 0 else self.down,
            device_id_type=MESH,
        )

    def start(self):
        self.copy(0, self.y, 0, 0).start()
        self.copy(1, self.y, 1, 0).start()
        self.copy(1, self.y, 0, 0).start()
        self.copy(0, self.y, 1, 0).start()

    def relay(self):
        below, above = lax.rem(self.y + 3, 4), lax.rem(self.y + 1, 4)
        self.copy(0, below, 0, 0).wait_recv()
        self.copy(0, below, 0, 1).start()
        self.copy(1, above, 1, 0).wait_recv()
        self.copy(1, above, 1, 1).start()

    def finish(self):
        below, above, far = lax.rem(self.y + 3, 4), lax.rem(self.y + 1, 4), lax.rem(self.y + 2, 4)
        self.copy(1, below, 0, 0).wait_recv()
        self.copy(0, above, 1, 0).wait_recv()
        self.copy(0, far, 0, 1).wait_recv()
        self.copy(1, far, 1, 1).wait_recv()
        self.sent()

    def sent(self):
        below, above = lax.rem(self.y + 3, 4), lax.rem(self.y + 1, 4)
        for half in (0, 1):
            for way in (0, 1):
                self.copy(half, self.y, way, 0).wait_send()
        self.copy(0, below, 0, 1).wait_send()
        self.copy(1, above, 1, 1).wait_send()


class YReduce:
    def __init__(self, part, far, near, send_sem, recv_sem, width):
        s, y, *_ = position()
        self.part, self.far, self.near = part, far, near
        self.send, self.recv, self.width = send_sem, recv_sem, width
        self.next = (lax.rem(y + 1, 4), lax.rem(y + 3, 4))
        self.across = lax.rem(y + 2, 4)
        self.dev = [(s, self.next[0]), (s, self.next[1])]

    def copy(self, n, way, kind):
        cols = pl.ds(n * self.width, self.width)
        low, high = pl.ds(0, 16), pl.ds(16, 16)
        merged, plain = (high, low) if way == 0 else (low, high)
        if kind == 0:
            src, dst = self.part.at[self.across, merged, cols], self.far.at[way, :, cols]
        else:
            rows = plain if kind == 1 else merged
            src, dst = self.part.at[self.next[way], rows, cols], self.near.at[way, rows, cols]
        return pltpu.make_async_remote_copy(
            src_ref=src,
            dst_ref=dst,
            send_sem=self.send.at[n, way, kind],
            recv_sem=self.recv.at[n, way, kind],
            device_id=self.dev[way],
            device_id_type=MESH,
        )

    def start(self, n):
        for kind in (0, 1):
            for way in (0, 1):
                self.copy(n, way, kind).start()

    def relay(self, n):
        cols = pl.ds(n * self.width, self.width)
        for way in (0, 1):
            rows = pl.ds(16, 16) if way == 0 else pl.ds(0, 16)
            self.copy(n, way, 0).wait_recv()
            self.part[self.next[way], rows, cols] = (
                self.part[self.next[way], rows, cols].astype(F32) + self.far[way, :, cols].astype(F32)
            ).astype(BF)
            self.copy(n, way, 2).start()

    def arrived(self, n):
        for kind in (1, 2):
            for way in (0, 1):
                self.copy(n, way, kind).wait_recv()

    def sent(self, n):
        for kind in (0, 1, 2):
            for way in (0, 1):
                self.copy(n, way, kind).wait_send()


REL = (0, -1, 1, -2, 2, -3, 3, 4)
AT = {r: i for i, r in enumerate(REL)}
AT[-4] = AT[4]


class Exchange:
    def __init__(self, src, dst, relay, send, recv, rsend, rrecv, width):
        self.width = width
        self.src, self.dst, self.rl = src, dst, relay
        self.send, self.recv, self.rsend, self.rrecv = send, recv, rsend, rrecv
        s, y, z, x, c = position()
        self.core = (c, 1 - c)
        self.dev = lambda d, core: (sp_of(z, x + d, core), y)

    def direct(self, g, d, crel, n=0):
        cols = pl.ds(n * self.width, self.width)
        m = d * 2 + crel
        slot = ((4 - d) % 4) * 2 + crel
        if d == 2:
            return pltpu.make_async_remote_copy(
                src_ref=self.src.at[pl.ds(g * 128 + 16 * m, 16), cols],
                dst_ref=self.rl.at[g, crel, :, cols],
                send_sem=self.send.at[n, g, m],
                recv_sem=self.rrecv.at[n, g, crel],
                device_id=self.dev(1 if crel == 0 else 3, self.core[0]),
                device_id_type=MESH,
            )
        return pltpu.make_async_remote_copy(
            src_ref=self.src.at[pl.ds(g * 128 + 16 * m, 16), cols],
            dst_ref=self.dst.at[pl.ds(g * 128 + 16 * slot, 16), cols],
            send_sem=self.send.at[n, g, m],
            recv_sem=self.recv.at[n, g, slot],
            device_id=self.dev(d, self.core[crel]),
            device_id_type=MESH,
        )

    def passed(self, g, crel, n=0):
        cols = pl.ds(n * self.width, self.width)
        slot = 4 + crel
        return pltpu.make_async_remote_copy(
            src_ref=self.rl.at[g, crel, :, cols],
            dst_ref=self.dst.at[pl.ds(g * 128 + 16 * slot, 16), cols],
            send_sem=self.rsend.at[n, g, crel],
            recv_sem=self.recv.at[n, g, slot],
            device_id=self.dev(1 if crel == 0 else 3, self.core[crel]),
            device_id_type=MESH,
        )

    def local(self, g, n=0):
        cols = pl.ds(n * self.width, self.width)
        return pltpu.make_async_copy(
            self.src.at[pl.ds(g * 128, 16), cols],
            self.dst.at[pl.ds(g * 128, 16), cols],
            self.recv.at[n, g, 0],
        )

    def start(self, g, n=0):
        for d, crel in ((2, 0), (2, 1), (1, 0), (3, 0), (1, 1), (3, 1), (0, 1)):
            self.direct(g, d, crel, n).start()
        self.local(g, n).start()

    def relay(self, g, n=0):
        for crel in (0, 1):
            self.direct(g, 2, crel, n).wait_recv()
            self.passed(g, crel, n).start()

    def arrived(self, g, n=0):
        self.local(g, n).wait()
        for d, crel in ((0, 1), (1, 0), (3, 0), (1, 1), (3, 1)):
            self.direct(g, d, crel, n).wait_recv()
        for crel in (0, 1):
            self.passed(g, crel, n).wait_recv()

    def sent(self, g, n=0):
        for d, crel in ((2, 0), (2, 1), (1, 0), (3, 0), (1, 1), (3, 1), (0, 1)):
            self.direct(g, d, crel, n).wait_send()
        for crel in (0, 1):
            self.passed(g, crel, n).wait_send()


def layer_kernel(
    fq, fk, fv, gf, hq, hk, hv, gh, res, wf, wh, gain, names_in, scale_in, eg, eu, ed, sg, su, sd,
    out,
    kva, kvb, qs, acc, mx, tot, att, part, far, near, resv, mid, wfv, whv,
    tiles, tok, sel, wts, sb, xr, yb, yr, rl0, rl1, pz, zr, gu, dn, hid, sgv, suv, sdv, nall, spart,
    sfar, snear,
    own_sem, kv_send, kv_recv, rs_send, rs_recv, res_sem,
    tile_send, tile_recv, ag_send, ag_recv, zs_send, zs_recv,
    x_send, x_recv, xr_send, xr_recv, w_send, w_recv, g_send, g_recv, s_send, s_recv, ld,
):
    s, y, z, x, c = position()
    sib = (s + 1 - 2 * c, y)
    to = {
        "z+": (sp_of(z + 1, x, c), y),
        "z-": (sp_of(z - 1, x, c), y),
        "x+": (sp_of(z, x + 1, c), y),
        "x-": (sp_of(z, x - 1, c), y),
    }
    zup, zdown = to["z+"], to["z-"]
    zs = [(sp_of(z + k, x, c), y) for k in range(1, 8)]
    xs = [(sp_of(z, x + d, core), y) for d in (1, 3) for core in (c, 1 - c)]
    greet(zs + xs + [sib] + [(s, lax.rem(y + k, 4)) for k in (1, 2, 3)])

    kv = (kva, kvb)
    pieces = [
        (fk, kva, 0), (fv, kva, 128), (hk, kvb, 0), (hv, kvb, 128),
    ]
    own = [
        pltpu.make_async_copy(src, dst.at[s, :, pl.ds(at, 128)], own_sem.at[i])
        for i, (src, dst, at) in enumerate(pieces)
    ]
    for copy in own:
        copy.start()
    res_copy = pltpu.make_async_copy(res.at[pl.ds(y * 32, 32)], resv, res_sem)
    res_copy.start()

    loads = [
        pltpu.make_async_copy(eg, gu.at[y, :, pl.ds(0, 128)], ld.at[1]),
        pltpu.make_async_copy(eu, gu.at[y, :, pl.ds(128, 128)], ld.at[2]),
        pltpu.make_async_copy(ed, dn.at[pl.ds(y * 128, 128)], ld.at[3]),
        pltpu.make_async_copy(sg, sgv, ld.at[4]),
        pltpu.make_async_copy(su, suv, ld.at[5]),
        pltpu.make_async_copy(sd, sdv, ld.at[6]),
        pltpu.make_async_copy(wf, wfv, ld.at[7]),
        pltpu.make_async_copy(wh, whv, ld.at[8]),
    ]
    table = jnp.concatenate([names_in[...].astype(F32), scale_in[...]], axis=0)
    own_table = jnp.zeros((8, 128), F32)
    for k in range(4):
        own_table = own_table + pltpu.roll(table, (128 - 32 * k) % 128, 1) * (y == k).astype(F32)
    own_table = jnp.where(lax.broadcasted_iota(jnp.int32, (8, 128), 1) < 32, own_table, 0.0)
    spread = own_table
    for k in (1, 2, 3):
        spread = spread + pltpu.roll(own_table, 32 * k, 1)
    tiles[z] = spread

    def hop(prt, idx, device):
        return pltpu.make_async_remote_copy(
            src_ref=kv[prt].at[idx],
            dst_ref=kv[prt].at[idx],
            send_sem=kv_send.at[prt],
            recv_sem=kv_recv.at[prt, idx],
            device_id=device,
            device_id_type=MESH,
        )

    own_events, events = kv_schedule()
    for prt, _, _, links in own_events:
        own[2 * prt].wait()
        own[2 * prt + 1].wait()
        for link in links:
            hop(prt, s, to[link]).start()
        hop(prt, s, sib).start()

    def tile_copy(k):
        return pltpu.make_async_remote_copy(
            src_ref=tiles.at[z],
            dst_ref=tiles.at[z],
            send_sem=tile_send.at[k - 1],
            recv_sem=tile_recv.at[k - 1],
            device_id=zs[k - 1],
            device_id_type=MESH,
        )


    for k in range(1, 8):
        tile_copy(k).start()

    gates = YGather(
        [eg.at[pl.ds(h * 2048, 2048)] for h in (0, 1)],
        lambda j, h: gu.at[j, pl.ds(h * 2048, 2048), pl.ds(0, 128)],
        w_send.at[0], w_recv.at[0],
    )

    def up_rows(at, count, slot):
        return YGather(
            [eu.at[pl.ds(at + h * count // 2, count // 2)] for h in (0, 1)],
            lambda j, h: gu.at[j, pl.ds(at + h * count // 2, count // 2), pl.ds(128, 128)],
            w_send.at[slot], w_recv.at[slot],
        )

    ups0 = up_rows(0, UP_ROWS, 1)
    ups = up_rows(UP_ROWS, 4096 - UP_ROWS, 2)
    gates.start()
    ups0.start()
    for copy in loads:
        copy.start()

    lane = lax.broadcasted_iota(jnp.int32, (128, 128), 1)
    qs[0, 0:128] = fq[:, 0:128]
    qs[0, 128:256] = fq[:, 128:256]
    h01 = hq[:, 0:128].astype(F32)
    h23 = hq[:, 128:256].astype(F32)
    qs[1, 0:128] = jnp.where(lane < 64, h01, 0.0).astype(BF)
    qs[1, 128:256] = jnp.where(lane < 64, pltpu.roll(h01, 64, 1), 0.0).astype(BF)
    qs[2, 0:128] = jnp.where(lane >= 64, pltpu.roll(h23, 64, 1), 0.0).astype(BF)
    qs[2, 128:256] = jnp.where(lane >= 64, h23, 0.0).astype(BF)
    acc[...] = jnp.zeros_like(acc)
    tot[...] = jnp.zeros_like(tot)
    mx[...] = jnp.full_like(mx, NEG)

    row0 = s * 128
    gfirst = gf[:, pl.ds(pl.multiple_of(row0, 128), 128)][:, 0:1]
    hfirst = gh[:, pl.ds(pl.multiple_of(row0, 128), 128)][:, 0:1]

    def attend_to(plane, g, masked):
        key0 = pl.multiple_of(plane * 1024, 1024)
        if g == 0:
            gate = (gf[:, pl.ds(key0, 1024)] - gfirst) * LOG2E
        else:
            gate = (gh[:, pl.ds(key0, 1024)] - hfirst) * LOG2E
        store = kva if g == 0 else kvb
        k = store[pl.ds(plane * 8, 8), :, 0:128].reshape(1024, 128)
        v = store[pl.ds(plane * 8, 8), :, 128:256].reshape(1024, 128)
        scale = (128 ** -0.5 if g == 0 else 0.125) * LOG2E
        scores = lax.dot_general(
            qs[g], k, (((1,), (1,)), ((), ())), preferred_element_type=F32
        )
        for r in (0, 1):
            head = r if g == 0 else 2 * (g - 1) + r
            t = scores[r * 128 : (r + 1) * 128] * scale - gate[head : head + 1]
            if masked:
                qpos = (s % 8) * 128 + lax.broadcasted_iota(jnp.int32, (128, 1024), 0)
                kpos = lax.broadcasted_iota(jnp.int32, (128, 1024), 1)
                t = jnp.where(kpos <= qpos, t, NEG)
            old = mx[g, pl.ds(r * 128, 128)]
            new = jnp.maximum(old, jnp.max(t, axis=1, keepdims=True))
            p = jnp.exp2(t - new[:, 0:1])
            shrink = jnp.exp2(old - new)
            mx[g, pl.ds(r * 128, 128)] = new
            tot[g, pl.ds(r * 128, 128)] = (
                tot[g, pl.ds(r * 128, 128)] * shrink + jnp.sum(p, axis=1, keepdims=True)
            )
            acc[g, pl.ds(r * 128, 128)] = acc[g, pl.ds(r * 128, 128)] * shrink + jnp.dot(
                p.astype(BF), v, preferred_element_type=F32
            )

    waiting = []
    for dz in range(-3, 5):
        for g in range(3):
            last = max(
                i for i, (prt, edz, *_) in enumerate(events) if edz == dz and prt == min(g, 1)
            )
            waiting.append((last + 3, g, dz))
    waiting.sort()

    def next_item():
        _, g, dz = waiting.pop(0)
        plane = lax.rem(z - dz + 8, 8)
        if g < 2:
            for col in range(4):
                hop(g, sp_of(plane, col, 1 - c), sib).wait_recv()
        if dz == 0:
            attend_to(z, g, True)
        else:

            @pl.when(plane < z)
            def _():
                attend_to(plane, g, False)

    for i, (prt, dz, dx, links) in enumerate(events):
        idx = sp_of(z - dz, x - dx, c)
        hop(prt, idx, sib).wait_recv()
        for link in links:
            hop(prt, idx, to[link]).start()
        hop(prt, idx, sib).start()
        if waiting and waiting[0][0] <= i:
            next_item()
        if i == 30:
            gates.relay()
        if i == 46:
            ups0.relay()
    while waiting:
        next_item()

    outs = [
        [acc[g, r * 128 : (r + 1) * 128] / tot[g, r * 128 : (r + 1) * 128] for r in (0, 1)]
        for g in range(3)
    ]
    att[:, 0:128] = outs[0][0].astype(BF)
    att[:, 128:256] = outs[0][1].astype(BF)
    att[:, 256:384] = jnp.where(lane < 64, outs[1][0], pltpu.roll(outs[1][1], 64, 1)).astype(BF)
    att[:, 384:512] = jnp.where(lane < 64, pltpu.roll(outs[2][0], 64, 1), outs[2][1]).astype(BF)

    for copy in loads[6:]:
        copy.wait()
    asums = YReduce(part, far, near, rs_send, rs_recv, 1024)
    for n in range(4):
        cols = slice(n * 1024, (n + 1) * 1024)
        product = jnp.dot(att[:, 0:256], wfv[:, cols], preferred_element_type=F32) + jnp.dot(
            att[:, 256:512], whv[:, cols], preferred_element_type=F32
        )
        part[:, :, cols] = product.astype(BF).reshape(4, 32, 1024)
        asums.start(n)
    for k in range(1, 8):
        tile_copy(k).wait_recv()

    lane4 = lax.broadcasted_iota(jnp.int32, (4, 128), 1) // 32
    row16 = lax.broadcasted_iota(jnp.int32, (16, 128), 0)
    lane16 = lax.broadcasted_iota(jnp.int32, (16, 128), 1) // 32
    r0 = lax.broadcasted_iota(jnp.int32, (128, 128), 0)
    r1 = lax.broadcasted_iota(jnp.int32, (128, 128), 1)
    earlier = jnp.where((r0 // 32 == r1 // 32) & (r0 < r1), 1.0, 0.0).astype(BF)

    def picks(g):
        names = jnp.zeros((4, 128), F32)
        scale = jnp.zeros((4, 128), F32)
        for i in range(4):
            src = lax.rem(z + REL[g * 4 + i] + 8, 8)
            names = jnp.where(lane4 == i, tiles[src, 0:4], names)
            scale = jnp.where(lane4 == i, tiles[src, 4:8], scale)
        occ, wrow = [], []
        for d in range(4):
            for crel in (0, 1):
                core = c + crel - 2 * c * crel
                expert = (z * 8 + lax.rem(x + d, 4) * 2 + core).astype(F32)
                hit = jnp.where(names == expert, 1.0, 0.0)
                occ.append(jnp.sum(hit, axis=0, keepdims=True))
                wrow.append(jnp.sum(hit * scale, axis=0, keepdims=True))
        occupied = jnp.concatenate(occ, axis=0)
        rank = jnp.dot(occupied.astype(BF), earlier, preferred_element_type=F32)
        weighted = []
        for m in range(8):
            chosen = (
                (lane16 == row16 // 4)
                & (rank[m : m + 1] == (row16 % 4).astype(F32))
                & (occ[m] > 0.5)
            )
            sel[g, pl.ds(16 * m, 16)] = jnp.where(chosen, 1.0, 0.0).astype(BF)
            weighted.append(jnp.where(chosen, wrow[m], 0.0))
        full = jnp.concatenate(weighted, axis=0).T
        high = full.astype(BF)
        wts[g, 0] = high
        wts[g, 1] = (full - high.astype(F32)).astype(BF)

    picks(0)
    picks(1)
    for n in range(4):
        asums.relay(n)
    ups.start()
    res_copy.wait()
    square = jnp.zeros((32, 1), F32)
    for n in range(4):
        cols = slice(n * 1024, (n + 1) * 1024)
        total = resv[:, cols].astype(F32) + part[y, :, cols].astype(F32)
        asums.arrived(n)
        total = total + near[0, :, cols].astype(F32) + near[1, :, cols].astype(F32)
        mid[:, cols] = total
        square = square + jnp.sum(total * total, axis=1, keepdims=True)
    factor = lax.rsqrt(square * (1.0 / D) + 1e-06)
    for n in range(4):
        cols = slice(n * 1024, (n + 1) * 1024)
        normed = (mid[:, cols] * factor * gain[:, cols]).astype(BF)
        tok[0:32, cols] = normed
        nall[y, :, cols] = normed

    def ag(way, k, h):
        sign = -1 if way == 0 else 1
        return pltpu.make_async_remote_copy(
            src_ref=tok.at[pl.ds(32 * AT[sign * (k - 1)] + 16 * h, 16)],
            dst_ref=tok.at[pl.ds(32 * AT[sign * k] + 16 * h, 16)],
            send_sem=ag_send.at[way, k - 1, h],
            recv_sem=ag_recv.at[way, k - 1, h],
            device_id=zup if way == 0 else zdown,
            device_id_type=MESH,
        )

    def hops(way, k):
        return (0, 1) if k < 4 else ((0,) if way == 0 else (1,))

    for h in (0, 1):
        for way in (0, 1):
            ag(way, 1, h).start()

    def down_chunk(n):
        cols = pl.ds(n * 1024, 1024)
        return YGather(
            [ed.at[pl.ds(h * 64, 64), cols] for h in (0, 1)],
            lambda j, h: dn.at[pl.ds(j * 128 + h * 64, 64), cols],
            w_send.at[3 + n], w_recv.at[3 + n],
        )

    downs = [down_chunk(n) for n in range(4)]
    rows = YGather(
        [nall.at[y, pl.ds(h * 16, 16)] for h in (0, 1)],
        lambda j, h: nall.at[j, pl.ds(h * 16, 16)],
        g_send, g_recv,
    )
    downs[0].start()

    fwd = Exchange(sb, xr, rl0, x_send.at[pl.ds(0, 1)], x_recv.at[pl.ds(0, 1)], xr_send.at[pl.ds(0, 1)], xr_recv.at[pl.ds(0, 1)], D)
    back = Exchange(yb, yr, rl1, x_send.at[pl.ds(1, 4)], x_recv.at[pl.ds(1, 4)], xr_send.at[pl.ds(1, 4)], xr_recv.at[pl.ds(1, 4)], 1024)

    def select(g):
        for n in range(4):
            cols = slice(n * 1024, (n + 1) * 1024)
            sb[g * 128 : (g + 1) * 128, cols] = jnp.dot(
                sel[g], tok[g * 128 : (g + 1) * 128, cols], preferred_element_type=F32
            ).astype(BF)
        fwd.start(g)

    for k in range(1, 5):
        for h in (0, 1):
            for way in (0, 1):
                if h in hops(way, k):
                    ag(way, k, h).wait_recv()
                    if k < 4 and h in hops(way, k + 1):
                        ag(way, k + 1, h).start()
        if k == 2:
            select(0)
            ups.relay()
            downs[1].start()
        if k == 3:
            fwd.relay(0)
            downs[0].relay()
            downs[2].start()
    select(1)
    downs[1].relay()
    downs[3].start()

    fwd.relay(1)
    downs[2].relay()
    rows.start()
    for copy in loads[:6]:
        copy.wait()
    gates.finish()
    ups0.finish()
    ups.finish()
    fwd.arrived(0)
    fwd.arrived(1)

    @pl.loop(0, 4)
    def _(j):
        both = jnp.dot(xr[...], gu[j], preferred_element_type=F32)
        g, u = both[:, 0:128], both[:, 128:256]
        hid[:, pl.ds(pl.multiple_of(j * 128, 128), 128)] = (g / (1.0 + jnp.exp(-g)) * u).astype(BF)

    sums = YReduce(spart, sfar, snear, s_send, s_recv, D)

    def finish_rows(n):
        downs[n].finish()
        cols = slice(n * 1024, (n + 1) * 1024)
        yb[:, cols] = jnp.dot(hid[...], dn[:, cols], preferred_element_type=F32).astype(BF)
        for g in (1, 0):
            back.start(g, n)

    def shared():
        rows.finish()
        everyone = nall[...].reshape(128, D)
        g = jnp.dot(everyone, sgv[...], preferred_element_type=F32)
        u = jnp.dot(everyone, suv[...], preferred_element_type=F32)
        shared_hidden = (g / (1.0 + jnp.exp(-g)) * u).astype(BF)
        for n in range(4):
            cols = slice(n * 1024, (n + 1) * 1024)
            spart[:, :, cols] = (
                jnp.dot(shared_hidden, sdv[:, cols], preferred_element_type=F32)
                .astype(BF)
                .reshape(4, 32, 1024)
            )
        sums.start(0)

    def combine(n):
        cols = slice(n * 1024, (n + 1) * 1024)
        for g in (1, 0):
            back.arrived(g, n)
            pz[g * 128 : (g + 1) * 128, cols] = (
                jnp.dot(wts[g, 0], yr[g * 128 : (g + 1) * 128, cols], preferred_element_type=F32)
                + jnp.dot(wts[g, 1], yr[g * 128 : (g + 1) * 128, cols], preferred_element_type=F32)
            ).astype(BF)

    def zsum(n, way, m, h):
        sign = 1 if way == 0 else -1
        cols = pl.ds(n * 1024, 1024)
        return pltpu.make_async_remote_copy(
            src_ref=pz.at[pl.ds(32 * AT[sign * m] + 16 * h, 16), cols],
            dst_ref=zr.at[way, m - 1, pl.ds(16 * h, 16), cols],
            send_sem=zs_send.at[n, way, m - 1, h],
            recv_sem=zs_recv.at[n, way, m - 1, h],
            device_id=zup if way == 0 else zdown,
            device_id_type=MESH,
        )

    def add_and_send(n, m):
        cols = slice(n * 1024, (n + 1) * 1024)
        for h in (0, 1):
            for way in (0, 1):
                if h not in hops(way, m):
                    continue
                sign = 1 if way == 0 else -1
                if m < 4 and h in hops(way, m + 1):
                    zsum(n, way, m + 1, h).wait_recv()
                    at = slice(32 * AT[sign * m] + 16 * h, 32 * AT[sign * m] + 16 * h + 16)
                    pz[at, cols] = (
                        pz[at, cols].astype(F32) + zr[way, m, 16 * h : 16 * h + 16, cols].astype(F32)
                    ).astype(BF)
                zsum(n, way, m, h).start()

    def last(n):
        cols = slice(n * 1024, (n + 1) * 1024)
        for h in (0, 1):
            for way in (0, 1):
                zsum(n, way, 1, h).wait_recv()
        total = mid[:, cols] + spart[y, :, cols].astype(F32)
        total = total + snear[0, :, cols].astype(F32) + snear[1, :, cols].astype(F32)
        total = total + pz[0:32, cols].astype(F32)
        total = total + zr[0, 0, :, cols].astype(F32) + zr[1, 0, :, cols].astype(F32)
        out[:, cols] = total.astype(BF)

    for t in range(10):
        for m in (1, 2, 3):
            if 0 <= t - 6 + m <= 3:
                add_and_send(t - 6 + m, m)
        if 2 <= t < 6:
            combine(t - 2)
            add_and_send(t - 2, 4)
        if 1 <= t < 5:
            for g in (1, 0):
                back.relay(g, t - 1)
        if t < 4:
            finish_rows(t)
        if t == 0:
            downs[3].relay()
        if t == 2:
            rows.relay()
        if t == 4:
            shared()
        if t == 6:
            sums.relay(0)
        if t == 8:
            sums.arrived(0)
            last(0)
            last(1)
            last(2)
    last(3)

    for k in range(1, 8):
        tile_copy(k).wait_send()
    for k in range(1, 5):
        for way in (0, 1):
            for h in hops(way, k):
                ag(way, k, h).wait_send()
                for n in range(4):
                    zsum(n, way, k, h).wait_send()
    for g in (0, 1):
        fwd.sent(g)
        for n in range(4):
            back.sent(g, n)
    sums.sent(0)

    for n in range(4):
        asums.sent(n)
    for prt in (0, 1):
        everything = kv[prt].at[pl.ds(0, 63)]
        pltpu.make_async_copy(everything, everything, kv_send.at[prt]).wait()


def layer(*args):
    vmem = pl.BlockSpec(memory_space=pltpu.VMEM)
    anym = pl.BlockSpec(memory_space=pl.ANY)
    dma = pltpu.SemaphoreType.DMA
    bf = lambda *shape: pltpu.VMEM(shape, BF)
    return pl.pallas_call(
        layer_kernel,
        name="layer",
        out_shape=jax.ShapeDtypeStruct((32, D), BF),
        in_specs=[vmem, anym, anym, vmem, vmem, anym, anym, vmem, anym, anym, anym, vmem, vmem, vmem]
        + [anym] * 6,
        out_specs=vmem,
        scratch_shapes=[
            bf(64, 128, 256), bf(64, 128, 256), bf(3, 256, 128),
            pltpu.VMEM((3, 256, 128), F32), pltpu.VMEM((3, 256, 128), F32),
            pltpu.VMEM((3, 256, 128), F32),
            bf(128, 512), bf(4, 32, D), bf(2, 16, D), bf(2, 32, D), bf(32, D),
            pltpu.VMEM((32, D), F32), bf(256, D), bf(256, D),
            pltpu.VMEM((8, 8, 128), F32), bf(256, D), bf(2, 128, 128), bf(2, 2, 128, 128),
            bf(256, D), bf(256, D), bf(256, D), bf(256, D), bf(2, 2, 16, D), bf(2, 2, 16, D),
            bf(256, D), bf(2, 4, 32, D), bf(4, 4096, 256), bf(512, D), bf(256, 512),
            bf(4096, 128), bf(4096, 128), bf(128, D), bf(4, 32, D), bf(4, 32, D),
            bf(2, 16, D), bf(2, 32, D),
            dma((4,)), dma((2,)), dma((2, 64)), dma((4, 2, 3)), dma((4, 2, 3)), dma,
            dma((7,)), dma((7,)), dma((2, 4, 2)), dma((2, 4, 2)),
            dma((4, 2, 4, 2)), dma((4, 2, 4, 2)), dma((5, 2, 8)), dma((5, 2, 8)),
            dma((5, 2, 2)), dma((5, 2, 2)), dma((7, 6)), dma((7, 6)), dma((6,)), dma((6,)),
            dma((1, 2, 3)), dma((1, 2, 3)), dma((9,)),
        ],
        compiler_params=pltpu.CompilerParams(
            collective_id=0, has_side_effects=True, vmem_limit_bytes=62 * 1024 * 1024
        ),
    )(*args)


def body(
    full_queries, full_keys, full_values, full_gates, half_queries, half_keys, half_values,
    half_gates, residual, full_output, half_output, norm_gain, routes, route_weights,
    expert_gate, expert_up, expert_down, shared_gate, shared_up, shared_down,
):
    return layer(
        full_queries, full_keys, full_values, full_gates.T, half_queries, half_keys, half_values,
        half_gates.T, residual, full_output, half_output, norm_gain.reshape(1, D), routes.T, route_weights.T,
        expert_gate[0], expert_up[0], expert_down[0], shared_gate, shared_up, shared_down,
    )


def solution(mesh):
    return jax.shard_map(
        body,
        mesh=mesh,
        in_specs=(
            P("sp", "tp"), P("sp", "tp"), P("sp", "tp"), P(None, "tp"),
            P("sp", "tp"), P("sp", "tp"), P("sp", "tp"), P(None, "tp"),
            P("sp", None), P("tp", None), P("tp", None), P(), P("sp", None), P("sp", None),
            P("sp", None, "tp"), P("sp", None, "tp"), P("sp", "tp", None),
            P(None, "tp"), P(None, "tp"), P("tp", None),
        ),
        out_specs=P(("sp", "tp"), None),
        check_vma=False,
    )
```

```python
import functools
import heapq

import jax
import jax.numpy as jnp
from jax import lax
from jax.experimental import pallas as pl
from jax.experimental.pallas import tpu as pltpu
from jax.sharding import PartitionSpec as P

D = 4096
LOG2E = 1.4426950408889634
BF = jnp.bfloat16
F32 = jnp.float32
MESH = pl.DeviceIdType.MESH
NEG = -1e30
UP_ROWS = 1024


def kv_schedule():
    def onward(part, dz, dx, link):
        out = []
        if part == 0:
            if link in ("own", "z+", "z-"):
                if link == "own":
                    out += ["z+", "z-"]
                elif link == "z+" and dz < 4:
                    out.append("z+")
                elif link == "z-" and dz > -3:
                    out.append("z-")
                out += ["x+", "x-"]
            elif link == "x+" and dx == 1 and dz % 2 == 0:
                out.append("x+")
            elif link == "x-" and dx == -1 and dz % 2 == 1:
                out.append("x-")
        else:
            if link in ("own", "x+", "x-"):
                if link == "own":
                    out += ["x+", "x-"]
                elif link == "x+" and dx == 1:
                    out.append("x+")
                out += ["z+", "z-"]
            elif link == "z+" and (dz < 3 or (dz == 3 and dx in (0, 1))):
                out.append("z+")
            elif link == "z-" and dz < 0 and (dz > -3 or dx not in (0, 1)):
                out.append("z-")
        return out

    free = {"z+": 0.0, "z-": 0.0, "x+": 0.0, "x-": 0.0}
    heap, events, count = [], [], 0

    def send(now, part, dz, dx, link):
        nonlocal count
        start = max(now, free[link])
        free[link] = start + 1.4
        step = 1 if link[1] == "+" else -1
        ndz, ndx = (dz + step, dx) if link[0] == "z" else (dz, dx + step)
        if link[0] == "z" and ndz == -4:
            ndz = 4
        if link[0] == "x" and ndx == -2:
            ndx = 2
        heapq.heappush(heap, (free[link] + 2.5, count, part, ndz, ndx, link))
        count += 1

    for part in (0, 1):
        for link in onward(part, 0, 0, "own"):
            send(0.0, part, 0, 0, link)
    seen = set()
    while heap:
        now, _, part, dz, dx, link = heapq.heappop(heap)
        assert (part, dz, dx) not in seen
        seen.add((part, dz, dx))
        links = onward(part, dz, dx, link)
        events.append((part, dz, dx, tuple(links)))
        for out in links:
            send(now, part, dz, dx, out)
    assert len(events) == 62
    own = [(part, 0, 0, tuple(onward(part, 0, 0, "own"))) for part in (0, 1)]
    return own, events


def position():
    s = lax.axis_index("sp")
    y = lax.axis_index("tp")
    z, x, c = s // 8, (s // 2) % 4, s % 2
    return s, y, z, x, c


def sp_of(z, x, c):
    return lax.rem(z + 8, 8) * 8 + lax.rem(x + 4, 4) * 2 + c


def greet(peers):
    barrier = pltpu.get_barrier_semaphore()
    for peer in peers:
        pl.semaphore_signal(barrier, inc=1, device_id=peer, device_id_type=MESH)
    pl.semaphore_wait(barrier, len(peers))


class YGather:
    def __init__(self, src, dst, send_sem, recv_sem):
        s, y, *_ = position()
        self.src, self.dst, self.send, self.recv = src, dst, send_sem, recv_sem
        self.y = y
        self.up = (s, lax.rem(y + 1, 4))
        self.down = (s, lax.rem(y + 3, 4))

    def copy(self, half, src_y, way, hop):
        slot = way * 3 + (half if hop == 0 else 2)
        return pltpu.make_async_remote_copy(
            src_ref=self.src[half] if hop == 0 else self.dst(src_y, half),
            dst_ref=self.dst(src_y, half),
            send_sem=self.send.at[slot],
            recv_sem=self.recv.at[slot],
            device_id=self.up if way == 0 else self.down,
            device_id_type=MESH,
        )

    def start(self):
        self.copy(0, self.y, 0, 0).start()
        self.copy(1, self.y, 1, 0).start()
        self.copy(1, self.y, 0, 0).start()
        self.copy(0, self.y, 1, 0).start()

    def relay(self):
        below, above = lax.rem(self.y + 3, 4), lax.rem(self.y + 1, 4)
        self.copy(0, below, 0, 0).wait_recv()
        self.copy(0, below, 0, 1).start()
        self.copy(1, above, 1, 0).wait_recv()
        self.copy(1, above, 1, 1).start()

    def finish(self):
        below, above, far = lax.rem(self.y + 3, 4), lax.rem(self.y + 1, 4), lax.rem(self.y + 2, 4)
        self.copy(1, below, 0, 0).wait_recv()
        self.copy(0, above, 1, 0).wait_recv()
        self.copy(0, far, 0, 1).wait_recv()
        self.copy(1, far, 1, 1).wait_recv()
        self.sent()

    def sent(self):
        below, above = lax.rem(self.y + 3, 4), lax.rem(self.y + 1, 4)
        for half in (0, 1):
            for way in (0, 1):
                self.copy(half, self.y, way, 0).wait_send()
        self.copy(0, below, 0, 1).wait_send()
        self.copy(1, above, 1, 1).wait_send()


class YReduce:
    def __init__(self, part, far, near, send_sem, recv_sem, width):
        s, y, *_ = position()
        self.part, self.far, self.near = part, far, near
        self.send, self.recv, self.width = send_sem, recv_sem, width
        self.next = (lax.rem(y + 1, 4), lax.rem(y + 3, 4))
        self.across = lax.rem(y + 2, 4)
        self.dev = [(s, self.next[0]), (s, self.next[1])]

    def copy(self, n, way, kind):
        cols = pl.ds(n * self.width, self.width)
        low, high = pl.ds(0, 16), pl.ds(16, 16)
        merged, plain = (high, low) if way == 0 else (low, high)
        if kind == 0:
            src, dst = self.part.at[self.across, merged, cols], self.far.at[way, :, cols]
        else:
            rows = plain if kind == 1 else merged
            src, dst = self.part.at[self.next[way], rows, cols], self.near.at[way, rows, cols]
        return pltpu.make_async_remote_copy(
            src_ref=src,
            dst_ref=dst,
            send_sem=self.send.at[n, way, kind],
            recv_sem=self.recv.at[n, way, kind],
            device_id=self.dev[way],
            device_id_type=MESH,
        )

    def start(self, n):
        for kind in (0, 1):
            for way in (0, 1):
                self.copy(n, way, kind).start()

    def relay(self, n):
        cols = pl.ds(n * self.width, self.width)
        for way in (0, 1):
            rows = pl.ds(16, 16) if way == 0 else pl.ds(0, 16)
            self.copy(n, way, 0).wait_recv()
            self.part[self.next[way], rows, cols] = (
                self.part[self.next[way], rows, cols].astype(F32) + self.far[way, :, cols].astype(F32)
            ).astype(BF)
            self.copy(n, way, 2).start()

    def arrived(self, n):
        for kind in (1, 2):
            for way in (0, 1):
                self.copy(n, way, kind).wait_recv()

    def sent(self, n):
        for kind in (0, 1, 2):
            for way in (0, 1):
                self.copy(n, way, kind).wait_send()


REL = (0, -1, 1, -2, 2, -3, 3, 4)
AT = {r: i for i, r in enumerate(REL)}
AT[-4] = AT[4]


class Exchange:
    def __init__(self, src, dst, relay, send, recv, rsend, rrecv, width):
        self.width = width
        self.src, self.dst, self.rl = src, dst, relay
        self.send, self.recv, self.rsend, self.rrecv = send, recv, rsend, rrecv
        s, y, z, x, c = position()
        self.core = (c, 1 - c)
        self.dev = lambda d, core: (sp_of(z, x + d, core), y)

    def direct(self, g, d, crel, n=0):
        cols = pl.ds(n * self.width, self.width)
        m = d * 2 + crel
        slot = ((4 - d) % 4) * 2 + crel
        if d == 2:
            return pltpu.make_async_remote_copy(
                src_ref=self.src.at[pl.ds(g * 128 + 16 * m, 16), cols],
                dst_ref=self.rl.at[g, crel, :, cols],
                send_sem=self.send.at[n, g, m],
                recv_sem=self.rrecv.at[n, g, crel],
                device_id=self.dev(1 if crel == 0 else 3, self.core[0]),
                device_id_type=MESH,
            )
        return pltpu.make_async_remote_copy(
            src_ref=self.src.at[pl.ds(g * 128 + 16 * m, 16), cols],
            dst_ref=self.dst.at[pl.ds(g * 128 + 16 * slot, 16), cols],
            send_sem=self.send.at[n, g, m],
            recv_sem=self.recv.at[n, g, slot],
            device_id=self.dev(d, self.core[crel]),
            device_id_type=MESH,
        )

    def passed(self, g, crel, n=0):
        cols = pl.ds(n * self.width, self.width)
        slot = 4 + crel
        return pltpu.make_async_remote_copy(
            src_ref=self.rl.at[g, crel, :, cols],
            dst_ref=self.dst.at[pl.ds(g * 128 + 16 * slot, 16), cols],
            send_sem=self.rsend.at[n, g, crel],
            recv_sem=self.recv.at[n, g, slot],
            device_id=self.dev(1 if crel == 0 else 3, self.core[crel]),
            device_id_type=MESH,
        )

    def local(self, g, n=0):
        cols = pl.ds(n * self.width, self.width)
        return pltpu.make_async_copy(
            self.src.at[pl.ds(g * 128, 16), cols],
            self.dst.at[pl.ds(g * 128, 16), cols],
            self.recv.at[n, g, 0],
        )

    def start(self, g, n=0):
        for d, crel in ((2, 0), (2, 1), (1, 0), (3, 0), (1, 1), (3, 1), (0, 1)):
            self.direct(g, d, crel, n).start()
        self.local(g, n).start()

    def relay(self, g, n=0):
        for crel in (0, 1):
            self.direct(g, 2, crel, n).wait_recv()
            self.passed(g, crel, n).start()

    def arrived(self, g, n=0):
        self.local(g, n).wait()
        for d, crel in ((0, 1), (1, 0), (3, 0), (1, 1), (3, 1)):
            self.direct(g, d, crel, n).wait_recv()
        for crel in (0, 1):
            self.passed(g, crel, n).wait_recv()

    def sent(self, g, n=0):
        for d, crel in ((2, 0), (2, 1), (1, 0), (3, 0), (1, 1), (3, 1), (0, 1)):
            self.direct(g, d, crel, n).wait_send()
        for crel in (0, 1):
            self.passed(g, crel, n).wait_send()


def layer_kernel(
    fq, fk, fv, gf, hq, hk, hv, gh, res, wf, wh, gain, names_in, scale_in, eg, eu, ed, sg, su, sd,
    out,
    kva, kvb, qs, acc, mx, tot, att, part, far, near, resv, mid, wfv, whv,
    tiles, tok, sel, wts, sb, xr, yb, yr, rl0, rl1, pz, zr, gu, dn, hid, sgv, suv, sdv, nall, spart,
    sfar, snear,
    own_sem, kv_send, kv_recv, rs_send, rs_recv, res_sem,
    tile_send, tile_recv, ag_send, ag_recv, zs_send, zs_recv,
    x_send, x_recv, xr_send, xr_recv, w_send, w_recv, g_send, g_recv, s_send, s_recv, ld,
):
    s, y, z, x, c = position()
    sib = (s + 1 - 2 * c, y)
    to = {
        "z+": (sp_of(z + 1, x, c), y),
        "z-": (sp_of(z - 1, x, c), y),
        "x+": (sp_of(z, x + 1, c), y),
        "x-": (sp_of(z, x - 1, c), y),
    }
    zup, zdown = to["z+"], to["z-"]
    zs = [(sp_of(z + k, x, c), y) for k in range(1, 8)]
    xs = [(sp_of(z, x + d, core), y) for d in (1, 3) for core in (c, 1 - c)]
    greet(zs + xs + [sib] + [(s, lax.rem(y + k, 4)) for k in (1, 2, 3)])

    kv = (kva, kvb)
    pieces = [
        (fk, kva, 0), (fv, kva, 128), (hk, kvb, 0), (hv, kvb, 128),
    ]
    own = [
        pltpu.make_async_copy(src, dst.at[s, :, pl.ds(at, 128)], own_sem.at[i])
        for i, (src, dst, at) in enumerate(pieces)
    ]
    for copy in own:
        copy.start()
    res_copy = pltpu.make_async_copy(res.at[pl.ds(y * 32, 32)], resv, res_sem)
    res_copy.start()

    loads = [
        pltpu.make_async_copy(eg, gu.at[y, :, pl.ds(0, 128)], ld.at[1]),
        pltpu.make_async_copy(eu, gu.at[y, :, pl.ds(128, 128)], ld.at[2]),
        pltpu.make_async_copy(ed, dn.at[pl.ds(y * 128, 128)], ld.at[3]),
        pltpu.make_async_copy(sg, sgv, ld.at[4]),
        pltpu.make_async_copy(su, suv, ld.at[5]),
        pltpu.make_async_copy(sd, sdv, ld.at[6]),
        pltpu.make_async_copy(wf, wfv, ld.at[7]),
        pltpu.make_async_copy(wh, whv, ld.at[8]),
    ]
    table = jnp.concatenate([names_in[...].astype(F32), scale_in[...]], axis=0)
    own_table = jnp.zeros((8, 128), F32)
    for k in range(4):
        own_table = own_table + pltpu.roll(table, (128 - 32 * k) % 128, 1) * (y == k).astype(F32)
    own_table = jnp.where(lax.broadcasted_iota(jnp.int32, (8, 128), 1) < 32, own_table, 0.0)
    spread = own_table
    for k in (1, 2, 3):
        spread = spread + pltpu.roll(own_table, 32 * k, 1)
    tiles[z] = spread

    def hop(prt, idx, device):
        return pltpu.make_async_remote_copy(
            src_ref=kv[prt].at[idx],
            dst_ref=kv[prt].at[idx],
            send_sem=kv_send.at[prt],
            recv_sem=kv_recv.at[prt, idx],
            device_id=device,
            device_id_type=MESH,
        )

    own_events, events = kv_schedule()
    for prt, _, _, links in own_events:
        own[2 * prt].wait()
        own[2 * prt + 1].wait()
        for link in links:
            hop(prt, s, to[link]).start()
        hop(prt, s, sib).start()

    def tile_copy(k):
        return pltpu.make_async_remote_copy(
            src_ref=tiles.at[z],
            dst_ref=tiles.at[z],
            send_sem=tile_send.at[k - 1],
            recv_sem=tile_recv.at[k - 1],
            device_id=zs[k - 1],
            device_id_type=MESH,
        )


    for k in range(1, 8):
        tile_copy(k).start()

    gates = YGather(
        [eg.at[pl.ds(h * 2048, 2048)] for h in (0, 1)],
        lambda j, h: gu.at[j, pl.ds(h * 2048, 2048), pl.ds(0, 128)],
        w_send.at[0], w_recv.at[0],
    )

    def up_rows(at, count, slot):
        return YGather(
            [eu.at[pl.ds(at + h * count // 2, count // 2)] for h in (0, 1)],
            lambda j, h: gu.at[j, pl.ds(at + h * count // 2, count // 2), pl.ds(128, 128)],
            w_send.at[slot], w_recv.at[slot],
        )

    ups0 = up_rows(0, UP_ROWS, 1)
    ups = up_rows(UP_ROWS, 4096 - UP_ROWS, 2)
    gates.start()
    ups0.start()
    for copy in loads:
        copy.start()

    lane = lax.broadcasted_iota(jnp.int32, (128, 128), 1)
    qs[0, 0:128] = fq[:, 0:128]
    qs[0, 128:256] = fq[:, 128:256]
    h01 = hq[:, 0:128].astype(F32)
    h23 = hq[:, 128:256].astype(F32)
    qs[1, 0:128] = jnp.where(lane < 64, h01, 0.0).astype(BF)
    qs[1, 128:256] = jnp.where(lane < 64, pltpu.roll(h01, 64, 1), 0.0).astype(BF)
    qs[2, 0:128] = jnp.where(lane >= 64, pltpu.roll(h23, 64, 1), 0.0).astype(BF)
    qs[2, 128:256] = jnp.where(lane >= 64, h23, 0.0).astype(BF)
    acc[...] = jnp.zeros_like(acc)
    tot[...] = jnp.zeros_like(tot)
    mx[...] = jnp.full_like(mx, NEG)

    row0 = s * 128
    gfirst = gf[:, pl.ds(pl.multiple_of(row0, 128), 128)][:, 0:1]
    hfirst = gh[:, pl.ds(pl.multiple_of(row0, 128), 128)][:, 0:1]

    def attend_to(plane, g, masked):
        key0 = pl.multiple_of(plane * 1024, 1024)
        if g == 0:
            gate = (gf[:, pl.ds(key0, 1024)] - gfirst) * LOG2E
        else:
            gate = (gh[:, pl.ds(key0, 1024)] - hfirst) * LOG2E
        store = kva if g == 0 else kvb
        k = store[pl.ds(plane * 8, 8), :, 0:128].reshape(1024, 128)
        v = store[pl.ds(plane * 8, 8), :, 128:256].reshape(1024, 128)
        scale = (128 ** -0.5 if g == 0 else 0.125) * LOG2E
        scores = lax.dot_general(
            qs[g], k, (((1,), (1,)), ((), ())), preferred_element_type=F32
        )
        for r in (0, 1):
            head = r if g == 0 else 2 * (g - 1) + r
            t = scores[r * 128 : (r + 1) * 128] * scale - gate[head : head + 1]
            if masked:
                qpos = (s % 8) * 128 + lax.broadcasted_iota(jnp.int32, (128, 1024), 0)
                kpos = lax.broadcasted_iota(jnp.int32, (128, 1024), 1)
                t = jnp.where(kpos <= qpos, t, NEG)
            old = mx[g, pl.ds(r * 128, 128)]
            new = jnp.maximum(old, jnp.max(t, axis=1, keepdims=True))
            p = jnp.exp2(t - new[:, 0:1])
            shrink = jnp.exp2(old - new)
            mx[g, pl.ds(r * 128, 128)] = new
            tot[g, pl.ds(r * 128, 128)] = (
                tot[g, pl.ds(r * 128, 128)] * shrink + jnp.sum(p, axis=1, keepdims=True)
            )
            acc[g, pl.ds(r * 128, 128)] = acc[g, pl.ds(r * 128, 128)] * shrink + jnp.dot(
                p.astype(BF), v, preferred_element_type=F32
            )

    waiting = []
    for dz in range(-3, 5):
        for g in range(3):
            last = max(
                i for i, (prt, edz, *_) in enumerate(events) if edz == dz and prt == min(g, 1)
            )
            waiting.append((last + 3, g, dz))
    waiting.sort()

    def next_item():
        _, g, dz = waiting.pop(0)
        plane = lax.rem(z - dz + 8, 8)
        if g < 2:
            for col in range(4):
                hop(g, sp_of(plane, col, 1 - c), sib).wait_recv()
        if dz == 0:
            attend_to(z, g, True)
        else:

            @pl.when(plane < z)
            def _():
                attend_to(plane, g, False)

    for i, (prt, dz, dx, links) in enumerate(events):
        idx = sp_of(z - dz, x - dx, c)
        hop(prt, idx, sib).wait_recv()
        for link in links:
            hop(prt, idx, to[link]).start()
        hop(prt, idx, sib).start()
        if waiting and waiting[0][0] <= i:
            next_item()
        if i == 30:
            gates.relay()
        if i == 46:
            ups0.relay()
    while waiting:
        next_item()

    outs = [
        [acc[g, r * 128 : (r + 1) * 128] / tot[g, r * 128 : (r + 1) * 128] for r in (0, 1)]
        for g in range(3)
    ]
    att[:, 0:128] = outs[0][0].astype(BF)
    att[:, 128:256] = outs[0][1].astype(BF)
    att[:, 256:384] = jnp.where(lane < 64, outs[1][0], pltpu.roll(outs[1][1], 64, 1)).astype(BF)
    att[:, 384:512] = jnp.where(lane < 64, pltpu.roll(outs[2][0], 64, 1), outs[2][1]).astype(BF)

    for copy in loads[6:]:
        copy.wait()
    asums = YReduce(part, far, near, rs_send, rs_recv, 1024)
    for n in range(4):
        cols = slice(n * 1024, (n + 1) * 1024)
        product = jnp.dot(att[:, 0:256], wfv[:, cols], preferred_element_type=F32) + jnp.dot(
            att[:, 256:512], whv[:, cols], preferred_element_type=F32
        )
        part[:, :, cols] = product.astype(BF).reshape(4, 32, 1024)
        asums.start(n)
    for k in range(1, 8):
        tile_copy(k).wait_recv()

    lane4 = lax.broadcasted_iota(jnp.int32, (4, 128), 1) // 32
    row16 = lax.broadcasted_iota(jnp.int32, (16, 128), 0)
    lane16 = lax.broadcasted_iota(jnp.int32, (16, 128), 1) // 32
    r0 = lax.broadcasted_iota(jnp.int32, (128, 128), 0)
    r1 = lax.broadcasted_iota(jnp.int32, (128, 128), 1)
    earlier = jnp.where((r0 // 32 == r1 // 32) & (r0 < r1), 1.0, 0.0).astype(BF)

    def picks(g):
        names = jnp.zeros((4, 128), F32)
        scale = jnp.zeros((4, 128), F32)
        for i in range(4):
            src = lax.rem(z + REL[g * 4 + i] + 8, 8)
            names = jnp.where(lane4 == i, tiles[src, 0:4], names)
            scale = jnp.where(lane4 == i, tiles[src, 4:8], scale)
        occ, wrow = [], []
        for d in range(4):
            for crel in (0, 1):
                core = c + crel - 2 * c * crel
                expert = (z * 8 + lax.rem(x + d, 4) * 2 + core).astype(F32)
                hit = jnp.where(names == expert, 1.0, 0.0)
                occ.append(jnp.sum(hit, axis=0, keepdims=True))
                wrow.append(jnp.sum(hit * scale, axis=0, keepdims=True))
        occupied = jnp.concatenate(occ, axis=0)
        rank = jnp.dot(occupied.astype(BF), earlier, preferred_element_type=F32)
        weighted = []
        for m in range(8):
            chosen = (
                (lane16 == row16 // 4)
                & (rank[m : m + 1] == (row16 % 4).astype(F32))
                & (occ[m] > 0.5)
            )
            sel[g, pl.ds(16 * m, 16)] = jnp.where(chosen, 1.0, 0.0).astype(BF)
            weighted.append(jnp.where(chosen, wrow[m], 0.0))
        full = jnp.concatenate(weighted, axis=0).T
        high = full.astype(BF)
        wts[g, 0] = high
        wts[g, 1] = (full - high.astype(F32)).astype(BF)

    picks(0)
    picks(1)
    for n in range(4):
        asums.relay(n)
    ups.start()
    res_copy.wait()
    square = jnp.zeros((32, 1), F32)
    for n in range(4):
        cols = slice(n * 1024, (n + 1) * 1024)
        total = resv[:, cols].astype(F32) + part[y, :, cols].astype(F32)
        asums.arrived(n)
        total = total + near[0, :, cols].astype(F32) + near[1, :, cols].astype(F32)
        mid[:, cols] = total
        square = square + jnp.sum(total * total, axis=1, keepdims=True)
    factor = lax.rsqrt(square * (1.0 / D) + 1e-06)
    for n in range(4):
        cols = slice(n * 1024, (n + 1) * 1024)
        normed = (mid[:, cols] * factor * gain[:, cols]).astype(BF)
        tok[0:32, cols] = normed
        nall[y, :, cols] = normed

    def ag(way, k, h):
        sign = -1 if way == 0 else 1
        return pltpu.make_async_remote_copy(
            src_ref=tok.at[pl.ds(32 * AT[sign * (k - 1)] + 16 * h, 16)],
            dst_ref=tok.at[pl.ds(32 * AT[sign * k] + 16 * h, 16)],
            send_sem=ag_send.at[way, k - 1, h],
            recv_sem=ag_recv.at[way, k - 1, h],
            device_id=zup if way == 0 else zdown,
            device_id_type=MESH,
        )

    def hops(way, k):
        return (0, 1) if k < 4 else ((0,) if way == 0 else (1,))

    for h in (0, 1):
        for way in (0, 1):
            ag(way, 1, h).start()

    def down_chunk(n):
        cols = pl.ds(n * 1024, 1024)
        return YGather(
            [ed.at[pl.ds(h * 64, 64), cols] for h in (0, 1)],
            lambda j, h: dn.at[pl.ds(j * 128 + h * 64, 64), cols],
            w_send.at[3 + n], w_recv.at[3 + n],
        )

    downs = [down_chunk(n) for n in range(4)]
    rows = YGather(
        [nall.at[y, pl.ds(h * 16, 16)] for h in (0, 1)],
        lambda j, h: nall.at[j, pl.ds(h * 16, 16)],
        g_send, g_recv,
    )
    downs[0].start()

    fwd = Exchange(sb, xr, rl0, x_send.at[pl.ds(0, 1)], x_recv.at[pl.ds(0, 1)], xr_send.at[pl.ds(0, 1)], xr_recv.at[pl.ds(0, 1)], D)
    back = Exchange(yb, yr, rl1, x_send.at[pl.ds(1, 4)], x_recv.at[pl.ds(1, 4)], xr_send.at[pl.ds(1, 4)], xr_recv.at[pl.ds(1, 4)], 1024)

    def select(g):
        for n in range(4):
            cols = slice(n * 1024, (n + 1) * 1024)
            sb[g * 128 : (g + 1) * 128, cols] = jnp.dot(
                sel[g], tok[g * 128 : (g + 1) * 128, cols], preferred_element_type=F32
            ).astype(BF)
        fwd.start(g)

    for k in range(1, 5):
        for h in (0, 1):
            for way in (0, 1):
                if h in hops(way, k):
                    ag(way, k, h).wait_recv()
                    if k < 4 and h in hops(way, k + 1):
                        ag(way, k + 1, h).start()
        if k == 2:
            select(0)
            ups.relay()
            downs[1].start()
        if k == 3:
            fwd.relay(0)
            downs[0].relay()
            downs[2].start()
    select(1)
    downs[1].relay()
    downs[3].start()

    fwd.relay(1)
    downs[2].relay()
    rows.start()
    for copy in loads[:6]:
        copy.wait()
    gates.finish()
    ups0.finish()
    ups.finish()
    fwd.arrived(0)
    fwd.arrived(1)

    @pl.loop(0, 4)
    def _(j):
        both = jnp.dot(xr[...], gu[j], preferred_element_type=F32)
        g, u = both[:, 0:128], both[:, 128:256]
        hid[:, pl.ds(pl.multiple_of(j * 128, 128), 128)] = (g / (1.0 + jnp.exp(-g)) * u).astype(BF)

    sums = YReduce(spart, sfar, snear, s_send, s_recv, D)

    def finish_rows(n):
        downs[n].finish()
        cols = slice(n * 1024, (n + 1) * 1024)
        yb[:, cols] = jnp.dot(hid[...], dn[:, cols], preferred_element_type=F32).astype(BF)
        for g in (1, 0):
            back.start(g, n)

    def shared():
        rows.finish()
        everyone = nall[...].reshape(128, D)
        g = jnp.dot(everyone, sgv[...], preferred_element_type=F32)
        u = jnp.dot(everyone, suv[...], preferred_element_type=F32)
        shared_hidden = (g / (1.0 + jnp.exp(-g)) * u).astype(BF)
        for n in range(4):
            cols = slice(n * 1024, (n + 1) * 1024)
            spart[:, :, cols] = (
                jnp.dot(shared_hidden, sdv[:, cols], preferred_element_type=F32)
                .astype(BF)
                .reshape(4, 32, 1024)
            )
        sums.start(0)

    def combine(n):
        cols = slice(n * 1024, (n + 1) * 1024)
        for g in (1, 0):
            back.arrived(g, n)
            pz[g * 128 : (g + 1) * 128, cols] = (
                jnp.dot(wts[g, 0], yr[g * 128 : (g + 1) * 128, cols], preferred_element_type=F32)
                + jnp.dot(wts[g, 1], yr[g * 128 : (g + 1) * 128, cols], preferred_element_type=F32)
            ).astype(BF)

    def zsum(n, way, m, h):
        sign = 1 if way == 0 else -1
        cols = pl.ds(n * 1024, 1024)
        return pltpu.make_async_remote_copy(
            src_ref=pz.at[pl.ds(32 * AT[sign * m] + 16 * h, 16), cols],
            dst_ref=zr.at[way, m - 1, pl.ds(16 * h, 16), cols],
            send_sem=zs_send.at[n, way, m - 1, h],
            recv_sem=zs_recv.at[n, way, m - 1, h],
            device_id=zup if way == 0 else zdown,
            device_id_type=MESH,
        )

    def add_and_send(n, m):
        cols = slice(n * 1024, (n + 1) * 1024)
        for h in (0, 1):
            for way in (0, 1):
                if h not in hops(way, m):
                    continue
                sign = 1 if way == 0 else -1
                if m < 4 and h in hops(way, m + 1):
                    zsum(n, way, m + 1, h).wait_recv()
                    at = slice(32 * AT[sign * m] + 16 * h, 32 * AT[sign * m] + 16 * h + 16)
                    pz[at, cols] = (
                        pz[at, cols].astype(F32) + zr[way, m, 16 * h : 16 * h + 16, cols].astype(F32)
                    ).astype(BF)
                zsum(n, way, m, h).start()

    def last(n):
        cols = slice(n * 1024, (n + 1) * 1024)
        for h in (0, 1):
            for way in (0, 1):
                zsum(n, way, 1, h).wait_recv()
        total = mid[:, cols] + spart[y, :, cols].astype(F32)
        total = total + snear[0, :, cols].astype(F32) + snear[1, :, cols].astype(F32)
        total = total + pz[0:32, cols].astype(F32)
        total = total + zr[0, 0, :, cols].astype(F32) + zr[1, 0, :, cols].astype(F32)
        out[:, cols] = total.astype(BF)

    for t in range(10):
        for m in (1, 2, 3):
            if 0 <= t - 6 + m <= 3:
                add_and_send(t - 6 + m, m)
        if 2 <= t < 6:
            combine(t - 2)
            add_and_send(t - 2, 4)
        if 1 <= t < 5:
            for g in (1, 0):
                back.relay(g, t - 1)
        if t < 4:
            finish_rows(t)
        if t == 0:
            downs[3].relay()
        if t == 2:
            rows.relay()
        if t == 5:
            shared()
        if t == 7:
            sums.relay(0)
        if t == 8:
            sums.arrived(0)
            last(0)
            last(1)
            last(2)
    last(3)

    for k in range(1, 8):
        tile_copy(k).wait_send()
    for k in range(1, 5):
        for way in (0, 1):
            for h in hops(way, k):
                ag(way, k, h).wait_send()
                for n in range(4):
                    zsum(n, way, k, h).wait_send()
    for g in (0, 1):
        fwd.sent(g)
        for n in range(4):
            back.sent(g, n)
    sums.sent(0)

    for n in range(4):
        asums.sent(n)
    for prt in (0, 1):
        everything = kv[prt].at[pl.ds(0, 63)]
        pltpu.make_async_copy(everything, everything, kv_send.at[prt]).wait()


def layer(*args):
    vmem = pl.BlockSpec(memory_space=pltpu.VMEM)
    anym = pl.BlockSpec(memory_space=pl.ANY)
    dma = pltpu.SemaphoreType.DMA
    bf = lambda *shape: pltpu.VMEM(shape, BF)
    return pl.pallas_call(
        layer_kernel,
        name="layer",
        out_shape=jax.ShapeDtypeStruct((32, D), BF),
        in_specs=[vmem, anym, anym, vmem, vmem, anym, anym, vmem, anym, anym, anym, vmem, vmem, vmem]
        + [anym] * 6,
        out_specs=vmem,
        scratch_shapes=[
            bf(64, 128, 256), bf(64, 128, 256), bf(3, 256, 128),
            pltpu.VMEM((3, 256, 128), F32), pltpu.VMEM((3, 256, 128), F32),
            pltpu.VMEM((3, 256, 128), F32),
            bf(128, 512), bf(4, 32, D), bf(2, 16, D), bf(2, 32, D), bf(32, D),
            pltpu.VMEM((32, D), F32), bf(256, D), bf(256, D),
            pltpu.VMEM((8, 8, 128), F32), bf(256, D), bf(2, 128, 128), bf(2, 2, 128, 128),
            bf(256, D), bf(256, D), bf(256, D), bf(256, D), bf(2, 2, 16, D), bf(2, 2, 16, D),
            bf(256, D), bf(2, 4, 32, D), bf(4, 4096, 256), bf(512, D), bf(256, 512),
            bf(4096, 128), bf(4096, 128), bf(128, D), bf(4, 32, D), bf(4, 32, D),
            bf(2, 16, D), bf(2, 32, D),
            dma((4,)), dma((2,)), dma((2, 64)), dma((4, 2, 3)), dma((4, 2, 3)), dma,
            dma((7,)), dma((7,)), dma((2, 4, 2)), dma((2, 4, 2)),
            dma((4, 2, 4, 2)), dma((4, 2, 4, 2)), dma((5, 2, 8)), dma((5, 2, 8)),
            dma((5, 2, 2)), dma((5, 2, 2)), dma((7, 6)), dma((7, 6)), dma((6,)), dma((6,)),
            dma((1, 2, 3)), dma((1, 2, 3)), dma((9,)),
        ],
        compiler_params=pltpu.CompilerParams(
            collective_id=0, has_side_effects=True, vmem_limit_bytes=62 * 1024 * 1024
        ),
    )(*args)


def body(
    full_queries, full_keys, full_values, full_gates, half_queries, half_keys, half_values,
    half_gates, residual, full_output, half_output, norm_gain, routes, route_weights,
    expert_gate, expert_up, expert_down, shared_gate, shared_up, shared_down,
):
    return layer(
        full_queries, full_keys, full_values, full_gates.T, half_queries, half_keys, half_values,
        half_gates.T, residual, full_output, half_output, norm_gain.reshape(1, D), routes.T, route_weights.T,
        expert_gate[0], expert_up[0], expert_down[0], shared_gate, shared_up, shared_down,
    )


def solution(mesh):
    return jax.shard_map(
        body,
        mesh=mesh,
        in_specs=(
            P("sp", "tp"), P("sp", "tp"), P("sp", "tp"), P(None, "tp"),
            P("sp", "tp"), P("sp", "tp"), P("sp", "tp"), P(None, "tp"),
            P("sp", None), P("tp", None), P("tp", None), P(), P("sp", None), P("sp", None),
            P("sp", None, "tp"), P("sp", None, "tp"), P("sp", "tp", None),
            P(None, "tp"), P(None, "tp"), P("tp", None),
        ),
        out_specs=P(("sp", "tp"), None),
        check_vma=False,
    )
```
